32 devices in a mesh: sp: 16 (over z, y, core), tp: 2 (over x).
Axes of the slice: x: 2, y: 2, z: 4, core: 2. Of those that a mesh axis runs over, the one named last changes fastest.
Arguments:
- tokens_in: bfloat16 [4096, 2048], P('sp', 'tp'), may hold values from -400 to 400
- norm_gain: float32 [2048], replicated, may hold values from 0.1 to 1.9
- w_query: bfloat16 [2048, 1024], P('sp', 'tp'), may hold values from -0.125 to 0.125
- w_forget: bfloat16 [2048, 1024], P('sp', 'tp'), may hold values from -0.125 to 0.125
- w_input: bfloat16 [2048, 1024], P('sp', 'tp'), may hold values from -0.125 to 0.125
- w_rgate: bfloat16 [2048, 1024], P('sp', 'tp'), may hold values from -0.125 to 0.125
- w_pool_in: bfloat16 [2048, 1024], P('sp', 'tp'), may hold values from -0.125 to 0.125
- w_pgate: bfloat16 [2048, 1024], P('sp', 'tp'), may hold values from -0.125 to 0.125
- floor_rate: float32 [1024], P('tp'), as said below
- extra_logdecay: float32 [4096, 8], P('sp', 'tp'), as said below
- state_gain: float32 [1024], P('tp'), may hold values from 0.1 to 1.9
- pool_mix: bfloat16 [8, 128, 128], P('tp'), may hold values from -0.5 to 0.5
- pool_gain: float32 [1024], P('tp'), may hold values from 0.1 to 1.9
- out_rec: bfloat16 [1024, 2048], P('tp', 'sp'), may hold values from -0.125 to 0.125
- out_pool: bfloat16 [1024, 2048], P('tp', 'sp'), may hold values from -0.125 to 0.125
- post_gain: float32 [2048], replicated, may hold values from 0.1 to 1.9
Outputs:
- mixed_out: bfloat16 [4096, 2048], P(('sp', 'tp'))
The draws below stay inside these ranges and needn't reach their ends.
Inputs may be any that keep to these rules, and one draw needn't show every extreme that they name: `floor_rate`: every entry is positive. `extra_logdecay`: every entry is at most zero.
All inputs are finite; a program needn't handle non-finite values.
Results may differ from the reference program's by a relative error of at most 0.015.
Values may be sent and summed in bfloat16 or wider, within the bound.
A program may use at most 64 MiB of HBM per device.

```python
import math
import jax
import jax.numpy as jnp
from jax import lax

D = 2048
HEADS = 8
DK = 128
BLOCK = 64
TOK_DEV = 256
W = 1024
TOKENS = 4096
N_TP = 2


def draw_tokens_in(key, part):
    first, second, third = jax.random.split(jax.random.fold_in(key, 3), 3)
    row_scale = jnp.exp(jax.random.uniform(first, (TOKENS, 1), jnp.float32) * math.log(10.0))
    col_scale = jnp.exp(jax.random.uniform(second, (1, D), jnp.float32) * math.log(10.0))
    starting_shift_amount = jax.random.normal(third, (TOKENS, D), jnp.float32)
    starting_shift_amount = jnp.clip(starting_shift_amount, -4.0, 4.0)
    return (starting_shift_amount * row_scale * col_scale).astype(jnp.bfloat16)


def draw_floor_rate(key, part):
    first, second = jax.random.split(jax.random.fold_in(key, 11), 2)
    ranks = jax.random.permutation(first, HEADS)
    uniform = jax.random.uniform(second, (HEADS, DK), jnp.float32)
    kind = jnp.where(ranks < HEADS // 4, 0, jnp.where(ranks < HEADS // 2, 1, 2))
    fast = jnp.exp(math.log(0.02) + uniform * math.log(4.0))
    medium_low = min(1.0 / TOK_DEV, 0.01)
    medium = jnp.exp(math.log(medium_low) + uniform * math.log(8.0))
    slow = jnp.exp(jnp.log(0.3 / TOKENS) + uniform * math.log(4.0 / 0.3))
    rate = jnp.where(kind[:, None] == 0, fast, jnp.where(kind[:, None] == 1, medium, slow))
    rate = jnp.minimum(rate, 0.08)
    return rate.reshape(HEADS * DK).astype(jnp.float32)


def draw_extra_logdecay(key, part):
    first, second, third = jax.random.split(jax.random.fold_in(key, 17), 3)
    devices = TOKENS // TOK_DEV
    factor = jnp.exp(math.log(0.3) + jax.random.uniform(first, (devices,), jnp.float32) * math.log(10.0))
    starting_shift_amount = -jnp.repeat(factor, TOK_DEV)[:, None] / TOKENS * jnp.ones((1, HEADS), jnp.float32)
    averaging_locations = jax.random.randint(second, (4, HEADS), 0, TOKENS)
    sigmoid_weighting = jnp.log(jax.random.uniform(third, (4, HEADS), jnp.float32, 0.5, 0.8))
    sequence_step_number = jnp.arange(TOKENS)[:, None, None]
    packet_clusters = jnp.sum(jnp.where(sequence_step_number == averaging_locations[None, :, :], sigmoid_weighting[None, :, :], 0.0), axis=1)
    return (starting_shift_amount + packet_clusters).astype(jnp.float32)


def shard_levels(rng, dims, pieces, least, largest):
    gain = 1.0
    for axis_at, blocks in pieces:
        heights = jax.random.uniform(jax.random.fold_in(jax.random.fold_in(rng, 6), axis_at), (blocks,), jnp.float32, least / len(pieces), largest / len(pieces))
        gain = gain * jnp.repeat(jnp.exp(heights), dims[axis_at] // blocks).reshape((-1,) + (1,) * (len(dims) - 1 - axis_at))
    return gain


def normal_values(rng, dims, width, bound, cuts=(), held_as=jnp.bfloat16):
    drawn = jax.random.normal(rng, dims, jnp.float32) * width
    if len(cuts) > 0:
        drawn = shard_levels(rng, dims, cuts, -0.22, 0.18) * drawn
    return jnp.clip(drawn, min=-bound, max=bound).astype(held_as)


def setup_inputs(seed: int = 0) -> dict:
    arg_keys = jax.random.split(jax.random.key(seed), 17)
    return {
        "tokens_in": draw_tokens_in(jax.random.fold_in(arg_keys[16], 71), 0),
        "norm_gain": jnp.clip(1.0 + 0.18 * jax.random.normal(arg_keys[1], (D,), jnp.float32), 0.1, 1.9),
        "w_query": normal_values(arg_keys[2], (D, W), D ** -0.5, 0.125, ((0, 16), (1, 2))),
        "w_forget": normal_values(arg_keys[3], (D, W), D ** -0.5, 0.125, ((0, 16), (1, 2))),
        "w_input": normal_values(arg_keys[4], (D, W), D ** -0.5, 0.125, ((0, 16), (1, 2))),
        "w_rgate": normal_values(arg_keys[5], (D, W), D ** -0.5, 0.125, ((0, 16), (1, 2))),
        "w_pool_in": normal_values(arg_keys[6], (D, W), D ** -0.5, 0.125, ((0, 16), (1, 2))),
        "w_pgate": normal_values(arg_keys[7], (D, W), D ** -0.5, 0.125, ((0, 16), (1, 2))),
        "floor_rate": draw_floor_rate(jax.random.fold_in(arg_keys[16], 71), 0),
        "extra_logdecay": draw_extra_logdecay(jax.random.fold_in(arg_keys[16], 71), 0),
        "state_gain": jnp.clip(1.0 + 0.18 * jax.random.normal(arg_keys[10], (W,), jnp.float32), 0.1, 1.9),
        "pool_mix": normal_values(arg_keys[11], (HEADS, DK, DK), DK ** -0.5, 0.5, ((0, 2),)),
        "pool_gain": jnp.clip(1.0 + 0.18 * jax.random.normal(arg_keys[12], (W,), jnp.float32), 0.1, 1.9),
        "out_rec": normal_values(arg_keys[13], (W, D), (2 * W) ** -0.5, 0.125, ((0, 2), (1, 16))),
        "out_pool": normal_values(arg_keys[14], (W, D), (2 * W) ** -0.5, 0.125, ((0, 2), (1, 16))),
        "post_gain": jnp.clip(1.0 + 0.18 * jax.random.normal(arg_keys[15], (D,), jnp.float32), 0.1, 1.9),
    }


eps = 1e-06
coarsest_scale_depth = lax.Precision.HIGHEST

def recurrence(query, key_gate, inputs, log_forget):
    blocks = TOKENS // BLOCK

    def to_blocks(array):
        return array.reshape(blocks, BLOCK, HEADS, DK).transpose(0, 2, 1, 3)
    causal = jnp.arange(BLOCK)[:, None] >= jnp.arange(BLOCK)[None, :]

    def advance(carried_memory_matrix, member):
        probe_segment, key_piece, input_piece, gc = member
        prefix_sum_vector = jnp.cumsum(gc, axis=1)
        last_index = prefix_sum_vector[:, -1]
        cross_segment_contribution = jnp.einsum('abz,azy->aby', probe_segment * jnp.exp(prefix_sum_vector), carried_memory_matrix, precision=coarsest_scale_depth)
        diff = prefix_sum_vector[:, :, None, :] - prefix_sum_vector[:, None, :, :]
        weight = jnp.where(causal[None, :, :, None], jnp.exp(jnp.minimum(diff, 0.0)), 0.0)
        scores = jnp.einsum('htk,hsk,htsk->hts', probe_segment, key_piece, weight, precision=coarsest_scale_depth)
        final_result = cross_segment_contribution + jnp.einsum('hts,hsv->htv', scores, input_piece, precision=coarsest_scale_depth)
        carried_memory_matrix = jnp.exp(last_index)[..., None] * carried_memory_matrix + jnp.einsum('njp,njq->npq', key_piece * jnp.exp(last_index[:, None, :] - prefix_sum_vector), input_piece, precision=coarsest_scale_depth)
        return (carried_memory_matrix, final_result)
    start = jnp.zeros((HEADS, DK, DK), jnp.float32)
    qs = query.astype(jnp.float32) * DK ** (-0.5)
    _, final_result = lax.scan(advance, start, (to_blocks(qs), to_blocks(key_gate), to_blocks(inputs.astype(jnp.float32)), to_blocks(log_forget)))
    return final_result.transpose(0, 2, 1, 3).reshape(TOKENS, HEADS * DK)

def reference(tokens_in, norm_gain, w_query, w_forget, w_input, w_rgate, w_pool_in, w_pgate, floor_rate, extra_logdecay, state_gain, pool_mix, pool_gain, out_rec, out_pool, post_gain):
    wide = tokens_in.astype(jnp.float32)
    inv_rms = lax.rsqrt(lax.optimization_barrier(jnp.mean(wide * wide, axis=1, keepdims=True)) + eps)
    scaled = (wide * norm_gain).astype(jnp.bfloat16)

    def project(weight):
        return (jnp.dot(scaled, weight, preferred_element_type=jnp.float32) * inv_rms).astype(jnp.bfloat16)
    query = project(w_query)
    forget = project(w_forget)
    inputs = project(w_input)
    rgate = project(w_rgate)
    pool_in = project(w_pool_in)
    pgate = project(w_pgate)
    forget32 = forget.astype(jnp.float32)
    key_gate = -jnp.expm1(-floor_rate)[None, :] * jax.nn.sigmoid(-forget32)
    log_forget = jnp.log1p(-key_gate) + jnp.repeat(extra_logdecay, DK, axis=1)
    recurrent_output = recurrence(query, key_gate, inputs, log_forget)
    grouped = recurrent_output.reshape(TOKENS, HEADS, DK)
    normed = grouped * lax.rsqrt(lax.optimization_barrier(jnp.mean(grouped * grouped, axis=2, keepdims=True)) + eps)
    y_rec = (normed.reshape(TOKENS, HEADS * DK) * state_gain * jax.nn.silu(rgate.astype(jnp.float32))).astype(jnp.bfloat16)
    group = (jnp.arange(HEADS * DK) // DK).astype(jnp.int32)
    window = jnp.power(2, 1 + group % 4).astype(jnp.int32)
    pool32 = pool_in.astype(jnp.float32)
    extended = jnp.concatenate([jnp.zeros((16, HEADS * DK), jnp.float32), pool32], axis=0)
    total = jnp.zeros((TOKENS, HEADS * DK), jnp.float32)
    for offset in range(16):
        rows_back = extended[16 - offset:16 - offset + TOKENS]
        total = total + jnp.where((offset < window)[None, :], rows_back, 0.0)
    sequence_step_number = jnp.arange(TOKENS).astype(jnp.int32)
    count = jnp.minimum(sequence_step_number[:, None] + 1, window[None, :]).astype(jnp.float32)
    mixed = (total / count - pool32).astype(jnp.bfloat16)
    mapped = jnp.einsum('tgc,gcd->tgd', mixed.reshape(TOKENS, HEADS, DK).astype(jnp.float32), pool_mix.astype(jnp.float32)).reshape(TOKENS, HEADS * DK)
    y_pool = (mapped * pool_gain * jax.nn.silu(pgate.astype(jnp.float32))).astype(jnp.bfloat16)
    share = HEADS * DK // N_TP
    summed = jnp.zeros((TOKENS, D), jnp.float32)
    for member in range(N_TP):
        lower = member * share
        left = jnp.concatenate([y_rec[:, lower:lower + share], y_pool[:, lower:lower + share]], axis=1)
        right = jnp.concatenate([out_rec[lower:lower + share], out_pool[lower:lower + share]], axis=0)
        partial_sum = jnp.dot(left, right, preferred_element_type=jnp.float32).astype(jnp.bfloat16)
        summed = summed + partial_sum.astype(jnp.float32)
    final = summed * lax.rsqrt(lax.optimization_barrier(jnp.mean(summed * summed, axis=1, keepdims=True)) + eps) * post_gain
    return final.astype(jnp.bfloat16)
```

```python
import functools

import jax
import jax.numpy as jnp
from jax import lax
from jax.experimental import pallas as pl
from jax.experimental.pallas import tpu as pltpu
from jax.sharding import PartitionSpec as P

DK = 128


eps = 1e-06
coarsest_scale_depth = lax.Precision.HIGHEST


PIECES = 4


def ring_place(chip, chips):
    odd = chip % 2
    return (1 - odd) * (chip // 2) + odd * (chips - 1 - chip // 2)


def ring_chip(place, chips):
    back = place // (chips // 2)
    return (1 - back) * (2 * place) + back * (2 * (chips - 1 - place) + 1)


def project_kernel(
    n,
    n_tp,
    tok_ref,
    gain_ref,
    w0,
    w1,
    w2,
    w3,
    w4,
    w5,
    proj_ref,
    wide,
    scaled,
    weights,
    acc,
    tok_send,
    tok_recv,
    own_sem,
    ring_send,
    ring_recv,
    core_send,
    core_recv,
):
    chips = n // 2
    steps = chips // 2
    me = lax.axis_index("sp")
    tp = lax.axis_index("tp")
    core = me % 2
    place = ring_place(me // 2, chips)

    def chip_at(offset):
        return ring_chip((place + offset + chips) % chips, chips)

    following = 2 * chip_at(1) + core
    preceding = 2 * chip_at(-1) + core
    partner = 2 * (me // 2) + 1 - core
    parts = (w0, w1, w2, w3, w4, w5)
    rows, part_cols = w0.shape
    my_rows = pl.ds(pl.multiple_of(me * rows, 16), rows)
    owns = []
    for i, part in enumerate(parts):
        block = weights.at[my_rows, pl.ds(i * part_cols, part_cols)]
        owns.append(pltpu.make_async_copy(part, block, own_sem.at[i]))
        owns[-1].start()
    piece = rows // PIECES
    features = tok_ref.shape[1]

    barrier = pltpu.get_barrier_semaphore()
    for peer in (following, preceding, partner):
        pl.semaphore_signal(barrier, inc=1, device_id={"sp": peer})
    for turn in range(1, n_tp):
        pl.semaphore_signal(barrier, inc=1, device_id={"tp": (tp + turn) % n_tp})
    pl.semaphore_wait(barrier, 3 + n_tp - 1)

    def rows_of(chip, which, q):
        start = (2 * chip + which) * rows + q * piece
        return pl.ds(pl.multiple_of(start, 8), piece)

    sends = []

    def to_core(offset, q, source):
        slot = offset + steps - 1
        copy = pltpu.make_async_remote_copy(
            src_ref=source,
            dst_ref=weights.at[rows_of(chip_at(offset), core, q)],
            send_sem=core_send.at[slot, q],
            recv_sem=core_recv.at[slot, q],
            device_id={"sp": partner},
        )
        copy.start()
        sends.append(copy)

    def from_core(offset, q):
        slot = offset + steps - 1
        dst = weights.at[rows_of(chip_at(offset), 1 - core, q)]
        pltpu.make_async_remote_copy(
            src_ref=dst,
            dst_ref=dst,
            send_sem=core_send.at[slot, q],
            recv_sem=core_recv.at[slot, q],
            device_id={"sp": partner},
        ).wait_recv()

    def pieces_of(direction, step):
        if step < steps - 1:
            return range(PIECES)
        half = PIECES // 2
        return range(half) if direction == 0 else range(half, PIECES)

    def ring_copy(direction, step, q, source):
        offset = -step if direction == 0 else step
        dst = weights.at[rows_of(chip_at(offset), core, q)]
        return pltpu.make_async_remote_copy(
            src_ref=dst if source is None else source,
            dst_ref=dst,
            send_sem=ring_send.at[direction, step, q],
            recv_sem=ring_recv.at[direction, step, q],
            device_id={"sp": following if direction == 0 else preceding},
        )

    def ring_arrival(direction, step, q):
        offset = -(step + 1) if direction == 0 else step + 1
        dst = weights.at[rows_of(chip_at(offset), core, q)]
        pltpu.make_async_remote_copy(
            src_ref=dst,
            dst_ref=dst,
            send_sem=ring_send.at[direction, step, q],
            recv_sem=ring_recv.at[direction, step, q],
            device_id={"sp": following if direction == 0 else preceding},
        ).wait_recv()

    for own in owns:
        own.wait()
    for q in range(PIECES):
        mine = weights.at[rows_of(me // 2, core, q)]
        for direction in range(2):
            if q in pieces_of(direction, 0):
                copy = ring_copy(direction, 0, q, mine)
                copy.start()
                sends.append(copy)
        to_core(0, q, mine)
    tokens_at = pl.ds(pl.multiple_of(tp * features, 128), features)
    for turn in range(1, n_tp):
        copy = pltpu.make_async_remote_copy(
            src_ref=tok_ref,
            dst_ref=wide.at[:, tokens_at],
            send_sem=tok_send.at[turn - 1],
            recv_sem=tok_recv.at[turn - 1],
            device_id={"tp": (tp + turn) % n_tp},
        )
        copy.start()
        sends.append(copy)
    acc[...] = jnp.zeros_like(acc)
    wide[:, tokens_at] = tok_ref[...]
    for turn in range(1, n_tp):
        theirs = pl.ds(
            pl.multiple_of((tp - turn + n_tp) % n_tp * features, 128), features
        )
        pltpu.make_async_remote_copy(
            src_ref=tok_ref,
            dst_ref=wide.at[:, theirs],
            send_sem=tok_send.at[turn - 1],
            recv_sem=tok_recv.at[turn - 1],
            device_id={"tp": (tp + turn) % n_tp},
        ).wait_recv()
    scaled[...] = (wide[...].astype(jnp.float32) * gain_ref[...]).astype(jnp.bfloat16)

    cols = weights.shape[1]
    tile = cols // 6

    by_chip = (2 * rows) % 128 == 0

    def multiply(offset):
        if not by_chip:
            return
        multiply_rows(pl.ds(pl.multiple_of(chip_at(offset) * 2 * rows, 2 * rows), 2 * rows))

    def multiply_rows(depth):
        def one(i, _):
            at = pl.ds(pl.multiple_of(i * tile, 128), tile)
            acc[:, at] += jnp.dot(
                scaled[:, depth], weights[depth, at], preferred_element_type=jnp.float32
            )
            return 0

        lax.fori_loop(0, 6, one, 0)

    for step in range(steps):
        for q in range(PIECES):
            for direction in range(2):
                if q not in pieces_of(direction, step):
                    continue
                offset = -(step + 1) if direction == 0 else step + 1
                ring_arrival(direction, step, q)
                if step + 1 < steps and q in pieces_of(direction, step + 1):
                    copy = ring_copy(direction, step + 1, q, None)
                    copy.start()
                    sends.append(copy)
                last = offset if abs(offset) < steps else steps
                dst = weights.at[rows_of(chip_at(last), core, q)]
                to_core(last, q, dst)
        for offset in [0] if step == 0 else [-step, step]:
            for q in range(PIECES):
                from_core(offset, q)
            multiply(offset)
    for q in range(PIECES):
        from_core(steps, q)
    multiply(steps)
    if not by_chip:
        multiply_rows(slice(None))
    values = wide[...].astype(jnp.float32)
    squares = jnp.sum(values * values, axis=1, keepdims=True)
    inv_rms = lax.rsqrt(squares / wide.shape[1] + eps)
    proj_ref[...] = (acc[...] * inv_rms).astype(jnp.bfloat16)
    for copy in sends:
        copy.wait_send()


def project(tokens, gain, shards):
    n = lax.axis_size("sp")
    n_tp = lax.axis_size("tp")
    positions, features = tokens.shape
    rows = shards[0].shape[0]
    cols = sum(shard.shape[1] for shard in shards)
    width = n * rows
    steps = n // 4
    dma = pltpu.SemaphoreType.DMA
    return pl.pallas_call(
        functools.partial(project_kernel, n, n_tp),
        out_shape=jax.ShapeDtypeStruct((positions, cols), jnp.bfloat16),
        in_specs=[pl.BlockSpec(memory_space=pltpu.VMEM)] * 2
        + [pl.BlockSpec(memory_space=pl.ANY)] * 6,
        out_specs=pl.BlockSpec(memory_space=pltpu.VMEM),
        scratch_shapes=[
            pltpu.VMEM((positions, width), jnp.bfloat16),
            pltpu.VMEM((positions, width), jnp.bfloat16),
            pltpu.VMEM((width, cols), jnp.bfloat16),
            pltpu.VMEM((positions, cols), jnp.float32),
            dma((n_tp,)),
            dma((n_tp,)),
            dma((6,)),
            dma((2, steps, PIECES)),
            dma((2, steps, PIECES)),
            dma((2 * steps, PIECES)),
            dma((2 * steps, PIECES)),
        ],
        compiler_params=pltpu.CompilerParams(
            collective_id=0, has_side_effects=True, vmem_limit_bytes=56 * 1024 * 1024
        ),
        cost_estimate=pl.CostEstimate(
            flops=2 * positions * width * cols, bytes_accessed=4 * rows * cols, transcendentals=0
        ),
    )(tokens, gain[None, :], *shards)


def mix_kernel(
    n,
    n_tp,
    proj_ref,
    keep_ref,
    extra_ref,
    sgain_ref,
    mix_ref,
    pgain_ref,
    w_ref,
    post_ref,
    out_ref,
    weights,
    local,
    reach,
    both,
    state,
    before,
    gone_state,
    gone_decay,
    come_state,
    come_decay,
    tail,
    tail_in,
    mine,
    gone_out,
    come_out,
    ring_send,
    ring_recv,
    core_send,
    core_recv,
    scan_send,
    scan_recv,
    tail_sem,
    own_sem,
    out_send,
    out_recv,
):
    f32, bf16 = jnp.float32, jnp.bfloat16
    chips = n // 2
    steps = chips // 2
    rounds = (n - 1).bit_length()
    me = lax.axis_index("sp")
    tp = lax.axis_index("tp")
    core = me % 2
    place = ring_place(me // 2, chips)

    def chip_at(offset):
        return ring_chip((place + offset + chips) % chips, chips)

    following = 2 * chip_at(1) + core
    preceding = 2 * chip_at(-1) + core
    partner = 2 * (me // 2) + 1 - core
    piece = w_ref.shape[0] // PIECES

    barrier = pltpu.get_barrier_semaphore()
    for peer in (following, preceding, partner):
        pl.semaphore_signal(barrier, inc=1, device_id={"sp": peer})
    for r in range(rounds):
        pl.semaphore_signal(barrier, inc=1, device_id={"sp": (me + 2**r) % n})
        pl.semaphore_signal(barrier, inc=1, device_id={"sp": (me - 2**r + n) % n})
    for turn in range(1, n_tp):
        pl.semaphore_signal(barrier, inc=1, device_id={"tp": (tp + turn) % n_tp})
    pl.semaphore_wait(barrier, 3 + 2 * rounds + n_tp - 1)

    sends = []

    def spot(chip, which, q):
        return weights.at[2 * chip + which, pl.ds(q * piece, piece)]

    def to_core(offset, q, source):
        slot = offset + steps - 1
        copy = pltpu.make_async_remote_copy(
            src_ref=source,
            dst_ref=spot(chip_at(offset), core, q),
            send_sem=core_send.at[slot, q],
            recv_sem=core_recv.at[slot, q],
            device_id={"sp": partner},
        )
        copy.start()
        sends.append(copy)

    def from_core(offset, q):
        slot = offset + steps - 1
        dst = spot(chip_at(offset), 1 - core, q)
        pltpu.make_async_remote_copy(
            src_ref=dst,
            dst_ref=dst,
            send_sem=core_send.at[slot, q],
            recv_sem=core_recv.at[slot, q],
            device_id={"sp": partner},
        ).wait_recv()

    def pieces_of(direction, step):
        if step < steps - 1:
            return range(PIECES)
        half = PIECES // 2
        return range(half) if direction == 0 else range(half, PIECES)

    def ring_copy(direction, step, q, source, offset):
        dst = spot(chip_at(offset), core, q)
        return pltpu.make_async_remote_copy(
            src_ref=dst if source is None else source,
            dst_ref=dst,
            send_sem=ring_send.at[direction, step, q],
            recv_sem=ring_recv.at[direction, step, q],
            device_id={"sp": following if direction == 0 else preceding},
        )

    def ring_step(step):
        for q in range(PIECES):
            for direction in range(2):
                if q not in pieces_of(direction, step):
                    continue
                offset = -(step + 1) if direction == 0 else step + 1
                ring_copy(direction, step, q, None, offset).wait_recv()
                if step + 1 < steps and q in pieces_of(direction, step + 1):
                    copy = ring_copy(direction, step + 1, q, None, offset)
                    copy.start()
                    sends.append(copy)
                last = offset if abs(offset) < steps else steps
                to_core(last, q, spot(chip_at(last), core, q))

    pending = list(range(steps))

    def advance_ring():
        if pending:
            ring_step(pending.pop(0))

    positions = proj_ref.shape[0]
    head_cols = proj_ref.shape[1] // 6
    heads = head_cols // DK
    reach_back = tail.shape[0]

    tail[...] = proj_ref[positions - reach_back :, 4 * head_cols : 5 * head_cols]
    for q in range(PIECES):
        own_piece = w_ref.at[pl.ds(q * piece, piece)]
        for direction in range(2):
            if q in pieces_of(direction, 0):
                copy = ring_copy(direction, 0, q, own_piece, 0)
                copy.start()
                sends.append(copy)
        to_core(0, q, own_piece)
    own = pltpu.make_async_copy(w_ref, weights.at[me], own_sem)
    own.start()
    tail_copy = pltpu.make_async_remote_copy(
        src_ref=tail,
        dst_ref=tail_in,
        send_sem=tail_sem.at[0],
        recv_sem=tail_sem.at[1],
        device_id={"sp": (me + 1) % n},
    )
    tail_copy.start()

    row = lax.broadcasted_iota(jnp.int32, (positions, positions), 0)
    col = lax.broadcasted_iota(jnp.int32, (positions, positions), 1)
    lower = jnp.where(row >= col, 1.0, 0.0).astype(f32)
    line = lax.broadcasted_iota(jnp.int32, (positions, DK), 0)
    units = positions // 8
    sub = lax.broadcasted_iota(jnp.int32, (units, 8, DK), 1)
    over_last = (((1,), (1,)), ((), ()))

    decay_now = []
    for h in range(heads):
        at = slice(h * DK, (h + 1) * DK)
        part = lambda i: proj_ref[:, i * head_cols + h * DK : i * head_cols + (h + 1) * DK]
        q = part(0).astype(f32) * DK ** (-0.5)
        kg = keep_ref[:, at] * jax.nn.sigmoid(-part(1).astype(f32))
        v = part(2)
        logs = jnp.log1p(-kg) + extra_ref[:, h : h + 1]
        c = jnp.dot(
            lower, logs, precision=coarsest_scale_depth, preferred_element_type=f32
        )
        last = c[positions - 1 :, :]
        state[h] = lax.dot_general(
            v,
            (kg * jnp.exp(last - c)).astype(bf16),
            (((0,), (0,)), ((), ())),
            preferred_element_type=f32,
        )
        gone_decay[0, h : h + 1, :] = jnp.exp(last)
        reach[:, at] = (q * jnp.exp(c)).astype(bf16)
        scores = jnp.zeros((positions, positions), f32)
        span = 8
        while span < positions:
            pair = 2 * span
            c3 = c.reshape(positions // pair, pair, DK)
            middle = jnp.broadcast_to(c3[:, span - 1 : span, :], c3.shape).reshape(c.shape)
            fade = jnp.exp(-jnp.abs(c - middle))
            later = (line // span) % 2 == 1
            probe = jnp.where(later, q * fade, 0.0).astype(bf16)
            keyed = jnp.where(later, 0.0, kg * fade).astype(bf16)
            found = lax.dot_general(probe, keyed, over_last, preferred_element_type=f32)
            scores = scores + jnp.where(row // pair == col // pair, found, 0.0)
            span = pair
        result = jnp.dot(scores.astype(bf16), v, preferred_element_type=f32)
        c3 = c.reshape(units, 8, DK)
        q3 = q.reshape(units, 8, DK)
        k3 = kg.reshape(units, 8, DK)
        v3 = v.astype(f32).reshape(units, 8, DK)
        near = result.reshape(units, 8, DK)
        for s in range(8):
            weight = jnp.exp(jnp.minimum(c3 - c3[:, s : s + 1, :], 0.0))
            score = jnp.sum(q3 * k3[:, s : s + 1, :] * weight, axis=2, keepdims=True)
            near = near + jnp.where(sub >= s, score * v3[:, s : s + 1, :], 0.0)
        local[:, at] = near.reshape(positions, DK)
        if h % 2 == 1:
            advance_ring()

    def scan_copies(r):
        target = {"sp": (me + 2**r) % n}
        return [
            pltpu.make_async_remote_copy(
                src_ref=gone.at[r],
                dst_ref=come.at[r],
                send_sem=scan_send.at[r, i],
                recv_sem=scan_recv.at[r, i],
                device_id=target,
            )
            for i, (gone, come) in enumerate(
                [(gone_state, come_state), (gone_decay, come_decay)]
            )
        ]

    before[...] = jnp.zeros_like(before)
    decay_w = [gone_decay[0, h : h + 1, :] for h in range(heads)]
    decay_e = [jnp.ones((1, DK), f32) for h in range(heads)]

    def pool(h):
        at = slice(h * DK, (h + 1) * DK)
        x = proj_ref[:, 4 * head_cols + h * DK : 4 * head_cols + (h + 1) * DK].astype(f32)
        prior = jnp.where(me > 0, tail_in[:, at].astype(f32), 0.0)
        level = (tp * heads + h) % 4
        total = jnp.concatenate([prior, x], axis=0)
        chosen = jnp.zeros((positions, DK), f32)
        for k in range(4):
            total = total + pltpu.roll(total, 2**k, 0)
            chosen = jnp.where(level == k, total[reach_back:, :], chosen)
        window = 2
        for k in range(1, 4):
            window = jnp.where(level == k, 2 ** (1 + k), window)
        count = jnp.minimum(me * positions + line + 1, window).astype(f32)
        mixed = (chosen / count - x).astype(bf16)
        mapped = jnp.dot(mixed, mix_ref[h], preferred_element_type=f32)
        gate = proj_ref[:, 5 * head_cols + h * DK : 5 * head_cols + (h + 1) * DK].astype(f32)
        both[:, head_cols + h * DK : head_cols + (h + 1) * DK] = (
            mapped * pgain_ref[:, at] * (gate * jax.nn.sigmoid(gate))
        ).astype(bf16)

    pools = list(range(heads))
    for r in range(rounds):
        gone_state[r] = state[...].astype(bf16)
        if r > 0:
            for h in range(heads):
                gone_decay[r, h : h + 1, :] = decay_w[h]
        for copy in scan_copies(r):
            copy.start()
            sends.append(copy)
        if r == 0:
            tail_copy.wait_recv()
        if pools:
            pool(pools.pop(0))
        advance_ring()
        for copy in scan_copies(r):
            copy.wait_recv()
        valid = me >= 2**r
        for h in range(heads):
            came = jnp.where(valid, come_state[r, h].astype(f32), 0.0)
            came_decay = jnp.where(valid, come_decay[r, h : h + 1, :], 1.0)
            before[h] = before[h] + decay_e[h] * came
            decay_e[h] = decay_e[h] * came_decay
            if r + 1 < rounds:
                state[h] = state[h] + decay_w[h] * came
                decay_w[h] = decay_w[h] * came_decay
    for h in pools:
        pool(h)
    while pending:
        advance_ring()

    for h in range(heads):
        at = slice(h * DK, (h + 1) * DK)
        rec = local[:, at] + lax.dot_general(
            reach[:, at], before[h].astype(bf16), over_last, preferred_element_type=f32
        )
        normed = rec * lax.rsqrt(jnp.mean(rec * rec, axis=1, keepdims=True) + eps)
        gate = proj_ref[:, 3 * head_cols + h * DK : 3 * head_cols + (h + 1) * DK].astype(f32)
        both[:, at] = (normed * sgain_ref[:, at] * (gate * jax.nn.sigmoid(gate))).astype(bf16)

    own.wait()
    for offset in range(-(steps - 1), steps + 1):
        for q in range(PIECES):
            from_core(offset, q)

    owned = positions // n_tp
    width = w_ref.shape[1]
    quarter = n // 4

    def share(rows, group):
        left = both[rows, :]
        for slot in range(group * quarter, (group + 1) * quarter, 2):
            right = jnp.concatenate([weights[slot], weights[slot + 1]], axis=1)
            yield slot, jnp.dot(left, right, preferred_element_type=f32).astype(bf16)

    def out_copy(turn, group):
        cols = pl.ds(group * quarter * width, quarter * width)
        return pltpu.make_async_remote_copy(
            src_ref=gone_out.at[turn - 1, :, cols],
            dst_ref=come_out.at[turn - 1, :, cols],
            send_sem=out_send.at[turn - 1, group],
            recv_sem=out_recv.at[turn - 1, group],
            device_id={"tp": (tp + turn) % n_tp},
        )

    for turn in range(1, n_tp):
        target = (tp + turn) % n_tp
        rows = pl.ds(pl.multiple_of(target * owned, owned), owned)
        for group in range(4):
            for slot, value in share(rows, group):
                gone_out[turn - 1, :, slot * width : (slot + 2) * width] = value
            copy = out_copy(turn, group)
            copy.start()
            sends.append(copy)
    rows = pl.ds(pl.multiple_of(tp * owned, owned), owned)
    for group in range(4):
        for slot, value in share(rows, group):
            mine[:, slot * width : (slot + 2) * width] = value.astype(f32)
    for turn in range(1, n_tp):
        for group in range(4):
            out_copy(turn, group).wait_recv()
        mine[...] += come_out[turn - 1].astype(f32)
    summed = mine[...]
    out_ref[...] = (
        summed
        * lax.rsqrt(jnp.mean(summed * summed, axis=1, keepdims=True) + eps)
        * post_ref[...]
    ).astype(bf16)
    tail_copy.wait_send()
    for copy in sends:
        copy.wait_send()


def mix(proj, keep, extra, sgain, pool_mix, pgain, shard, post):
    n = lax.axis_size("sp")
    n_tp = lax.axis_size("tp")
    positions, heads = extra.shape
    head_cols = heads * DK
    depth, width = shard.shape
    steps = n // 4
    rounds = (n - 1).bit_length()
    owned = positions // n_tp
    model = n * width
    padded = -(-heads // 8) * 8
    f32, bf16, dma = jnp.float32, jnp.bfloat16, pltpu.SemaphoreType.DMA
    return pl.pallas_call(
        functools.partial(mix_kernel, n, n_tp),
        out_shape=jax.ShapeDtypeStruct((owned, model), bf16),
        in_specs=[pl.BlockSpec(memory_space=pltpu.VMEM)] * 8,
        out_specs=pl.BlockSpec(memory_space=pltpu.VMEM),
        scratch_shapes=[
            pltpu.VMEM((n, depth, width), bf16),
            pltpu.VMEM((positions, head_cols), f32),
            pltpu.VMEM((positions, head_cols), bf16),
            pltpu.VMEM((positions, 2 * head_cols), bf16),
            pltpu.VMEM((heads, DK, DK), f32),
            pltpu.VMEM((heads, DK, DK), f32),
            pltpu.VMEM((rounds, heads, DK, DK), bf16),
            pltpu.VMEM((rounds, padded, DK), f32),
            pltpu.VMEM((rounds, heads, DK, DK), bf16),
            pltpu.VMEM((rounds, padded, DK), f32),
            pltpu.VMEM((16, head_cols), bf16),
            pltpu.VMEM((16, head_cols), bf16),
            pltpu.VMEM((owned, model), f32),
            pltpu.VMEM((n_tp, owned, model), bf16),
            pltpu.VMEM((n_tp, owned, model), bf16),
            dma((2, steps, PIECES)),
            dma((2, steps, PIECES)),
            dma((2 * steps, PIECES)),
            dma((2 * steps, PIECES)),
            dma((rounds, 2)),
            dma((rounds, 2)),
            dma((2,)),
            dma,
            dma((n_tp, 4)),
            dma((n_tp, 4)),
        ],
        compiler_params=pltpu.CompilerParams(
            collective_id=1, has_side_effects=True, vmem_limit_bytes=56 * 1024 * 1024
        ),
        cost_estimate=pl.CostEstimate(
            flops=2 * positions * depth * model, bytes_accessed=4 * depth * width, transcendentals=0
        ),
    )(proj, keep, extra, sgain, pool_mix, pgain, shard, post)


def pair_kernel(
    tok_hbm,
    gain_ref,
    w0,
    w1,
    w2,
    w3,
    w4,
    w5,
    rate_ref,
    extra_hbm,
    sgain_ref,
    mix_hbm,
    pgain_ref,
    orec_hbm,
    opool_hbm,
    post_ref,
    out_ref,
    wide,
    scaled,
    inv_rms,
    w_own,
    w_all,
    o_all,
    extra,
    mix_own,
    proj,
    local,
    reach,
    state,
    state_go,
    state_come,
    decay_go,
    decay_come,
    tail_go,
    tail_come,
    total_go,
    total_come,
    last_go,
    last_come,
    y_all,
    y_go,
    part_go,
    part_come,
    mine,
    own_sem,
    tok_send,
    tok_recv,
    extra_send,
    extra_recv,
    w_send,
    w_recv,
    wy_send,
    wy_recv,
    o_send,
    o_recv,
    oy_send,
    oy_recv,
    scan_send,
    scan_recv,
    y_send,
    y_recv,
    part_send,
    part_recv,
):
    f32, bf16 = jnp.float32, jnp.bfloat16
    me = lax.axis_index("sp")
    x = lax.axis_index("tp")
    z, y, c = me // 4, (me // 2) % 2, me % 2
    odd = z % 2
    pair = z // 2
    head = odd * 2 + c
    slabs = [z, z + 1 - 2 * odd, (z + 2) % 4, 3 - z]
    rows, feats = tok_hbm.shape
    shard = w0.shape[0]
    parts = (w0, w1, w2, w3, w4, w5)
    units = len(parts)
    positions = wide.shape[0]
    half = positions // 2
    block = rows
    blocks = positions // block
    piece = rows // 2

    def peer(zz, yy, cc):
        return {"sp": zz * 4 + yy * 2 + cc}

    def peer_x(cc):
        return {"sp": z * 4 + y * 2 + cc, "tp": 1 - x}

    other_c = peer(z, y, 1 - c)
    other_y = peer(z, 1 - y, c)

    def lanes(i, n=1):
        return pl.ds(pl.multiple_of(i * DK, DK), n * DK)

    def own_rows(base, size):
        return pl.ds(pl.multiple_of(base, 16), size)

    def tok_at(zq, cc, xx, q):
        start = zq * half + cc * rows + q * piece
        return wide.at[own_rows(start, piece), pl.ds(pl.multiple_of(xx * feats, 128), feats)]

    owns = {}

    def own_copy(name, src, dst):
        copy = pltpu.make_async_copy(src, dst, own_sem.at[len(owns)])
        copy.start()
        owns[name] = copy

    for q in range(2):
        own_copy(("tok", q), tok_hbm.at[pl.ds(q * piece, piece)], tok_at(odd, c, x, q))
    for u, part in enumerate(parts):
        own_copy(("w", u), part, w_own.at[u])
    own_copy("extra", extra_hbm, extra.at[odd * 2 + c])
    here = z * 2 + y
    own_copy(("o", 0), orec_hbm, o_all.at[here, pl.ds(0, 4 * DK)])
    own_copy(("o", 1), opool_hbm, o_all.at[here, pl.ds(4 * DK, 4 * DK)])
    own_copy("mix", mix_hbm.at[head], mix_own)

    barrier = pltpu.get_barrier_semaphore()
    peers = [other_c, other_y, peer_x(c), peer_x(1 - c)]
    for k in range(1, 4):
        peers += [peer(slabs[k], y, c), peer(slabs[k], y, 1 - c)]
    for to in peers:
        pl.semaphore_signal(barrier, inc=1, device_id=to)
    pl.semaphore_wait(barrier, len(peers))

    sends = []

    def send(src, dst, send_sem, recv_sem, to):
        copy = pltpu.make_async_remote_copy(
            src_ref=src, dst_ref=dst, send_sem=send_sem, recv_sem=recv_sem, device_id=to
        )
        copy.start()
        sends.append(copy)

    def arrive(dst, send_sem, recv_sem, to):
        pltpu.make_async_remote_copy(
            src_ref=dst, dst_ref=dst, send_sem=send_sem, recv_sem=recv_sem, device_id=to
        ).wait_recv()

    def tok_send_to(kind, q, zq, cc, xx, to):
        at = tok_at(zq, cc, xx, q)
        send(at, at, tok_send.at[kind, q], tok_recv.at[kind, q], to)

    def tok_arrive(kind, q, zq, cc, xx):
        at = tok_at(zq, cc, xx, q)
        arrive(at, tok_send.at[kind, q], tok_recv.at[kind, q], other_c)

    for q in range(2):
        owns[("tok", q)].wait()
        tok_send_to(0, q, odd, c, x, peer(slabs[1], y, c))
        tok_send_to(1, q, odd, c, x, peer_x(c))
        tok_send_to(3, q, odd, c, x, other_c)

    def w_piece(slab, cc, n=1):
        return own_rows((slab * 4 + y * 2 + cc) * shard, n * shard)

    w_locals = []
    for u in range(units):
        owns[("w", u)].wait()
        keep_here = pltpu.make_async_copy(
            w_own.at[u, :, lanes(head)], w_all.at[u, w_piece(z, c)], own_sem.at[len(owns) + u]
        )
        keep_here.start()
        w_locals.append(keep_here)
        send(
            w_own.at[u, :, lanes(odd * 2 + 1 - c)],
            w_all.at[u, w_piece(z, c)],
            w_send.at[u, 0, 1],
            w_recv.at[u, 0, 1],
            other_c,
        )
        for k in (1, 2, 3):
            for e in range(2):
                cc = c if e == 0 else 1 - c
                to_head = (slabs[k] % 2) * 2 + cc
                send(
                    w_own.at[u, :, lanes(to_head)],
                    w_all.at[u, w_piece(z, c)],
                    w_send.at[u, k, e],
                    w_recv.at[u, k, e],
                    peer(slabs[k], y, cc),
                )
    owns["extra"].wait()
    for e, to in enumerate([other_c, peer(slabs[1], y, c), peer(slabs[1], y, 1 - c)]):
        at = extra.at[odd * 2 + c]
        send(at, at, extra_send.at[e], extra_recv.at[e], to)

    def w_relay(u, k):
        if k == 0:
            w_locals[u].wait()
        else:
            arrive(
                w_all.at[u, w_piece(slabs[k], c)], w_send.at[u, k, 0], w_recv.at[u, k, 0], other_c
            )
        arrive(
            w_all.at[u, w_piece(slabs[k], 1 - c)], w_send.at[u, k, 1], w_recv.at[u, k, 1], other_c
        )
        at = w_all.at[u, w_piece(slabs[k], 0, 2)]
        send(at, at, wy_send.at[u, k], wy_recv.at[u, k], other_y)

    def w_need(u):
        for k in range(4):
            start = (slabs[k] * 4 + (1 - y) * 2) * shard
            at = w_all.at[u, own_rows(start, 2 * shard)]
            arrive(at, wy_send.at[u, k], wy_recv.at[u, k], other_y)

    def o_at(slab, yy, part):
        return o_all.at[slab * 2 + yy, pl.ds(part * 4 * DK, 4 * DK)]

    def o_out(part):
        for k in (1, 2, 3):
            at = o_at(z, y, part)
            send(at, at, o_send.at[k, part], o_recv.at[k, part], peer(slabs[k], y, c))

    def o_relay(k, part):
        at = o_at(slabs[k], y, part)
        if k > 0:
            arrive(at, o_send.at[k, part], o_recv.at[k, part], other_c)
        send(at, at, oy_send.at[k, part], oy_recv.at[k, part], other_y)

    def o_need(k):
        for part in range(2):
            at = o_at(slabs[k], 1 - y, part)
            arrive(at, oy_send.at[k, part], oy_recv.at[k, part], other_y)

    for u in range(units):
        w_relay(u, 0)
    for part in range(2):
        owns[("o", part)].wait()
    o_out(0)

    def tok_z(q):
        tok_arrive(0, q, 1 - odd, c, x)
        tok_send_to(2, q, 1 - odd, c, x, peer_x(c))
        tok_send_to(4, q, 1 - odd, c, x, other_c)

    def tok_x(q):
        tok_arrive(1, q, odd, c, 1 - x)
        tok_send_to(5, q, odd, c, 1 - x, other_c)

    def tok_diagonal(q):
        tok_arrive(2, q, 1 - odd, c, 1 - x)
        tok_send_to(6, q, 1 - odd, c, 1 - x, other_c)

    def scale(zq, cc):
        at = own_rows(zq * half + cc * rows, rows)
        values = wide[at, :].astype(f32)
        scaled[at, :] = (values * gain_ref[...]).astype(bf16)
        squares = jnp.sum(values * values, axis=1, keepdims=True)
        inv_rms[at, :] = jnp.broadcast_to(
            lax.rsqrt(squares / wide.shape[1] + eps), (rows, DK)
        )

    todo = []

    def plan(tag, fn, *args):
        todo.append((tag, lambda: fn(*args)))

    def pump(count=1):
        for _ in range(count):
            if todo:
                todo.pop(0)[1]()

    def upto(tag):
        while any(t == tag for t, _ in todo):
            pump()

    plan("t", tok_z, 0)
    plan("w0", w_relay, 0, 2)
    plan("w0", w_relay, 0, 3)
    plan("t", tok_z, 1)
    plan("tx", tok_x, 0)
    plan("tx", tok_x, 1)
    plan("w0", w_relay, 0, 1)
    for k in (2, 3, 1):
        plan("w1", w_relay, 1, k)
    plan("td", tok_diagonal, 0)
    plan("w2", w_relay, 2, 2)
    plan("w2", w_relay, 2, 3)
    plan("td", tok_diagonal, 1)
    plan("w2", w_relay, 2, 1)
    for u in range(3, units):
        for k in (2, 3, 1):
            plan("w%d" % u, w_relay, u, k)
    for k in (2, 3, 1):
        plan("o", o_relay, k, 0)

    upto("tx")
    o_relay(0, 0)
    o_relay(0, 1)
    scale(odd, c)
    for q in range(2):
        tok_arrive(3, q, odd, 1 - c, x)
        tok_arrive(5, q, odd, 1 - c, 1 - x)
    scale(odd, 1 - c)
    upto("td")
    scale(1 - odd, c)
    for q in range(2):
        tok_arrive(4, q, 1 - odd, 1 - c, x)
        tok_arrive(6, q, 1 - odd, 1 - c, 1 - x)
    scale(1 - odd, 1 - c)

    def project_units(first, count):
        def one(i, _):
            at = own_rows(i * block, block)
            right = [w_all[u] for u in range(first, first + count)]
            right = right[0] if count == 1 else jnp.concatenate(right, axis=1)
            acc = jnp.dot(scaled[at, :], right, preferred_element_type=f32)
            norm = inv_rms[at, :]
            for j in range(count):
                proj[first + j, at, :] = (acc[:, j * DK : (j + 1) * DK] * norm).astype(bf16)
            return 0

        lax.fori_loop(0, blocks, one, 0)

    upto("w1")
    w_need(0)
    w_need(1)
    project_units(0, 2)
    for e, (zq, cc) in enumerate([(odd, 1 - c), (1 - odd, c), (1 - odd, 1 - c)]):
        arrive(extra.at[zq * 2 + cc], extra_send.at[e], extra_recv.at[e], other_c)
    upto("w2")
    w_need(2)
    project_units(2, 1)

    rate = rate_ref[:, lanes(head)]
    series = jnp.ones_like(rate)
    for n in range(10, 1, -1):
        series = 1.0 - series * rate / n
    keep = jnp.where(rate < 0.5, rate * series, 1.0 - jnp.exp(-rate))

    row = lax.broadcasted_iota(jnp.int32, (block, block), 0)
    col = lax.broadcasted_iota(jnp.int32, (block, block), 1)
    lower = jnp.where(row >= col, 1.0, 0.0).astype(f32)
    line = lax.broadcasted_iota(jnp.int32, (block, DK), 0)
    eighths = block // 8
    sub = lax.broadcasted_iota(jnp.int32, (eighths, 8, DK), 1)
    over_last = (((1,), (1,)), ((), ()))
    decays = []
    for b in range(blocks):
        at = slice(b * block, (b + 1) * block)
        q = proj[1, at, :].astype(f32) * DK ** (-0.5)
        kg = keep * jax.nn.sigmoid(-proj[0, at, :].astype(f32))
        v = proj[2, at, :]
        added = jnp.broadcast_to(extra[b, pl.ds(head, 1), :], (DK, block)).T
        logs = jnp.log1p(-kg) + added
        cum = jnp.dot(lower, logs, precision=coarsest_scale_depth, preferred_element_type=f32)
        last = cum[block - 1 :, :]
        state[b] = lax.dot_general(
            v,
            (kg * jnp.exp(last - cum)).astype(bf16),
            (((0,), (0,)), ((), ())),
            preferred_element_type=f32,
        )
        decays.append(jnp.exp(last))
        reach[at, :] = (q * jnp.exp(cum)).astype(bf16)
        scores = jnp.zeros((block, block), f32)
        span = 8
        while span < block:
            twice = 2 * span
            c3 = cum.reshape(block // twice, twice, DK)
            middle = jnp.broadcast_to(c3[:, span - 1 : span, :], c3.shape).reshape(cum.shape)
            fade = jnp.exp(-jnp.abs(cum - middle))
            later = (line // span) % 2 == 1
            probe = jnp.where(later, q * fade, 0.0).astype(bf16)
            keyed = jnp.where(later, 0.0, kg * fade).astype(bf16)
            found = lax.dot_general(probe, keyed, over_last, preferred_element_type=f32)
            scores = scores + jnp.where(row // twice == col // twice, found, 0.0)
            span = twice
        result = jnp.dot(scores.astype(bf16), v, preferred_element_type=f32)
        c3 = cum.reshape(eighths, 8, DK)
        q3 = q.reshape(eighths, 8, DK)
        k3 = kg.reshape(eighths, 8, DK)
        v3 = v.astype(f32).reshape(eighths, 8, DK)
        near = result.reshape(eighths, 8, DK)
        for s in range(8):
            weight = jnp.exp(jnp.minimum(c3 - c3[:, s : s + 1, :], 0.0))
            score = jnp.sum(q3 * k3[:, s : s + 1, :] * weight, axis=2, keepdims=True)
            near = near + jnp.where(sub >= s, score * v3[:, s : s + 1, :], 0.0)
        local[at, :] = near.reshape(block, DK)
        if b == 0:
            upto("w3")
        elif b == 1:
            pump(1)
        else:
            pump(1)

    sums = [decays[2 * i + 1] * state[2 * i] + state[2 * i + 1] for i in range(2)]
    fades = [decays[2 * i] * decays[2 * i + 1] for i in range(2)]
    for i in range(2):
        state_go[i] = sums[i].astype(bf16)
        decay_go[i : i + 1, :] = fades[i]
    send(state_go, state_come, scan_send.at[0], scan_recv.at[0], other_y)
    send(decay_go, decay_come, scan_send.at[1], scan_recv.at[1], other_y)
    w_need(3)
    project_units(3, 1)
    for i in range(2):
        tail_go[i] = proj[3, (i + 1) * half - 16 : (i + 1) * half, :]
    send(tail_go, tail_come, scan_send.at[2], scan_recv.at[2], other_y)
    upto("w4")

    arrive(state_come, scan_send.at[0], scan_recv.at[0], other_y)
    arrive(decay_come, scan_send.at[1], scan_recv.at[1], other_y)
    first_y = y == 0
    theirs = [state_come[i].astype(f32) for i in range(2)]
    their_fades = [decay_come[i : i + 1, :] for i in range(2)]
    order = []
    for i in range(2):
        order.append(
            (jnp.where(first_y, sums[i], theirs[i]), jnp.where(first_y, fades[i], their_fades[i]))
        )
        order.append(
            (jnp.where(first_y, theirs[i], sums[i]), jnp.where(first_y, their_fades[i], fades[i]))
        )
    total = order[0][0]
    for add, fade in order[1:]:
        total = fade * total + add
    total_go[...] = total.astype(bf16)
    arrive(tail_come, scan_send.at[2], scan_recv.at[2], other_y)
    last_go[...] = jnp.where(first_y, tail_come[1].astype(f32), tail_go[1].astype(f32)).astype(bf16)
    across = peer(slabs[2], y, c)
    send(total_go, total_come, scan_send.at[3], scan_recv.at[3], across)
    send(last_go, last_come, scan_send.at[4], scan_recv.at[4], across)

    upto("w5")
    w_need(4)
    w_need(5)
    project_units(4, 2)
    owns["mix"].wait()
    arrive(total_come, scan_send.at[3], scan_recv.at[3], across)
    arrive(last_come, scan_send.at[4], scan_recv.at[4], across)

    later_pair = pair > 0
    at_head = lanes(head)
    level = (x * 4 + head) % 4
    window = 2
    for k in range(1, 4):
        window = jnp.where(level == k, 2 ** (1 + k), window)
    line_half = lax.broadcasted_iota(jnp.int32, (half, DK), 0)
    far = [jnp.where(later_pair, last_come[...].astype(f32), 0.0), tail_come[0].astype(f32)]
    their_tails = [tail_come[i].astype(f32) for i in range(2)]
    befores = []
    running = jnp.where(later_pair, total_come[...].astype(f32), 0.0)
    for i in range(2):
        after_first = order[2 * i][1] * running + order[2 * i][0]
        befores.append(jnp.where(first_y, running, after_first))
        running = order[2 * i + 1][1] * after_first + order[2 * i + 1][0]

    def y_half(i):
        at = own_rows(i * half, half)
        at_static = slice(i * half, (i + 1) * half)
        xin = proj[3, at_static, :].astype(f32)
        prior = jnp.where(first_y, far[i], their_tails[i])
        sums_in = jnp.concatenate([prior, xin], axis=0)
        chosen = jnp.zeros((half, DK), f32)
        for k in range(4):
            sums_in = sums_in + pltpu.roll(sums_in, 2**k, 0)
            chosen = jnp.where(level == k, sums_in[16:, :], chosen)
        begins = (4 * pair + 2 * i + y) * half
        count = jnp.minimum(begins + line_half + 1, window).astype(f32)
        mixed = (chosen / count - xin).astype(bf16)
        mapped = jnp.dot(mixed, mix_own[...], preferred_element_type=f32)
        gate = proj[5, at_static, :].astype(f32)
        pooled = (mapped * pgain_ref[:, at_head] * (gate * jax.nn.sigmoid(gate))).astype(bf16)
        cur = befores[i]
        recs = []
        for j in range(2):
            b = 2 * i + j
            rows_b = slice(b * block, (b + 1) * block)
            rec = local[rows_b, :] + lax.dot_general(
                reach[rows_b, :], cur.astype(bf16), over_last, preferred_element_type=f32
            )
            cur = decays[b] * cur + state[b]
            normed = rec * lax.rsqrt(jnp.mean(rec * rec, axis=1, keepdims=True) + eps)
            gate = proj[4, rows_b, :].astype(f32)
            recs.append(
                (normed * sgain_ref[:, at_head] * (gate * jax.nn.sigmoid(gate))).astype(bf16)
            )
        return jnp.concatenate(recs, axis=0), pooled

    halves = [y_half(i) for i in range(2)]
    is_odd = odd == 1
    for part in range(2):
        low, high = halves[0][part].astype(f32), halves[1][part].astype(f32)
        y_go[part] = jnp.where(is_odd, low, high).astype(bf16)
        y_all[part * 4 + head] = jnp.where(is_odd, high, low).astype(bf16)
    z_peer = peer(slabs[1], y, c)
    their_head = (1 - odd) * 2 + c
    for part in range(2):
        send(
            y_go.at[part],
            y_all.at[part * 4 + head],
            y_send.at[0, part],
            y_recv.at[0, part],
            z_peer,
        )
        at = y_all.at[part * 4 + head]
        send(at, at, y_send.at[1, part], y_recv.at[1, part], other_c)
    o_out(1)
    upto("o")
    for part in range(2):
        at = y_all.at[part * 4 + their_head]
        arrive(at, y_send.at[0, part], y_recv.at[0, part], z_peer)
        send(at, at, y_send.at[2, part], y_recv.at[2, part], other_c)
    for part in range(2):
        at = y_all.at[part * 4 + odd * 2 + 1 - c]
        arrive(at, y_send.at[1, part], y_recv.at[1, part], other_c)
    for part in range(2):
        at = y_all.at[part * 4 + (1 - odd) * 2 + 1 - c]
        arrive(at, y_send.at[2, part], y_recv.at[2, part], other_c)

    owned = part_come.shape[2]
    part_peers = [(x, 1 - c, other_c), (1 - x, c, peer_x(c)), (1 - x, 1 - c, peer_x(1 - c))]

    def rows_for(xx, cc):
        return own_rows(cc * rows + xx * owned, owned)

    def out_chunk(k):
        if k > 0:
            o_relay(k, 1)
        o_need(k)
        left = jnp.concatenate([y_all[i] for i in range(8)], axis=1)
        right = jnp.concatenate([o_all[slabs[k] * 2], o_all[slabs[k] * 2 + 1]], axis=1)
        part_go[k] = jnp.dot(left, right, preferred_element_type=f32).astype(bf16)
        for i, (xx, cc, to) in enumerate(part_peers):
            send(
                part_go.at[k, rows_for(xx, cc)],
                part_come.at[k, i],
                part_send.at[k, i],
                part_recv.at[k, i],
                to,
            )

    def gather_chunk(k):
        for i, (xx, cc, to) in enumerate(part_peers):
            arrive(part_come.at[k, i], part_send.at[k, i], part_recv.at[k, i], to)
        ours = part_go[k, rows_for(x, c), :].astype(f32) + part_come[k, 1].astype(f32)
        others = part_come[k, 0].astype(f32) + part_come[k, 2].astype(f32)
        for yy in range(2):
            cols = slice(yy * DK, (yy + 1) * DK)
            mine[:, lanes(slabs[k] * 4 + yy * 2 + c)] = ours[:, cols]
            mine[:, lanes(slabs[k] * 4 + yy * 2 + 1 - c)] = others[:, cols]

    turns = (0, 2, 3, 1)
    for turn, k in enumerate(turns):
        out_chunk(k)
        if turn > 0:
            gather_chunk(turns[turn - 1])
    gather_chunk(turns[-1])
    summed = mine[...]
    out_ref[...] = (
        summed
        * lax.rsqrt(jnp.mean(summed * summed, axis=1, keepdims=True) + eps)
        * post_ref[...]
    ).astype(bf16)
    for copy in sends:
        copy.wait_send()


def pair_layer(
    tokens,
    gain,
    shards,
    rate,
    extra,
    sgain,
    pool_mix,
    pgain,
    out_rec,
    out_pool,
    post,
):
    n = lax.axis_size("sp")
    n_tp = lax.axis_size("tp")
    rows, feats = tokens.shape
    shard, cols = shards[0].shape
    heads = cols // DK
    depth, width = out_rec.shape
    slabs = n // 4
    positions = 4 * rows
    half = 2 * rows
    owned = rows // n_tp
    model = n * width
    f32, bf16, dma = jnp.float32, jnp.bfloat16, pltpu.SemaphoreType.DMA
    units = len(shards)
    vmem, hbm = pl.BlockSpec(memory_space=pltpu.VMEM), pl.BlockSpec(memory_space=pl.ANY)
    return pl.pallas_call(
        pair_kernel,
        out_shape=jax.ShapeDtypeStruct((owned, model), bf16),
        in_specs=[hbm, vmem] + [hbm] * 6 + [vmem, hbm, vmem, hbm, vmem, hbm, hbm, vmem],
        out_specs=vmem,
        scratch_shapes=[
            pltpu.VMEM((positions, n_tp * feats), bf16),
            pltpu.VMEM((positions, n_tp * feats), bf16),
            pltpu.VMEM((positions, DK), f32),
            pltpu.VMEM((units, shard, cols), bf16),
            pltpu.VMEM((units, n * shard, DK), bf16),
            pltpu.VMEM((2 * slabs, 2 * depth, width), bf16),
            pltpu.VMEM((4, heads, rows), f32),
            pltpu.VMEM((DK, DK), bf16),
            pltpu.VMEM((units, positions, DK), bf16),
            pltpu.VMEM((positions, DK), f32),
            pltpu.VMEM((positions, DK), bf16),
            pltpu.VMEM((4, DK, DK), f32),
            pltpu.VMEM((2, DK, DK), bf16),
            pltpu.VMEM((2, DK, DK), bf16),
            pltpu.VMEM((8, DK), f32),
            pltpu.VMEM((8, DK), f32),
            pltpu.VMEM((2, 16, DK), bf16),
            pltpu.VMEM((2, 16, DK), bf16),
            pltpu.VMEM((DK, DK), bf16),
            pltpu.VMEM((DK, DK), bf16),
            pltpu.VMEM((16, DK), bf16),
            pltpu.VMEM((16, DK), bf16),
            pltpu.VMEM((2 * heads, half, DK), bf16),
            pltpu.VMEM((2, half, DK), bf16),
            pltpu.VMEM((slabs, half, 2 * width), bf16),
            pltpu.VMEM((slabs, 3, owned, 2 * width), bf16),
            pltpu.VMEM((owned, model), f32),
            dma((2 * units + 6,)),
            dma((7, 2)),
            dma((7, 2)),
            dma((3,)),
            dma((3,)),
            dma((units, slabs, 2)),
            dma((units, slabs, 2)),
            dma((units, slabs)),
            dma((units, slabs)),
            dma((slabs, 2)),
            dma((slabs, 2)),
            dma((slabs, 2)),
            dma((slabs, 2)),
            dma((5,)),
            dma((5,)),
            dma((3, 2)),
            dma((3, 2)),
            dma((slabs, 3)),
            dma((slabs, 3)),
        ],
        compiler_params=pltpu.CompilerParams(
            collective_id=0, has_side_effects=True, vmem_limit_bytes=56 * 1024 * 1024
        ),
        cost_estimate=pl.CostEstimate(
            flops=2 * positions * n * shard * units * DK,
            bytes_accessed=4 * units * shard * cols,
            transcendentals=0,
        ),
    )(
        tokens,
        gain[None, :],
        *shards,
        rate[None, :],
        extra.T,
        sgain[None, :],
        pool_mix,
        pgain[None, :],
        out_rec,
        out_pool,
        post[None, :],
    )


def per_device(
    tokens_in,
    norm_gain,
    w_query,
    w_forget,
    w_input,
    w_rgate,
    w_pool_in,
    w_pgate,
    floor_rate,
    extra_logdecay,
    state_gain,
    pool_mix,
    pool_gain,
    out_rec,
    out_pool,
    post_gain,
):
    n, n_tp, heads = lax.axis_size("sp"), lax.axis_size("tp"), extra_logdecay.shape[1]
    if n == 16 and n_tp == 2 and heads == 4:
        return pair_layer(
            tokens_in,
            norm_gain,
            [w_forget, w_query, w_input, w_pool_in, w_rgate, w_pgate],
            floor_rate,
            extra_logdecay,
            state_gain,
            pool_mix,
            pool_gain,
            out_rec,
            out_pool,
            post_gain,
        )
    shards = [w_query, w_forget, w_input, w_rgate, w_pool_in, w_pgate]
    proj = project(tokens_in, norm_gain, shards)
    return mix(
        proj,
        -jnp.expm1(-floor_rate)[None, :],
        extra_logdecay,
        state_gain[None, :],
        pool_mix,
        pool_gain[None, :],
        jnp.concatenate([out_rec, out_pool], axis=0),
        post_gain[None, :],
    )


def solution(mesh):
    placed = (
        P("sp", "tp"),
        P(),
        P("sp", "tp"),
        P("sp", "tp"),
        P("sp", "tp"),
        P("sp", "tp"),
        P("sp", "tp"),
        P("sp", "tp"),
        P("tp"),
        P("sp", "tp"),
        P("tp"),
        P("tp", None, None),
        P("tp"),
        P("tp", "sp"),
        P("tp", "sp"),
        P(),
    )
    return jax.shard_map(
        per_device, mesh=mesh, in_specs=placed, out_specs=P(("sp", "tp"), None), check_vma=False
    )
```

```python
import functools

import jax
import jax.numpy as jnp
from jax import lax
from jax.experimental import pallas as pl
from jax.experimental.pallas import tpu as pltpu
from jax.sharding import PartitionSpec as P

DK = 128


eps = 1e-06
coarsest_scale_depth = lax.Precision.HIGHEST


PIECES = 4


def ring_place(chip, chips):
    odd = chip % 2
    return (1 - odd) * (chip // 2) + odd * (chips - 1 - chip // 2)


def ring_chip(place, chips):
    back = place // (chips // 2)
    return (1 - back) * (2 * place) + back * (2 * (chips - 1 - place) + 1)


def project_kernel(
    n,
    n_tp,
    tok_ref,
    gain_ref,
    w0,
    w1,
    w2,
    w3,
    w4,
    w5,
    proj_ref,
    wide,
    scaled,
    weights,
    acc,
    tok_send,
    tok_recv,
    own_sem,
    ring_send,
    ring_recv,
    core_send,
    core_recv,
):
    chips = n // 2
    steps = chips // 2
    me = lax.axis_index("sp")
    tp = lax.axis_index("tp")
    core = me % 2
    place = ring_place(me // 2, chips)

    def chip_at(offset):
        return ring_chip((place + offset + chips) % chips, chips)

    following = 2 * chip_at(1) + core
    preceding = 2 * chip_at(-1) + core
    partner = 2 * (me // 2) + 1 - core
    parts = (w0, w1, w2, w3, w4, w5)
    rows, part_cols = w0.shape
    my_rows = pl.ds(pl.multiple_of(me * rows, 16), rows)
    owns = []
    for i, part in enumerate(parts):
        block = weights.at[my_rows, pl.ds(i * part_cols, part_cols)]
        owns.append(pltpu.make_async_copy(part, block, own_sem.at[i]))
        owns[-1].start()
    piece = rows // PIECES
    features = tok_ref.shape[1]

    barrier = pltpu.get_barrier_semaphore()
    for peer in (following, preceding, partner):
        pl.semaphore_signal(barrier, inc=1, device_id={"sp": peer})
    for turn in range(1, n_tp):
        pl.semaphore_signal(barrier, inc=1, device_id={"tp": (tp + turn) % n_tp})
    pl.semaphore_wait(barrier, 3 + n_tp - 1)

    def rows_of(chip, which, q):
        start = (2 * chip + which) * rows + q * piece
        return pl.ds(pl.multiple_of(start, 8), piece)

    sends = []

    def to_core(offset, q, source):
        slot = offset + steps - 1
        copy = pltpu.make_async_remote_copy(
            src_ref=source,
            dst_ref=weights.at[rows_of(chip_at(offset), core, q)],
            send_sem=core_send.at[slot, q],
            recv_sem=core_recv.at[slot, q],
            device_id={"sp": partner},
        )
        copy.start()
        sends.append(copy)

    def from_core(offset, q):
        slot = offset + steps - 1
        dst = weights.at[rows_of(chip_at(offset), 1 - core, q)]
        pltpu.make_async_remote_copy(
            src_ref=dst,
            dst_ref=dst,
            send_sem=core_send.at[slot, q],
            recv_sem=core_recv.at[slot, q],
            device_id={"sp": partner},
        ).wait_recv()

    def pieces_of(direction, step):
        if step < steps - 1:
            return range(PIECES)
        half = PIECES // 2
        return range(half) if direction == 0 else range(half, PIECES)

    def ring_copy(direction, step, q, source):
        offset = -step if direction == 0 else step
        dst = weights.at[rows_of(chip_at(offset), core, q)]
        return pltpu.make_async_remote_copy(
            src_ref=dst if source is None else source,
            dst_ref=dst,
            send_sem=ring_send.at[direction, step, q],
            recv_sem=ring_recv.at[direction, step, q],
            device_id={"sp": following if direction == 0 else preceding},
        )

    def ring_arrival(direction, step, q):
        offset = -(step + 1) if direction == 0 else step + 1
        dst = weights.at[rows_of(chip_at(offset), core, q)]
        pltpu.make_async_remote_copy(
            src_ref=dst,
            dst_ref=dst,
            send_sem=ring_send.at[direction, step, q],
            recv_sem=ring_recv.at[direction, step, q],
            device_id={"sp": following if direction == 0 else preceding},
        ).wait_recv()

    for own in owns:
        own.wait()
    for q in range(PIECES):
        mine = weights.at[rows_of(me // 2, core, q)]
        for direction in range(2):
            if q in pieces_of(direction, 0):
                copy = ring_copy(direction, 0, q, mine)
                copy.start()
                sends.append(copy)
        to_core(0, q, mine)
    tokens_at = pl.ds(pl.multiple_of(tp * features, 128), features)
    for turn in range(1, n_tp):
        copy = pltpu.make_async_remote_copy(
            src_ref=tok_ref,
            dst_ref=wide.at[:, tokens_at],
            send_sem=tok_send.at[turn - 1],
            recv_sem=tok_recv.at[turn - 1],
            device_id={"tp": (tp + turn) % n_tp},
        )
        copy.start()
        sends.append(copy)
    acc[...] = jnp.zeros_like(acc)
    wide[:, tokens_at] = tok_ref[...]
    for turn in range(1, n_tp):
        theirs = pl.ds(
            pl.multiple_of((tp - turn + n_tp) % n_tp * features, 128), features
        )
        pltpu.make_async_remote_copy(
            src_ref=tok_ref,
            dst_ref=wide.at[:, theirs],
            send_sem=tok_send.at[turn - 1],
            recv_sem=tok_recv.at[turn - 1],
            device_id={"tp": (tp + turn) % n_tp},
        ).wait_recv()
    scaled[...] = (wide[...].astype(jnp.float32) * gain_ref[...]).astype(jnp.bfloat16)

    cols = weights.shape[1]
    tile = cols // 6

    by_chip = (2 * rows) % 128 == 0

    def multiply(offset):
        if not by_chip:
            return
        multiply_rows(pl.ds(pl.multiple_of(chip_at(offset) * 2 * rows, 2 * rows), 2 * rows))

    def multiply_rows(depth):
        def one(i, _):
            at = pl.ds(pl.multiple_of(i * tile, 128), tile)
            acc[:, at] += jnp.dot(
                scaled[:, depth], weights[depth, at], preferred_element_type=jnp.float32
            )
            return 0

        lax.fori_loop(0, 6, one, 0)

    for step in range(steps):
        for q in range(PIECES):
            for direction in range(2):
                if q not in pieces_of(direction, step):
                    continue
                offset = -(step + 1) if direction == 0 else step + 1
                ring_arrival(direction, step, q)
                if step + 1 < steps and q in pieces_of(direction, step + 1):
                    copy = ring_copy(direction, step + 1, q, None)
                    copy.start()
                    sends.append(copy)
                last = offset if abs(offset) < steps else steps
                dst = weights.at[rows_of(chip_at(last), core, q)]
                to_core(last, q, dst)
        for offset in [0] if step == 0 else [-step, step]:
            for q in range(PIECES):
                from_core(offset, q)
            multiply(offset)
    for q in range(PIECES):
        from_core(steps, q)
    multiply(steps)
    if not by_chip:
        multiply_rows(slice(None))
    values = wide[...].astype(jnp.float32)
    squares = jnp.sum(values * values, axis=1, keepdims=True)
    inv_rms = lax.rsqrt(squares / wide.shape[1] + eps)
    proj_ref[...] = (acc[...] * inv_rms).astype(jnp.bfloat16)
    for copy in sends:
        copy.wait_send()


def project(tokens, gain, shards):
    n = lax.axis_size("sp")
    n_tp = lax.axis_size("tp")
    positions, features = tokens.shape
    rows = shards[0].shape[0]
    cols = sum(shard.shape[1] for shard in shards)
    width = n * rows
    steps = n // 4
    dma = pltpu.SemaphoreType.DMA
    return pl.pallas_call(
        functools.partial(project_kernel, n, n_tp),
        out_shape=jax.ShapeDtypeStruct((positions, cols), jnp.bfloat16),
        in_specs=[pl.BlockSpec(memory_space=pltpu.VMEM)] * 2
        + [pl.BlockSpec(memory_space=pl.ANY)] * 6,
        out_specs=pl.BlockSpec(memory_space=pltpu.VMEM),
        scratch_shapes=[
            pltpu.VMEM((positions, width), jnp.bfloat16),
            pltpu.VMEM((positions, width), jnp.bfloat16),
            pltpu.VMEM((width, cols), jnp.bfloat16),
            pltpu.VMEM((positions, cols), jnp.float32),
            dma((n_tp,)),
            dma((n_tp,)),
            dma((6,)),
            dma((2, steps, PIECES)),
            dma((2, steps, PIECES)),
            dma((2 * steps, PIECES)),
            dma((2 * steps, PIECES)),
        ],
        compiler_params=pltpu.CompilerParams(
            collective_id=0, has_side_effects=True, vmem_limit_bytes=56 * 1024 * 1024
        ),
        cost_estimate=pl.CostEstimate(
            flops=2 * positions * width * cols, bytes_accessed=4 * rows * cols, transcendentals=0
        ),
    )(tokens, gain[None, :], *shards)


def mix_kernel(
    n,
    n_tp,
    proj_ref,
    keep_ref,
    extra_ref,
    sgain_ref,
    mix_ref,
    pgain_ref,
    w_ref,
    post_ref,
    out_ref,
    weights,
    local,
    reach,
    both,
    state,
    before,
    gone_state,
    gone_decay,
    come_state,
    come_decay,
    tail,
    tail_in,
    mine,
    gone_out,
    come_out,
    ring_send,
    ring_recv,
    core_send,
    core_recv,
    scan_send,
    scan_recv,
    tail_sem,
    own_sem,
    out_send,
    out_recv,
):
    f32, bf16 = jnp.float32, jnp.bfloat16
    chips = n // 2
    steps = chips // 2
    rounds = (n - 1).bit_length()
    me = lax.axis_index("sp")
    tp = lax.axis_index("tp")
    core = me % 2
    place = ring_place(me // 2, chips)

    def chip_at(offset):
        return ring_chip((place + offset + chips) % chips, chips)

    following = 2 * chip_at(1) + core
    preceding = 2 * chip_at(-1) + core
    partner = 2 * (me // 2) + 1 - core
    piece = w_ref.shape[0] // PIECES

    barrier = pltpu.get_barrier_semaphore()
    for peer in (following, preceding, partner):
        pl.semaphore_signal(barrier, inc=1, device_id={"sp": peer})
    for r in range(rounds):
        pl.semaphore_signal(barrier, inc=1, device_id={"sp": (me + 2**r) % n})
        pl.semaphore_signal(barrier, inc=1, device_id={"sp": (me - 2**r + n) % n})
    for turn in range(1, n_tp):
        pl.semaphore_signal(barrier, inc=1, device_id={"tp": (tp + turn) % n_tp})
    pl.semaphore_wait(barrier, 3 + 2 * rounds + n_tp - 1)

    sends = []

    def spot(chip, which, q):
        return weights.at[2 * chip + which, pl.ds(q * piece, piece)]

    def to_core(offset, q, source):
        slot = offset + steps - 1
        copy = pltpu.make_async_remote_copy(
            src_ref=source,
            dst_ref=spot(chip_at(offset), core, q),
            send_sem=core_send.at[slot, q],
            recv_sem=core_recv.at[slot, q],
            device_id={"sp": partner},
        )
        copy.start()
        sends.append(copy)

    def from_core(offset, q):
        slot = offset + steps - 1
        dst = spot(chip_at(offset), 1 - core, q)
        pltpu.make_async_remote_copy(
            src_ref=dst,
            dst_ref=dst,
            send_sem=core_send.at[slot, q],
            recv_sem=core_recv.at[slot, q],
            device_id={"sp": partner},
        ).wait_recv()

    def pieces_of(direction, step):
        if step < steps - 1:
            return range(PIECES)
        half = PIECES // 2
        return range(half) if direction == 0 else range(half, PIECES)

    def ring_copy(direction, step, q, source, offset):
        dst = spot(chip_at(offset), core, q)
        return pltpu.make_async_remote_copy(
            src_ref=dst if source is None else source,
            dst_ref=dst,
            send_sem=ring_send.at[direction, step, q],
            recv_sem=ring_recv.at[direction, step, q],
            device_id={"sp": following if direction == 0 else preceding},
        )

    def ring_step(step):
        for q in range(PIECES):
            for direction in range(2):
                if q not in pieces_of(direction, step):
                    continue
                offset = -(step + 1) if direction == 0 else step + 1
                ring_copy(direction, step, q, None, offset).wait_recv()
                if step + 1 < steps and q in pieces_of(direction, step + 1):
                    copy = ring_copy(direction, step + 1, q, None, offset)
                    copy.start()
                    sends.append(copy)
                last = offset if abs(offset) < steps else steps
                to_core(last, q, spot(chip_at(last), core, q))

    pending = list(range(steps))

    def advance_ring():
        if pending:
            ring_step(pending.pop(0))

    positions = proj_ref.shape[0]
    head_cols = proj_ref.shape[1] // 6
    heads = head_cols // DK
    reach_back = tail.shape[0]

    tail[...] = proj_ref[positions - reach_back :, 4 * head_cols : 5 * head_cols]
    for q in range(PIECES):
        own_piece = w_ref.at[pl.ds(q * piece, piece)]
        for direction in range(2):
            if q in pieces_of(direction, 0):
                copy = ring_copy(direction, 0, q, own_piece, 0)
                copy.start()
                sends.append(copy)
        to_core(0, q, own_piece)
    own = pltpu.make_async_copy(w_ref, weights.at[me], own_sem)
    own.start()
    tail_copy = pltpu.make_async_remote_copy(
        src_ref=tail,
        dst_ref=tail_in,
        send_sem=tail_sem.at[0],
        recv_sem=tail_sem.at[1],
        device_id={"sp": (me + 1) % n},
    )
    tail_copy.start()

    row = lax.broadcasted_iota(jnp.int32, (positions, positions), 0)
    col = lax.broadcasted_iota(jnp.int32, (positions, positions), 1)
    lower = jnp.where(row >= col, 1.0, 0.0).astype(f32)
    line = lax.broadcasted_iota(jnp.int32, (positions, DK), 0)
    units = positions // 8
    sub = lax.broadcasted_iota(jnp.int32, (units, 8, DK), 1)
    over_last = (((1,), (1,)), ((), ()))

    decay_now = []
    for h in range(heads):
        at = slice(h * DK, (h + 1) * DK)
        part = lambda i: proj_ref[:, i * head_cols + h * DK : i * head_cols + (h + 1) * DK]
        q = part(0).astype(f32) * DK ** (-0.5)
        kg = keep_ref[:, at] * jax.nn.sigmoid(-part(1).astype(f32))
        v = part(2)
        logs = jnp.log1p(-kg) + extra_ref[:, h : h + 1]
        c = jnp.dot(
            lower, logs, precision=coarsest_scale_depth, preferred_element_type=f32
        )
        last = c[positions - 1 :, :]
        state[h] = lax.dot_general(
            v,
            (kg * jnp.exp(last - c)).astype(bf16),
            (((0,), (0,)), ((), ())),
            preferred_element_type=f32,
        )
        gone_decay[0, h : h + 1, :] = jnp.exp(last)
        reach[:, at] = (q * jnp.exp(c)).astype(bf16)
        scores = jnp.zeros((positions, positions), f32)
        span = 8
        while span < positions:
            pair = 2 * span
            c3 = c.reshape(positions // pair, pair, DK)
            middle = jnp.broadcast_to(c3[:, span - 1 : span, :], c3.shape).reshape(c.shape)
            fade = jnp.exp(-jnp.abs(c - middle))
            later = (line // span) % 2 == 1
            probe = jnp.where(later, q * fade, 0.0).astype(bf16)
            keyed = jnp.where(later, 0.0, kg * fade).astype(bf16)
            found = lax.dot_general(probe, keyed, over_last, preferred_element_type=f32)
            scores = scores + jnp.where(row // pair == col // pair, found, 0.0)
            span = pair
        result = jnp.dot(scores.astype(bf16), v, preferred_element_type=f32)
        c3 = c.reshape(units, 8, DK)
        q3 = q.reshape(units, 8, DK)
        k3 = kg.reshape(units, 8, DK)
        v3 = v.astype(f32).reshape(units, 8, DK)
        near = result.reshape(units, 8, DK)
        for s in range(8):
            weight = jnp.exp(jnp.minimum(c3 - c3[:, s : s + 1, :], 0.0))
            score = jnp.sum(q3 * k3[:, s : s + 1, :] * weight, axis=2, keepdims=True)
            near = near + jnp.where(sub >= s, score * v3[:, s : s + 1, :], 0.0)
        local[:, at] = near.reshape(positions, DK)
        if h % 2 == 1:
            advance_ring()

    def scan_copies(r):
        target = {"sp": (me + 2**r) % n}
        return [
            pltpu.make_async_remote_copy(
                src_ref=gone.at[r],
                dst_ref=come.at[r],
                send_sem=scan_send.at[r, i],
                recv_sem=scan_recv.at[r, i],
                device_id=target,
            )
            for i, (gone, come) in enumerate(
                [(gone_state, come_state), (gone_decay, come_decay)]
            )
        ]

    before[...] = jnp.zeros_like(before)
    decay_w = [gone_decay[0, h : h + 1, :] for h in range(heads)]
    decay_e = [jnp.ones((1, DK), f32) for h in range(heads)]

    def pool(h):
        at = slice(h * DK, (h + 1) * DK)
        x = proj_ref[:, 4 * head_cols + h * DK : 4 * head_cols + (h + 1) * DK].astype(f32)
        prior = jnp.where(me > 0, tail_in[:, at].astype(f32), 0.0)
        level = (tp * heads + h) % 4
        total = jnp.concatenate([prior, x], axis=0)
        chosen = jnp.zeros((positions, DK), f32)
        for k in range(4):
            total = total + pltpu.roll(total, 2**k, 0)
            chosen = jnp.where(level == k, total[reach_back:, :], chosen)
        window = 2
        for k in range(1, 4):
            window = jnp.where(level == k, 2 ** (1 + k), window)
        count = jnp.minimum(me * positions + line + 1, window).astype(f32)
        mixed = (chosen / count - x).astype(bf16)
        mapped = jnp.dot(mixed, mix_ref[h], preferred_element_type=f32)
        gate = proj_ref[:, 5 * head_cols + h * DK : 5 * head_cols + (h + 1) * DK].astype(f32)
        both[:, head_cols + h * DK : head_cols + (h + 1) * DK] = (
            mapped * pgain_ref[:, at] * (gate * jax.nn.sigmoid(gate))
        ).astype(bf16)

    pools = list(range(heads))
    for r in range(rounds):
        gone_state[r] = state[...].astype(bf16)
        if r > 0:
            for h in range(heads):
                gone_decay[r, h : h + 1, :] = decay_w[h]
        for copy in scan_copies(r):
            copy.start()
            sends.append(copy)
        if r == 0:
            tail_copy.wait_recv()
        if pools:
            pool(pools.pop(0))
        advance_ring()
        for copy in scan_copies(r):
            copy.wait_recv()
        valid = me >= 2**r
        for h in range(heads):
            came = jnp.where(valid, come_state[r, h].astype(f32), 0.0)
            came_decay = jnp.where(valid, come_decay[r, h : h + 1, :], 1.0)
            before[h] = before[h] + decay_e[h] * came
            decay_e[h] = decay_e[h] * came_decay
            if r + 1 < rounds:
                state[h] = state[h] + decay_w[h] * came
                decay_w[h] = decay_w[h] * came_decay
    for h in pools:
        pool(h)
    while pending:
        advance_ring()

    for h in range(heads):
        at = slice(h * DK, (h + 1) * DK)
        rec = local[:, at] + lax.dot_general(
            reach[:, at], before[h].astype(bf16), over_last, preferred_element_type=f32
        )
        normed = rec * lax.rsqrt(jnp.mean(rec * rec, axis=1, keepdims=True) + eps)
        gate = proj_ref[:, 3 * head_cols + h * DK : 3 * head_cols + (h + 1) * DK].astype(f32)
        both[:, at] = (normed * sgain_ref[:, at] * (gate * jax.nn.sigmoid(gate))).astype(bf16)

    own.wait()
    for offset in range(-(steps - 1), steps + 1):
        for q in range(PIECES):
            from_core(offset, q)

    owned = positions // n_tp
    width = w_ref.shape[1]
    quarter = n // 4

    def share(rows, group):
        left = both[rows, :]
        for slot in range(group * quarter, (group + 1) * quarter, 2):
            right = jnp.concatenate([weights[slot], weights[slot + 1]], axis=1)
            yield slot, jnp.dot(left, right, preferred_element_type=f32).astype(bf16)

    def out_copy(turn, group):
        cols = pl.ds(group * quarter * width, quarter * width)
        return pltpu.make_async_remote_copy(
            src_ref=gone_out.at[turn - 1, :, cols],
            dst_ref=come_out.at[turn - 1, :, cols],
            send_sem=out_send.at[turn - 1, group],
            recv_sem=out_recv.at[turn - 1, group],
            device_id={"tp": (tp + turn) % n_tp},
        )

    for turn in range(1, n_tp):
        target = (tp + turn) % n_tp
        rows = pl.ds(pl.multiple_of(target * owned, owned), owned)
        for group in range(4):
            for slot, value in share(rows, group):
                gone_out[turn - 1, :, slot * width : (slot + 2) * width] = value
            copy = out_copy(turn, group)
            copy.start()
            sends.append(copy)
    rows = pl.ds(pl.multiple_of(tp * owned, owned), owned)
    for group in range(4):
        for slot, value in share(rows, group):
            mine[:, slot * width : (slot + 2) * width] = value.astype(f32)
    for turn in range(1, n_tp):
        for group in range(4):
            out_copy(turn, group).wait_recv()
        mine[...] += come_out[turn - 1].astype(f32)
    summed = mine[...]
    out_ref[...] = (
        summed
        * lax.rsqrt(jnp.mean(summed * summed, axis=1, keepdims=True) + eps)
        * post_ref[...]
    ).astype(bf16)
    tail_copy.wait_send()
    for copy in sends:
        copy.wait_send()


def mix(proj, keep, extra, sgain, pool_mix, pgain, shard, post):
    n = lax.axis_size("sp")
    n_tp = lax.axis_size("tp")
    positions, heads = extra.shape
    head_cols = heads * DK
    depth, width = shard.shape
    steps = n // 4
    rounds = (n - 1).bit_length()
    owned = positions // n_tp
    model = n * width
    padded = -(-heads // 8) * 8
    f32, bf16, dma = jnp.float32, jnp.bfloat16, pltpu.SemaphoreType.DMA
    return pl.pallas_call(
        functools.partial(mix_kernel, n, n_tp),
        out_shape=jax.ShapeDtypeStruct((owned, model), bf16),
        in_specs=[pl.BlockSpec(memory_space=pltpu.VMEM)] * 8,
        out_specs=pl.BlockSpec(memory_space=pltpu.VMEM),
        scratch_shapes=[
            pltpu.VMEM((n, depth, width), bf16),
            pltpu.VMEM((positions, head_cols), f32),
            pltpu.VMEM((positions, head_cols), bf16),
            pltpu.VMEM((positions, 2 * head_cols), bf16),
            pltpu.VMEM((heads, DK, DK), f32),
            pltpu.VMEM((heads, DK, DK), f32),
            pltpu.VMEM((rounds, heads, DK, DK), bf16),
            pltpu.VMEM((rounds, padded, DK), f32),
            pltpu.VMEM((rounds, heads, DK, DK), bf16),
            pltpu.VMEM((rounds, padded, DK), f32),
            pltpu.VMEM((16, head_cols), bf16),
            pltpu.VMEM((16, head_cols), bf16),
            pltpu.VMEM((owned, model), f32),
            pltpu.VMEM((n_tp, owned, model), bf16),
            pltpu.VMEM((n_tp, owned, model), bf16),
            dma((2, steps, PIECES)),
            dma((2, steps, PIECES)),
            dma((2 * steps, PIECES)),
            dma((2 * steps, PIECES)),
            dma((rounds, 2)),
            dma((rounds, 2)),
            dma((2,)),
            dma,
            dma((n_tp, 4)),
            dma((n_tp, 4)),
        ],
        compiler_params=pltpu.CompilerParams(
            collective_id=1, has_side_effects=True, vmem_limit_bytes=56 * 1024 * 1024
        ),
        cost_estimate=pl.CostEstimate(
            flops=2 * positions * depth * model, bytes_accessed=4 * depth * width, transcendentals=0
        ),
    )(proj, keep, extra, sgain, pool_mix, pgain, shard, post)


def pair_kernel(
    tok_hbm,
    gain_ref,
    w0,
    w1,
    w2,
    w3,
    w4,
    w5,
    rate_ref,
    extra_hbm,
    sgain_ref,
    mix_hbm,
    pgain_ref,
    orec_hbm,
    opool_hbm,
    post_ref,
    out_ref,
    wide,
    scaled,
    inv_rms,
    w_own,
    w_all,
    o_all,
    extra,
    mix_own,
    proj,
    local,
    reach,
    faded,
    kept,
    scored,
    state,
    state_go,
    state_come,
    decay_go,
    decay_come,
    tail_go,
    tail_come,
    total_go,
    total_come,
    last_go,
    last_come,
    y_all,
    y_go,
    part_go,
    part_come,
    mine,
    own_sem,
    tok_send,
    tok_recv,
    extra_send,
    extra_recv,
    w_send,
    w_recv,
    wy_send,
    wy_recv,
    o_send,
    o_recv,
    oy_send,
    oy_recv,
    scan_send,
    scan_recv,
    y_send,
    y_recv,
    part_send,
    part_recv,
):
    f32, bf16 = jnp.float32, jnp.bfloat16
    me = lax.axis_index("sp")
    x = lax.axis_index("tp")
    z, y, c = me // 4, (me // 2) % 2, me % 2
    odd = z % 2
    pair = z // 2
    head = odd * 2 + c
    is_mid = (z == 1) | (z == 2)
    slabs = [z, z + 1 - 2 * odd, 2 - pair, 3 * (1 - pair)]
    my_slot = jnp.where(is_mid, 2, 3)
    rows, feats = tok_hbm.shape
    shard = w0.shape[0]
    parts = (w0, w1, w2, w3, w4, w5)
    units = len(parts)
    positions = wide.shape[0]
    half = positions // 2
    block = rows
    blocks = positions // block
    piece = rows // 2

    def peer(zz, yy, cc):
        return {"sp": zz * 4 + yy * 2 + cc}

    def peer_x(cc):
        return {"sp": z * 4 + y * 2 + cc, "tp": 1 - x}

    other_c = peer(z, y, 1 - c)
    other_y = peer(z, 1 - y, c)

    def lanes(i, n=1):
        return pl.ds(pl.multiple_of(i * DK, DK), n * DK)

    def own_rows(base, size):
        return pl.ds(pl.multiple_of(base, 16), size)

    def tok_at(zq, cc, xx, q):
        start = zq * half + cc * rows + q * piece
        return wide.at[own_rows(start, piece), pl.ds(pl.multiple_of(xx * feats, 128), feats)]

    owns = {}

    def own_copy(name, src, dst):
        copy = pltpu.make_async_copy(src, dst, own_sem.at[len(owns)])
        copy.start()
        owns[name] = copy

    for q in range(2):
        own_copy(("tok", q), tok_hbm.at[pl.ds(q * piece, piece)], tok_at(odd, c, x, q))
    for u, part in enumerate(parts):
        own_copy(("w", u), part, w_own.at[u])
    own_copy("extra", extra_hbm, extra.at[odd * 2 + c])
    here = z * 2 + y
    own_copy(("o", 0), orec_hbm, o_all.at[here, pl.ds(0, 4 * DK)])
    own_copy(("o", 1), opool_hbm, o_all.at[here, pl.ds(4 * DK, 4 * DK)])
    own_copy("mix", mix_hbm.at[head], mix_own)

    barrier = pltpu.get_barrier_semaphore()
    peers = [other_c, other_y, peer_x(c), peer_x(1 - c)]
    for k in range(1, 4):
        peers += [peer(slabs[k], y, c), peer(slabs[k], y, 1 - c)]
    for to in peers:
        pl.semaphore_signal(barrier, inc=1, device_id=to)
    pl.semaphore_wait(barrier, len(peers))

    sends = []

    def send(src, dst, send_sem, recv_sem, to):
        copy = pltpu.make_async_remote_copy(
            src_ref=src, dst_ref=dst, send_sem=send_sem, recv_sem=recv_sem, device_id=to
        )
        copy.start()
        sends.append(copy)

    def arrive(dst, send_sem, recv_sem, to):
        pltpu.make_async_remote_copy(
            src_ref=dst, dst_ref=dst, send_sem=send_sem, recv_sem=recv_sem, device_id=to
        ).wait_recv()

    def tok_send_to(kind, q, zq, cc, xx, to):
        at = tok_at(zq, cc, xx, q)
        send(at, at, tok_send.at[kind, q], tok_recv.at[kind, q], to)

    def tok_arrive(kind, q, zq, cc, xx):
        at = tok_at(zq, cc, xx, q)
        arrive(at, tok_send.at[kind, q], tok_recv.at[kind, q], other_c)

    for q in range(2):
        owns[("tok", q)].wait()
        tok_send_to(0, q, odd, c, x, peer(slabs[1], y, c))
        tok_send_to(1, q, odd, c, x, peer_x(c))
        tok_send_to(3, q, odd, c, x, other_c)

    def w_piece(slab, cc, n=1):
        return own_rows((slab * 4 + y * 2 + cc) * shard, n * shard)

    def send_copy(src, dst, send_sem, recv_sem, to):
        return pltpu.make_async_remote_copy(
            src_ref=src, dst_ref=dst, send_sem=send_sem, recv_sem=recv_sem, device_id=to
        )

    def w_send_to(u, k, only=None):
        copies = []
        for e in range(2):
            cc = c if e == 0 else 1 - c
            slot = 1 if k == 1 else my_slot
            copies.append(
                send_copy(
                    w_own.at[u, :, lanes((slabs[k] % 2) * 2 + cc)],
                    w_all.at[u, w_piece(z, c)],
                    w_send.at[u, k, e],
                    w_recv.at[u, slot, e],
                    peer(slabs[k], y, cc),
                )
            )
        issue(copies, only, last=only is not is_mid)

    def issue(copies, only=None, last=True):
        if only is None:
            for copy in copies:
                copy.start()
        else:

            @pl.when(only)
            def _():
                for copy in copies:
                    copy.start()

        if last:
            sends.extend(copies)

    w_locals = []
    for u in range(units):
        owns[("w", u)].wait()
        keep_here = pltpu.make_async_copy(
            w_own.at[u, :, lanes(head)], w_all.at[u, w_piece(z, c)], own_sem.at[len(owns) + u]
        )
        keep_here.start()
        w_locals.append(keep_here)
        send(
            w_own.at[u, :, lanes(odd * 2 + 1 - c)],
            w_all.at[u, w_piece(z, c)],
            w_send.at[u, 0, 1],
            w_recv.at[u, 0, 1],
            other_c,
        )
        w_send_to(u, 1)
    for u in range(units):
        w_send_to(u, 2, is_mid)
    owns["extra"].wait()
    for e, to in enumerate([other_c, peer(slabs[1], y, c), peer(slabs[1], y, 1 - c)]):
        at = extra.at[odd * 2 + c]
        send(at, at, extra_send.at[e], extra_recv.at[e], to)

    def w_relay(u, k):
        if k == 0:
            w_locals[u].wait()
        else:
            arrive(
                w_all.at[u, w_piece(slabs[k], c)], w_send.at[u, k, 0], w_recv.at[u, k, 0], other_c
            )
        arrive(
            w_all.at[u, w_piece(slabs[k], 1 - c)], w_send.at[u, k, 1], w_recv.at[u, k, 1], other_c
        )
        at = w_all.at[u, w_piece(slabs[k], 0, 2)]
        send_copy(at, at, wy_send.at[u, k], wy_recv.at[u, k], other_y).start()

    def w_relay_mid():
        @pl.when(is_mid)
        def _():
            for u in range(units):
                w_relay(u, 2)

    def w_relay_end(u):
        @pl.when(jnp.logical_not(is_mid))
        def _():
            w_relay(u, 2)

    def w_late():
        for u in range(units):
            w_send_to(u, 2, jnp.logical_not(is_mid))
            w_send_to(u, 3)

    def w_need(u):
        for k in range(4):
            start = (slabs[k] * 4 + (1 - y) * 2) * shard
            at = w_all.at[u, own_rows(start, 2 * shard)]
            arrive(at, wy_send.at[u, k], wy_recv.at[u, k], other_y)

    pieces = 4
    depth = o_all.shape[1] // pieces

    def o_at(slab, yy, part):
        return o_all.at[slab * 2 + yy, pl.ds(part * depth, depth)]

    def o_out(k, only=None, which=range(pieces)):
        slot = 1 if k == 1 else my_slot
        copies = []
        for part in which:
            at = o_at(z, y, part)
            copies.append(
                send_copy(
                    at, at, o_send.at[k, part], o_recv.at[slot, part], peer(slabs[k], y, c)
                )
            )
        issue(copies, only, last=only is not is_mid)

    def o_relay(k, part):
        at = o_at(slabs[k], y, part)
        if k > 0:
            arrive(at, o_send.at[k, part], o_recv.at[k, part], other_c)
        send(at, at, oy_send.at[k, part], oy_recv.at[k, part], other_y)

    def o_need(k):
        for part in range(pieces):
            at = o_at(slabs[k], 1 - y, part)
            arrive(at, oy_send.at[k, part], oy_recv.at[k, part], other_y)

    is_end = jnp.logical_not(is_mid)

    for u in range(units):
        w_relay(u, 0)
    for part in range(2):
        owns[("o", part)].wait()

    def tok_z(q):
        tok_arrive(0, q, 1 - odd, c, x)
        tok_send_to(2, q, 1 - odd, c, x, peer_x(c))
        tok_send_to(4, q, 1 - odd, c, x, other_c)

    def tok_x(q):
        tok_arrive(1, q, odd, c, 1 - x)
        tok_send_to(5, q, odd, c, 1 - x, other_c)

    def tok_diagonal(q):
        tok_arrive(2, q, 1 - odd, c, 1 - x)
        tok_send_to(6, q, 1 - odd, c, 1 - x, other_c)

    def scale(zq, cc):
        at = own_rows(zq * half + cc * rows, rows)
        values = wide[at, :].astype(f32)
        scaled[at, :] = (values * gain_ref[...]).astype(bf16)
        squares = jnp.sum(values * values, axis=1, keepdims=True)
        inv_rms[at, :] = jnp.broadcast_to(
            lax.rsqrt(squares / wide.shape[1] + eps), (rows, DK)
        )

    tok_z(0)
    for part in range(pieces):
        o_relay(0, part)
    tok_z(1)
    w_late()
    for q in range(2):
        tok_x(q)
    w_relay_mid()
    scale(odd, c)
    for q in range(2):
        tok_arrive(3, q, odd, 1 - c, x)
        tok_arrive(5, q, odd, 1 - c, 1 - x)
    scale(odd, 1 - c)

    def w_relays(u):
        w_relay(u, 1)
        w_relay_end(u)
        w_relay(u, 3)

    w_relays(0)
    tok_diagonal(0)
    w_relays(1)
    tok_diagonal(1)
    scale(1 - odd, c)
    for q in range(2):
        tok_arrive(4, q, 1 - odd, 1 - c, x)
        tok_arrive(6, q, 1 - odd, 1 - c, 1 - x)
    scale(1 - odd, 1 - c)
    w_relays(2)

    def project_units(first, count):
        def one(i, _):
            at = own_rows(i * block, block)
            right = [w_all[u] for u in range(first, first + count)]
            right = right[0] if count == 1 else jnp.concatenate(right, axis=1)
            acc = jnp.dot(scaled[at, :], right, preferred_element_type=f32)
            norm = inv_rms[at, :]
            for j in range(count):
                proj[first + j, at, :] = (acc[:, j * DK : (j + 1) * DK] * norm).astype(bf16)
            return 0

        lax.fori_loop(0, blocks, one, 0)

    w_need(0)
    w_need(1)
    project_units(0, 2)
    for e, (zq, cc) in enumerate([(odd, 1 - c), (1 - odd, c), (1 - odd, 1 - c)]):
        arrive(extra.at[zq * 2 + cc], extra_send.at[e], extra_recv.at[e], other_c)
    w_relays(3)

    rate = rate_ref[:, lanes(head)]
    series = jnp.ones_like(rate)
    for n in range(10, 1, -1):
        series = 1.0 - series * rate / n
    keep = jnp.where(rate < 0.5, rate * series, 1.0 - jnp.exp(-rate))

    row = lax.broadcasted_iota(jnp.int32, (block, block), 0)
    col = lax.broadcasted_iota(jnp.int32, (block, block), 1)
    lower = jnp.where(row >= col, 1.0, 0.0).astype(f32)
    line = lax.broadcasted_iota(jnp.int32, (block, DK), 0)
    eighths = block // 8
    sub = lax.broadcasted_iota(jnp.int32, (eighths, 8, DK), 1)
    over_last = (((1,), (1,)), ((), ()))
    decays = []

    def score_block(b):
        at = slice(b * block, (b + 1) * block)
        q = proj[1, at, :].astype(f32) * DK ** (-0.5)
        kg = keep * jax.nn.sigmoid(-proj[0, at, :].astype(f32))
        added = jnp.broadcast_to(extra[b, pl.ds(head, 1), :], (DK, block)).T
        logs = jnp.log1p(-kg) + added
        cum = jnp.dot(lower, logs, precision=coarsest_scale_depth, preferred_element_type=f32)
        last = cum[block - 1 :, :]
        faded[at, :] = (kg * jnp.exp(last - cum)).astype(bf16)
        decays.append(jnp.exp(last))
        reach[at, :] = (q * jnp.exp(cum)).astype(bf16)
        kept[0, at, :] = cum
        kept[1, at, :] = kg
        scores = jnp.zeros((block, block), f32)
        span = 8
        while span < block:
            twice = 2 * span
            c3 = cum.reshape(block // twice, twice, DK)
            middle = jnp.broadcast_to(c3[:, span - 1 : span, :], c3.shape).reshape(cum.shape)
            fade = jnp.exp(-jnp.abs(cum - middle))
            later = (line // span) % 2 == 1
            probe = jnp.where(later, q * fade, 0.0).astype(bf16)
            keyed = jnp.where(later, 0.0, kg * fade).astype(bf16)
            found = lax.dot_general(probe, keyed, over_last, preferred_element_type=f32)
            scores = scores + jnp.where(row // twice == col // twice, found, 0.0)
            span = twice
        scored[b] = scores.astype(bf16)

    def value_block(b):
        at = slice(b * block, (b + 1) * block)
        q = proj[1, at, :].astype(f32) * DK ** (-0.5)
        v = proj[2, at, :]
        state[b] = lax.dot_general(
            v, faded[at, :], (((0,), (0,)), ((), ())), preferred_element_type=f32
        )
        result = jnp.dot(scored[b], v, preferred_element_type=f32)
        c3 = kept[0, at, :].reshape(eighths, 8, DK)
        q3 = q.reshape(eighths, 8, DK)
        k3 = kept[1, at, :].reshape(eighths, 8, DK)
        v3 = v.astype(f32).reshape(eighths, 8, DK)
        near = result.reshape(eighths, 8, DK)
        for s in range(8):
            weight = jnp.exp(jnp.minimum(c3 - c3[:, s : s + 1, :], 0.0))
            score = jnp.sum(q3 * k3[:, s : s + 1, :] * weight, axis=2, keepdims=True)
            near = near + jnp.where(sub >= s, score * v3[:, s : s + 1, :], 0.0)
        local[at, :] = near.reshape(block, DK)

    score_block(0)
    score_block(1)
    w_need(2)
    project_units(2, 1)
    w_relays(4)
    o_out(1)
    o_out(2, is_mid)
    score_block(2)
    score_block(3)
    for b in range(blocks):
        value_block(b)

    sums = [decays[2 * i + 1] * state[2 * i] + state[2 * i + 1] for i in range(2)]
    fades = [decays[2 * i] * decays[2 * i + 1] for i in range(2)]
    for i in range(2):
        state_go[i] = sums[i].astype(bf16)
        decay_go[i : i + 1, :] = fades[i]
    send(state_go, state_come, scan_send.at[0], scan_recv.at[0], other_y)
    send(decay_go, decay_come, scan_send.at[1], scan_recv.at[1], other_y)
    w_need(3)
    project_units(3, 1)
    for i in range(2):
        tail_go[i] = proj[3, (i + 1) * half - 16 : (i + 1) * half, :]
    send(tail_go, tail_come, scan_send.at[2], scan_recv.at[2], other_y)
    w_relays(5)

    arrive(state_come, scan_send.at[0], scan_recv.at[0], other_y)
    arrive(decay_come, scan_send.at[1], scan_recv.at[1], other_y)
    first_y = y == 0
    theirs = [state_come[i].astype(f32) for i in range(2)]
    their_fades = [decay_come[i : i + 1, :] for i in range(2)]
    order = []
    for i in range(2):
        order.append(
            (jnp.where(first_y, sums[i], theirs[i]), jnp.where(first_y, fades[i], their_fades[i]))
        )
        order.append(
            (jnp.where(first_y, theirs[i], sums[i]), jnp.where(first_y, their_fades[i], fades[i]))
        )
    total = order[0][0]
    for add, fade in order[1:]:
        total = fade * total + add
    total_go[...] = total.astype(bf16)
    arrive(tail_come, scan_send.at[2], scan_recv.at[2], other_y)
    last_go[...] = jnp.where(first_y, tail_come[1].astype(f32), tail_go[1].astype(f32)).astype(bf16)
    across = peer((z + 2) % 4, y, c)
    send(total_go, total_come, scan_send.at[3], scan_recv.at[3], across)
    send(last_go, last_come, scan_send.at[4], scan_recv.at[4], across)

    o_out(2, is_end, range(2))
    o_out(3, is_mid)
    for part in range(pieces):
        o_relay(1, part)
    w_need(4)
    w_need(5)
    project_units(4, 2)
    owns["mix"].wait()
    arrive(total_come, scan_send.at[3], scan_recv.at[3], across)
    arrive(last_come, scan_send.at[4], scan_recv.at[4], across)

    later_pair = pair > 0
    at_head = lanes(head)
    level = (x * 4 + head) % 4
    window = 2
    for k in range(1, 4):
        window = jnp.where(level == k, 2 ** (1 + k), window)
    line_half = lax.broadcasted_iota(jnp.int32, (half, DK), 0)
    far = [jnp.where(later_pair, last_come[...].astype(f32), 0.0), tail_come[0].astype(f32)]
    their_tails = [tail_come[i].astype(f32) for i in range(2)]
    befores = []
    running = jnp.where(later_pair, total_come[...].astype(f32), 0.0)
    for i in range(2):
        after_first = order[2 * i][1] * running + order[2 * i][0]
        befores.append(jnp.where(first_y, running, after_first))
        running = order[2 * i + 1][1] * after_first + order[2 * i + 1][0]

    def y_half(i):
        at = own_rows(i * half, half)
        at_static = slice(i * half, (i + 1) * half)
        xin = proj[3, at_static, :].astype(f32)
        prior = jnp.where(first_y, far[i], their_tails[i])
        sums_in = jnp.concatenate([prior, xin], axis=0)
        chosen = jnp.zeros((half, DK), f32)
        for k in range(4):
            sums_in = sums_in + pltpu.roll(sums_in, 2**k, 0)
            chosen = jnp.where(level == k, sums_in[16:, :], chosen)
        begins = (4 * pair + 2 * i + y) * half
        count = jnp.minimum(begins + line_half + 1, window).astype(f32)
        mixed = (chosen / count - xin).astype(bf16)
        mapped = jnp.dot(mixed, mix_own[...], preferred_element_type=f32)
        gate = proj[5, at_static, :].astype(f32)
        pooled = (mapped * pgain_ref[:, at_head] * (gate * jax.nn.sigmoid(gate))).astype(bf16)
        cur = befores[i]
        recs = []
        for j in range(2):
            b = 2 * i + j
            rows_b = slice(b * block, (b + 1) * block)
            rec = local[rows_b, :] + lax.dot_general(
                reach[rows_b, :], cur.astype(bf16), over_last, preferred_element_type=f32
            )
            cur = decays[b] * cur + state[b]
            normed = rec * lax.rsqrt(jnp.mean(rec * rec, axis=1, keepdims=True) + eps)
            gate = proj[4, rows_b, :].astype(f32)
            recs.append(
                (normed * sgain_ref[:, at_head] * (gate * jax.nn.sigmoid(gate))).astype(bf16)
            )
        return jnp.concatenate(recs, axis=0), pooled

    halves = [y_half(i) for i in range(2)]
    is_odd = odd == 1
    for part in range(2):
        low, high = halves[0][part].astype(f32), halves[1][part].astype(f32)
        y_go[part] = jnp.where(is_odd, low, high).astype(bf16)
        y_all[part * 4 + head] = jnp.where(is_odd, high, low).astype(bf16)
    z_peer = peer(slabs[1], y, c)
    their_head = (1 - odd) * 2 + c
    for part in range(2):
        send(
            y_go.at[part],
            y_all.at[part * 4 + head],
            y_send.at[0, part],
            y_recv.at[0, part],
            z_peer,
        )
        at = y_all.at[part * 4 + head]
        send(at, at, y_send.at[1, part], y_recv.at[1, part], other_c)
    o_out(2, is_end, range(2, pieces))
    o_out(3, is_end)
    for part in range(pieces):
        o_relay(2, part)
    for part in range(2):
        at = y_all.at[part * 4 + their_head]
        arrive(at, y_send.at[0, part], y_recv.at[0, part], z_peer)
        send(at, at, y_send.at[2, part], y_recv.at[2, part], other_c)
    for part in range(2):
        at = y_all.at[part * 4 + odd * 2 + 1 - c]
        arrive(at, y_send.at[1, part], y_recv.at[1, part], other_c)
    for part in range(2):
        at = y_all.at[part * 4 + (1 - odd) * 2 + 1 - c]
        arrive(at, y_send.at[2, part], y_recv.at[2, part], other_c)

    owned = part_come.shape[2]
    part_peers = [(x, 1 - c, other_c), (1 - x, c, peer_x(c)), (1 - x, 1 - c, peer_x(1 - c))]

    def rows_for(xx, cc):
        return own_rows(cc * rows + xx * owned, owned)

    def out_chunk(k):
        o_need(k)
        left = jnp.concatenate([y_all[i] for i in range(8)], axis=1)
        right = jnp.concatenate([o_all[slabs[k] * 2], o_all[slabs[k] * 2 + 1]], axis=1)
        part_go[k] = jnp.dot(left, right, preferred_element_type=f32).astype(bf16)
        for i, (xx, cc, to) in enumerate(part_peers):
            send(
                part_go.at[k, rows_for(xx, cc)],
                part_come.at[k, i],
                part_send.at[k, i],
                part_recv.at[k, i],
                to,
            )

    def gather_chunk(k):
        for i, (xx, cc, to) in enumerate(part_peers):
            arrive(part_come.at[k, i], part_send.at[k, i], part_recv.at[k, i], to)
        ours = part_go[k, rows_for(x, c), :].astype(f32) + part_come[k, 1].astype(f32)
        others = part_come[k, 0].astype(f32) + part_come[k, 2].astype(f32)
        for yy in range(2):
            cols = slice(yy * DK, (yy + 1) * DK)
            mine[:, lanes(slabs[k] * 4 + yy * 2 + c)] = ours[:, cols]
            mine[:, lanes(slabs[k] * 4 + yy * 2 + 1 - c)] = others[:, cols]

    out_chunk(0)
    out_chunk(1)
    for part in range(2):
        o_relay(3, part)
    out_chunk(2)
    for part in range(2, pieces):
        o_relay(3, part)
    for k in range(3):
        gather_chunk(k)
    out_chunk(3)
    gather_chunk(3)
    summed = mine[...]
    out_ref[...] = (
        summed
        * lax.rsqrt(jnp.mean(summed * summed, axis=1, keepdims=True) + eps)
        * post_ref[...]
    ).astype(bf16)
    for u in range(units):
        for k in range(4):
            at = w_all.at[u, w_piece(slabs[k], 0, 2)]
            send_copy(at, at, wy_send.at[u, k], wy_recv.at[u, k], other_y).wait_send()
    for copy in sends:
        copy.wait_send()


def pair_layer(
    tokens,
    gain,
    shards,
    rate,
    extra,
    sgain,
    pool_mix,
    pgain,
    out_rec,
    out_pool,
    post,
):
    n = lax.axis_size("sp")
    n_tp = lax.axis_size("tp")
    rows, feats = tokens.shape
    shard, cols = shards[0].shape
    heads = cols // DK
    depth, width = out_rec.shape
    slabs = n // 4
    positions = 4 * rows
    half = 2 * rows
    owned = rows // n_tp
    model = n * width
    f32, bf16, dma = jnp.float32, jnp.bfloat16, pltpu.SemaphoreType.DMA
    units = len(shards)
    vmem, hbm = pl.BlockSpec(memory_space=pltpu.VMEM), pl.BlockSpec(memory_space=pl.ANY)
    return pl.pallas_call(
        pair_kernel,
        out_shape=jax.ShapeDtypeStruct((owned, model), bf16),
        in_specs=[hbm, vmem] + [hbm] * 6 + [vmem, hbm, vmem, hbm, vmem, hbm, hbm, vmem],
        out_specs=vmem,
        scratch_shapes=[
            pltpu.VMEM((positions, n_tp * feats), bf16),
            pltpu.VMEM((positions, n_tp * feats), bf16),
            pltpu.VMEM((positions, DK), f32),
            pltpu.VMEM((units, shard, cols), bf16),
            pltpu.VMEM((units, n * shard, DK), bf16),
            pltpu.VMEM((2 * slabs, 2 * depth, width), bf16),
            pltpu.VMEM((4, heads, rows), f32),
            pltpu.VMEM((DK, DK), bf16),
            pltpu.VMEM((units, positions, DK), bf16),
            pltpu.VMEM((positions, DK), f32),
            pltpu.VMEM((positions, DK), bf16),
            pltpu.VMEM((positions, DK), bf16),
            pltpu.VMEM((2, positions, DK), f32),
            pltpu.VMEM((4, rows, rows), bf16),
            pltpu.VMEM((4, DK, DK), f32),
            pltpu.VMEM((2, DK, DK), bf16),
            pltpu.VMEM((2, DK, DK), bf16),
            pltpu.VMEM((8, DK), f32),
            pltpu.VMEM((8, DK), f32),
            pltpu.VMEM((2, 16, DK), bf16),
            pltpu.VMEM((2, 16, DK), bf16),
            pltpu.VMEM((DK, DK), bf16),
            pltpu.VMEM((DK, DK), bf16),
            pltpu.VMEM((16, DK), bf16),
            pltpu.VMEM((16, DK), bf16),
            pltpu.VMEM((2 * heads, half, DK), bf16),
            pltpu.VMEM((2, half, DK), bf16),
            pltpu.VMEM((slabs, half, 2 * width), bf16),
            pltpu.VMEM((slabs, 3, owned, 2 * width), bf16),
            pltpu.VMEM((owned, model), f32),
            dma((2 * units + 6,)),
            dma((7, 2)),
            dma((7, 2)),
            dma((3,)),
            dma((3,)),
            dma((units, slabs, 2)),
            dma((units, slabs, 2)),
            dma((units, slabs)),
            dma((units, slabs)),
            dma((slabs, 4)),
            dma((slabs, 4)),
            dma((slabs, 4)),
            dma((slabs, 4)),
            dma((5,)),
            dma((5,)),
            dma((3, 2)),
            dma((3, 2)),
            dma((slabs, 3)),
            dma((slabs, 3)),
        ],
        compiler_params=pltpu.CompilerParams(
            collective_id=0, has_side_effects=True, vmem_limit_bytes=56 * 1024 * 1024
        ),
        cost_estimate=pl.CostEstimate(
            flops=2 * positions * n * shard * units * DK,
            bytes_accessed=4 * units * shard * cols,
            transcendentals=0,
        ),
    )(
        tokens,
        gain[None, :],
        *shards,
        rate[None, :],
        extra.T,
        sgain[None, :],
        pool_mix,
        pgain[None, :],
        out_rec,
        out_pool,
        post[None, :],
    )


def per_device(
    tokens_in,
    norm_gain,
    w_query,
    w_forget,
    w_input,
    w_rgate,
    w_pool_in,
    w_pgate,
    floor_rate,
    extra_logdecay,
    state_gain,
    pool_mix,
    pool_gain,
    out_rec,
    out_pool,
    post_gain,
):
    n, n_tp, heads = lax.axis_size("sp"), lax.axis_size("tp"), extra_logdecay.shape[1]
    if n == 16 and n_tp == 2 and heads == 4:
        return pair_layer(
            tokens_in,
            norm_gain,
            [w_forget, w_query, w_input, w_pool_in, w_rgate, w_pgate],
            floor_rate,
            extra_logdecay,
            state_gain,
            pool_mix,
            pool_gain,
            out_rec,
            out_pool,
            post_gain,
        )
    shards = [w_query, w_forget, w_input, w_rgate, w_pool_in, w_pgate]
    proj = project(tokens_in, norm_gain, shards)
    return mix(
        proj,
        -jnp.expm1(-floor_rate)[None, :],
        extra_logdecay,
        state_gain[None, :],
        pool_mix,
        pool_gain[None, :],
        jnp.concatenate([out_rec, out_pool], axis=0),
        post_gain[None, :],
    )


def solution(mesh):
    placed = (
        P("sp", "tp"),
        P(),
        P("sp", "tp"),
        P("sp", "tp"),
        P("sp", "tp"),
        P("sp", "tp"),
        P("sp", "tp"),
        P("sp", "tp"),
        P("tp"),
        P("sp", "tp"),
        P("tp"),
        P("tp", None, None),
        P("tp"),
        P("tp", "sp"),
        P("tp", "sp"),
        P(),
    )
    return jax.shard_map(
        per_device, mesh=mesh, in_specs=placed, out_specs=P(("sp", "tp"), None), check_vma=False
    )
```

```python
import functools

import jax
import jax.numpy as jnp
from jax import lax
from jax.experimental import pallas as pl
from jax.experimental.pallas import tpu as pltpu
from jax.sharding import PartitionSpec as P

DK = 128


eps = 1e-06
coarsest_scale_depth = lax.Precision.HIGHEST


PIECES = 4


def ring_place(chip, chips):
    odd = chip % 2
    return (1 - odd) * (chip // 2) + odd * (chips - 1 - chip // 2)


def ring_chip(place, chips):
    back = place // (chips // 2)
    return (1 - back) * (2 * place) + back * (2 * (chips - 1 - place) + 1)


def project_kernel(
    n,
    n_tp,
    tok_ref,
    gain_ref,
    w0,
    w1,
    w2,
    w3,
    w4,
    w5,
    proj_ref,
    wide,
    scaled,
    weights,
    acc,
    tok_send,
    tok_recv,
    own_sem,
    ring_send,
    ring_recv,
    core_send,
    core_recv,
):
    chips = n // 2
    steps = chips // 2
    me = lax.axis_index("sp")
    tp = lax.axis_index("tp")
    core = me % 2
    place = ring_place(me // 2, chips)

    def chip_at(offset):
        return ring_chip((place + offset + chips) % chips, chips)

    following = 2 * chip_at(1) + core
    preceding = 2 * chip_at(-1) + core
    partner = 2 * (me // 2) + 1 - core
    parts = (w0, w1, w2, w3, w4, w5)
    rows, part_cols = w0.shape
    my_rows = pl.ds(pl.multiple_of(me * rows, 16), rows)
    owns = []
    for i, part in enumerate(parts):
        block = weights.at[my_rows, pl.ds(i * part_cols, part_cols)]
        owns.append(pltpu.make_async_copy(part, block, own_sem.at[i]))
        owns[-1].start()
    piece = rows // PIECES
    features = tok_ref.shape[1]

    barrier = pltpu.get_barrier_semaphore()
    for peer in (following, preceding, partner):
        pl.semaphore_signal(barrier, inc=1, device_id={"sp": peer})
    for turn in range(1, n_tp):
        pl.semaphore_signal(barrier, inc=1, device_id={"tp": (tp + turn) % n_tp})
    pl.semaphore_wait(barrier, 3 + n_tp - 1)

    def rows_of(chip, which, q):
        start = (2 * chip + which) * rows + q * piece
        return pl.ds(pl.multiple_of(start, 8), piece)

    sends = []

    def to_core(offset, q, source):
        slot = offset + steps - 1
        copy = pltpu.make_async_remote_copy(
            src_ref=source,
            dst_ref=weights.at[rows_of(chip_at(offset), core, q)],
            send_sem=core_send.at[slot, q],
            recv_sem=core_recv.at[slot, q],
            device_id={"sp": partner},
        )
        copy.start()
        sends.append(copy)

    def from_core(offset, q):
        slot = offset + steps - 1
        dst = weights.at[rows_of(chip_at(offset), 1 - core, q)]
        pltpu.make_async_remote_copy(
            src_ref=dst,
            dst_ref=dst,
            send_sem=core_send.at[slot, q],
            recv_sem=core_recv.at[slot, q],
            device_id={"sp": partner},
        ).wait_recv()

    def pieces_of(direction, step):
        if step < steps - 1:
            return range(PIECES)
        half = PIECES // 2
        return range(half) if direction == 0 else range(half, PIECES)

    def ring_copy(direction, step, q, source):
        offset = -step if direction == 0 else step
        dst = weights.at[rows_of(chip_at(offset), core, q)]
        return pltpu.make_async_remote_copy(
            src_ref=dst if source is None else source,
            dst_ref=dst,
            send_sem=ring_send.at[direction, step, q],
            recv_sem=ring_recv.at[direction, step, q],
            device_id={"sp": following if direction == 0 else preceding},
        )

    def ring_arrival(direction, step, q):
        offset = -(step + 1) if direction == 0 else step + 1
        dst = weights.at[rows_of(chip_at(offset), core, q)]
        pltpu.make_async_remote_copy(
            src_ref=dst,
            dst_ref=dst,
            send_sem=ring_send.at[direction, step, q],
            recv_sem=ring_recv.at[direction, step, q],
            device_id={"sp": following if direction == 0 else preceding},
        ).wait_recv()

    for own in owns:
        own.wait()
    for q in range(PIECES):
        mine = weights.at[rows_of(me // 2, core, q)]
        for direction in range(2):
            if q in pieces_of(direction, 0):
                copy = ring_copy(direction, 0, q, mine)
                copy.start()
                sends.append(copy)
        to_core(0, q, mine)
    tokens_at = pl.ds(pl.multiple_of(tp * features, 128), features)
    for turn in range(1, n_tp):
        copy = pltpu.make_async_remote_copy(
            src_ref=tok_ref,
            dst_ref=wide.at[:, tokens_at],
            send_sem=tok_send.at[turn - 1],
            recv_sem=tok_recv.at[turn - 1],
            device_id={"tp": (tp + turn) % n_tp},
        )
        copy.start()
        sends.append(copy)
    acc[...] = jnp.zeros_like(acc)
    wide[:, tokens_at] = tok_ref[...]
    for turn in range(1, n_tp):
        theirs = pl.ds(
            pl.multiple_of((tp - turn + n_tp) % n_tp * features, 128), features
        )
        pltpu.make_async_remote_copy(
            src_ref=tok_ref,
            dst_ref=wide.at[:, theirs],
            send_sem=tok_send.at[turn - 1],
            recv_sem=tok_recv.at[turn - 1],
            device_id={"tp": (tp + turn) % n_tp},
        ).wait_recv()
    scaled[...] = (wide[...].astype(jnp.float32) * gain_ref[...]).astype(jnp.bfloat16)

    cols = weights.shape[1]
    tile = cols // 6

    by_chip = (2 * rows) % 128 == 0

    def multiply(offset):
        if not by_chip:
            return
        multiply_rows(pl.ds(pl.multiple_of(chip_at(offset) * 2 * rows, 2 * rows), 2 * rows))

    def multiply_rows(depth):
        def one(i, _):
            at = pl.ds(pl.multiple_of(i * tile, 128), tile)
            acc[:, at] += jnp.dot(
                scaled[:, depth], weights[depth, at], preferred_element_type=jnp.float32
            )
            return 0

        lax.fori_loop(0, 6, one, 0)

    for step in range(steps):
        for q in range(PIECES):
            for direction in range(2):
                if q not in pieces_of(direction, step):
                    continue
                offset = -(step + 1) if direction == 0 else step + 1
                ring_arrival(direction, step, q)
                if step + 1 < steps and q in pieces_of(direction, step + 1):
                    copy = ring_copy(direction, step + 1, q, None)
                    copy.start()
                    sends.append(copy)
                last = offset if abs(offset) < steps else steps
                dst = weights.at[rows_of(chip_at(last), core, q)]
                to_core(last, q, dst)
        for offset in [0] if step == 0 else [-step, step]:
            for q in range(PIECES):
                from_core(offset, q)
            multiply(offset)
    for q in range(PIECES):
        from_core(steps, q)
    multiply(steps)
    if not by_chip:
        multiply_rows(slice(None))
    values = wide[...].astype(jnp.float32)
    squares = jnp.sum(values * values, axis=1, keepdims=True)
    inv_rms = lax.rsqrt(squares / wide.shape[1] + eps)
    proj_ref[...] = (acc[...] * inv_rms).astype(jnp.bfloat16)
    for copy in sends:
        copy.wait_send()


def project(tokens, gain, shards):
    n = lax.axis_size("sp")
    n_tp = lax.axis_size("tp")
    positions, features = tokens.shape
    rows = shards[0].shape[0]
    cols = sum(shard.shape[1] for shard in shards)
    width = n * rows
    steps = n // 4
    dma = pltpu.SemaphoreType.DMA
    return pl.pallas_call(
        functools.partial(project_kernel, n, n_tp),
        out_shape=jax.ShapeDtypeStruct((positions, cols), jnp.bfloat16),
        in_specs=[pl.BlockSpec(memory_space=pltpu.VMEM)] * 2
        + [pl.BlockSpec(memory_space=pl.ANY)] * 6,
        out_specs=pl.BlockSpec(memory_space=pltpu.VMEM),
        scratch_shapes=[
            pltpu.VMEM((positions, width), jnp.bfloat16),
            pltpu.VMEM((positions, width), jnp.bfloat16),
            pltpu.VMEM((width, cols), jnp.bfloat16),
            pltpu.VMEM((positions, cols), jnp.float32),
            dma((n_tp,)),
            dma((n_tp,)),
            dma((6,)),
            dma((2, steps, PIECES)),
            dma((2, steps, PIECES)),
            dma((2 * steps, PIECES)),
            dma((2 * steps, PIECES)),
        ],
        compiler_params=pltpu.CompilerParams(
            collective_id=0, has_side_effects=True, vmem_limit_bytes=56 * 1024 * 1024
        ),
        cost_estimate=pl.CostEstimate(
            flops=2 * positions * width * cols, bytes_accessed=4 * rows * cols, transcendentals=0
        ),
    )(tokens, gain[None, :], *shards)


def mix_kernel(
    n,
    n_tp,
    proj_ref,
    keep_ref,
    extra_ref,
    sgain_ref,
    mix_ref,
    pgain_ref,
    w_ref,
    post_ref,
    out_ref,
    weights,
    local,
    reach,
    both,
    state,
    before,
    gone_state,
    gone_decay,
    come_state,
    come_decay,
    tail,
    tail_in,
    mine,
    gone_out,
    come_out,
    ring_send,
    ring_recv,
    core_send,
    core_recv,
    scan_send,
    scan_recv,
    tail_sem,
    own_sem,
    out_send,
    out_recv,
):
    f32, bf16 = jnp.float32, jnp.bfloat16
    chips = n // 2
    steps = chips // 2
    rounds = (n - 1).bit_length()
    me = lax.axis_index("sp")
    tp = lax.axis_index("tp")
    core = me % 2
    place = ring_place(me // 2, chips)

    def chip_at(offset):
        return ring_chip((place + offset + chips) % chips, chips)

    following = 2 * chip_at(1) + core
    preceding = 2 * chip_at(-1) + core
    partner = 2 * (me // 2) + 1 - core
    piece = w_ref.shape[0] // PIECES

    barrier = pltpu.get_barrier_semaphore()
    for peer in (following, preceding, partner):
        pl.semaphore_signal(barrier, inc=1, device_id={"sp": peer})
    for r in range(rounds):
        pl.semaphore_signal(barrier, inc=1, device_id={"sp": (me + 2**r) % n})
        pl.semaphore_signal(barrier, inc=1, device_id={"sp": (me - 2**r + n) % n})
    for turn in range(1, n_tp):
        pl.semaphore_signal(barrier, inc=1, device_id={"tp": (tp + turn) % n_tp})
    pl.semaphore_wait(barrier, 3 + 2 * rounds + n_tp - 1)

    sends = []

    def spot(chip, which, q):
        return weights.at[2 * chip + which, pl.ds(q * piece, piece)]

    def to_core(offset, q, source):
        slot = offset + steps - 1
        copy = pltpu.make_async_remote_copy(
            src_ref=source,
            dst_ref=spot(chip_at(offset), core, q),
            send_sem=core_send.at[slot, q],
            recv_sem=core_recv.at[slot, q],
            device_id={"sp": partner},
        )
        copy.start()
        sends.append(copy)

    def from_core(offset, q):
        slot = offset + steps - 1
        dst = spot(chip_at(offset), 1 - core, q)
        pltpu.make_async_remote_copy(
            src_ref=dst,
            dst_ref=dst,
            send_sem=core_send.at[slot, q],
            recv_sem=core_recv.at[slot, q],
            device_id={"sp": partner},
        ).wait_recv()

    def pieces_of(direction, step):
        if step < steps - 1:
            return range(PIECES)
        half = PIECES // 2
        return range(half) if direction == 0 else range(half, PIECES)

    def ring_copy(direction, step, q, source, offset):
        dst = spot(chip_at(offset), core, q)
        return pltpu.make_async_remote_copy(
            src_ref=dst if source is None else source,
            dst_ref=dst,
            send_sem=ring_send.at[direction, step, q],
            recv_sem=ring_recv.at[direction, step, q],
            device_id={"sp": following if direction == 0 else preceding},
        )

    def ring_step(step):
        for q in range(PIECES):
            for direction in range(2):
                if q not in pieces_of(direction, step):
                    continue
                offset = -(step + 1) if direction == 0 else step + 1
                ring_copy(direction, step, q, None, offset).wait_recv()
                if step + 1 < steps and q in pieces_of(direction, step + 1):
                    copy = ring_copy(direction, step + 1, q, None, offset)
                    copy.start()
                    sends.append(copy)
                last = offset if abs(offset) < steps else steps
                to_core(last, q, spot(chip_at(last), core, q))

    pending = list(range(steps))

    def advance_ring():
        if pending:
            ring_step(pending.pop(0))

    positions = proj_ref.shape[0]
    head_cols = proj_ref.shape[1] // 6
    heads = head_cols // DK
    reach_back = tail.shape[0]

    tail[...] = proj_ref[positions - reach_back :, 4 * head_cols : 5 * head_cols]
    for q in range(PIECES):
        own_piece = w_ref.at[pl.ds(q * piece, piece)]
        for direction in range(2):
            if q in pieces_of(direction, 0):
                copy = ring_copy(direction, 0, q, own_piece, 0)
                copy.start()
                sends.append(copy)
        to_core(0, q, own_piece)
    own = pltpu.make_async_copy(w_ref, weights.at[me], own_sem)
    own.start()
    tail_copy = pltpu.make_async_remote_copy(
        src_ref=tail,
        dst_ref=tail_in,
        send_sem=tail_sem.at[0],
        recv_sem=tail_sem.at[1],
        device_id={"sp": (me + 1) % n},
    )
    tail_copy.start()

    row = lax.broadcasted_iota(jnp.int32, (positions, positions), 0)
    col = lax.broadcasted_iota(jnp.int32, (positions, positions), 1)
    lower = jnp.where(row >= col, 1.0, 0.0).astype(f32)
    line = lax.broadcasted_iota(jnp.int32, (positions, DK), 0)
    units = positions // 8
    sub = lax.broadcasted_iota(jnp.int32, (units, 8, DK), 1)
    over_last = (((1,), (1,)), ((), ()))

    decay_now = []
    for h in range(heads):
        at = slice(h * DK, (h + 1) * DK)
        part = lambda i: proj_ref[:, i * head_cols + h * DK : i * head_cols + (h + 1) * DK]
        q = part(0).astype(f32) * DK ** (-0.5)
        kg = keep_ref[:, at] * jax.nn.sigmoid(-part(1).astype(f32))
        v = part(2)
        logs = jnp.log1p(-kg) + extra_ref[:, h : h + 1]
        c = jnp.dot(
            lower, logs, precision=coarsest_scale_depth, preferred_element_type=f32
        )
        last = c[positions - 1 :, :]
        state[h] = lax.dot_general(
            v,
            (kg * jnp.exp(last - c)).astype(bf16),
            (((0,), (0,)), ((), ())),
            preferred_element_type=f32,
        )
        gone_decay[0, h : h + 1, :] = jnp.exp(last)
        reach[:, at] = (q * jnp.exp(c)).astype(bf16)
        scores = jnp.zeros((positions, positions), f32)
        span = 8
        while span < positions:
            pair = 2 * span
            c3 = c.reshape(positions // pair, pair, DK)
            middle = jnp.broadcast_to(c3[:, span - 1 : span, :], c3.shape).reshape(c.shape)
            fade = jnp.exp(-jnp.abs(c - middle))
            later = (line // span) % 2 == 1
            probe = jnp.where(later, q * fade, 0.0).astype(bf16)
            keyed = jnp.where(later, 0.0, kg * fade).astype(bf16)
            found = lax.dot_general(probe, keyed, over_last, preferred_element_type=f32)
            scores = scores + jnp.where(row // pair == col // pair, found, 0.0)
            span = pair
        result = jnp.dot(scores.astype(bf16), v, preferred_element_type=f32)
        c3 = c.reshape(units, 8, DK)
        q3 = q.reshape(units, 8, DK)
        k3 = kg.reshape(units, 8, DK)
        v3 = v.astype(f32).reshape(units, 8, DK)
        near = result.reshape(units, 8, DK)
        for s in range(8):
            weight = jnp.exp(jnp.minimum(c3 - c3[:, s : s + 1, :], 0.0))
            score = jnp.sum(q3 * k3[:, s : s + 1, :] * weight, axis=2, keepdims=True)
            near = near + jnp.where(sub >= s, score * v3[:, s : s + 1, :], 0.0)
        local[:, at] = near.reshape(positions, DK)
        if h % 2 == 1:
            advance_ring()

    def scan_copies(r):
        target = {"sp": (me + 2**r) % n}
        return [
            pltpu.make_async_remote_copy(
                src_ref=gone.at[r],
                dst_ref=come.at[r],
                send_sem=scan_send.at[r, i],
                recv_sem=scan_recv.at[r, i],
                device_id=target,
            )
            for i, (gone, come) in enumerate(
                [(gone_state, come_state), (gone_decay, come_decay)]
            )
        ]

    before[...] = jnp.zeros_like(before)
    decay_w = [gone_decay[0, h : h + 1, :] for h in range(heads)]
    decay_e = [jnp.ones((1, DK), f32) for h in range(heads)]

    def pool(h):
        at = slice(h * DK, (h + 1) * DK)
        x = proj_ref[:, 4 * head_cols + h * DK : 4 * head_cols + (h + 1) * DK].astype(f32)
        prior = jnp.where(me > 0, tail_in[:, at].astype(f32), 0.0)
        level = (tp * heads + h) % 4
        total = jnp.concatenate([prior, x], axis=0)
        chosen = jnp.zeros((positions, DK), f32)
        for k in range(4):
            total = total + pltpu.roll(total, 2**k, 0)
            chosen = jnp.where(level == k, total[reach_back:, :], chosen)
        window = 2
        for k in range(1, 4):
            window = jnp.where(level == k, 2 ** (1 + k), window)
        count = jnp.minimum(me * positions + line + 1, window).astype(f32)
        mixed = (chosen / count - x).astype(bf16)
        mapped = jnp.dot(mixed, mix_ref[h], preferred_element_type=f32)
        gate = proj_ref[:, 5 * head_cols + h * DK : 5 * head_cols + (h + 1) * DK].astype(f32)
        both[:, head_cols + h * DK : head_cols + (h + 1) * DK] = (
            mapped * pgain_ref[:, at] * (gate * jax.nn.sigmoid(gate))
        ).astype(bf16)

    pools = list(range(heads))
    for r in range(rounds):
        gone_state[r] = state[...].astype(bf16)
        if r > 0:
            for h in range(heads):
                gone_decay[r, h : h + 1, :] = decay_w[h]
        for copy in scan_copies(r):
            copy.start()
            sends.append(copy)
        if r == 0:
            tail_copy.wait_recv()
        if pools:
            pool(pools.pop(0))
        advance_ring()
        for copy in scan_copies(r):
            copy.wait_recv()
        valid = me >= 2**r
        for h in range(heads):
            came = jnp.where(valid, come_state[r, h].astype(f32), 0.0)
            came_decay = jnp.where(valid, come_decay[r, h : h + 1, :], 1.0)
            before[h] = before[h] + decay_e[h] * came
            decay_e[h] = decay_e[h] * came_decay
            if r + 1 < rounds:
                state[h] = state[h] + decay_w[h] * came
                decay_w[h] = decay_w[h] * came_decay
    for h in pools:
        pool(h)
    while pending:
        advance_ring()

    for h in range(heads):
        at = slice(h * DK, (h + 1) * DK)
        rec = local[:, at] + lax.dot_general(
            reach[:, at], before[h].astype(bf16), over_last, preferred_element_type=f32
        )
        normed = rec * lax.rsqrt(jnp.mean(rec * rec, axis=1, keepdims=True) + eps)
        gate = proj_ref[:, 3 * head_cols + h * DK : 3 * head_cols + (h + 1) * DK].astype(f32)
        both[:, at] = (normed * sgain_ref[:, at] * (gate * jax.nn.sigmoid(gate))).astype(bf16)

    own.wait()
    for offset in range(-(steps - 1), steps + 1):
        for q in range(PIECES):
            from_core(offset, q)

    owned = positions // n_tp
    width = w_ref.shape[1]
    quarter = n // 4

    def share(rows, group):
        left = both[rows, :]
        for slot in range(group * quarter, (group + 1) * quarter, 2):
            right = jnp.concatenate([weights[slot], weights[slot + 1]], axis=1)
            yield slot, jnp.dot(left, right, preferred_element_type=f32).astype(bf16)

    def out_copy(turn, group):
        cols = pl.ds(group * quarter * width, quarter * width)
        return pltpu.make_async_remote_copy(
            src_ref=gone_out.at[turn - 1, :, cols],
            dst_ref=come_out.at[turn - 1, :, cols],
            send_sem=out_send.at[turn - 1, group],
            recv_sem=out_recv.at[turn - 1, group],
            device_id={"tp": (tp + turn) % n_tp},
        )

    for turn in range(1, n_tp):
        target = (tp + turn) % n_tp
        rows = pl.ds(pl.multiple_of(target * owned, owned), owned)
        for group in range(4):
            for slot, value in share(rows, group):
                gone_out[turn - 1, :, slot * width : (slot + 2) * width] = value
            copy = out_copy(turn, group)
            copy.start()
            sends.append(copy)
    rows = pl.ds(pl.multiple_of(tp * owned, owned), owned)
    for group in range(4):
        for slot, value in share(rows, group):
            mine[:, slot * width : (slot + 2) * width] = value.astype(f32)
    for turn in range(1, n_tp):
        for group in range(4):
            out_copy(turn, group).wait_recv()
        mine[...] += come_out[turn - 1].astype(f32)
    summed = mine[...]
    out_ref[...] = (
        summed
        * lax.rsqrt(jnp.mean(summed * summed, axis=1, keepdims=True) + eps)
        * post_ref[...]
    ).astype(bf16)
    tail_copy.wait_send()
    for copy in sends:
        copy.wait_send()


def mix(proj, keep, extra, sgain, pool_mix, pgain, shard, post):
    n = lax.axis_size("sp")
    n_tp = lax.axis_size("tp")
    positions, heads = extra.shape
    head_cols = heads * DK
    depth, width = shard.shape
    steps = n // 4
    rounds = (n - 1).bit_length()
    owned = positions // n_tp
    model = n * width
    padded = -(-heads // 8) * 8
    f32, bf16, dma = jnp.float32, jnp.bfloat16, pltpu.SemaphoreType.DMA
    return pl.pallas_call(
        functools.partial(mix_kernel, n, n_tp),
        out_shape=jax.ShapeDtypeStruct((owned, model), bf16),
        in_specs=[pl.BlockSpec(memory_space=pltpu.VMEM)] * 8,
        out_specs=pl.BlockSpec(memory_space=pltpu.VMEM),
        scratch_shapes=[
            pltpu.VMEM((n, depth, width), bf16),
            pltpu.VMEM((positions, head_cols), f32),
            pltpu.VMEM((positions, head_cols), bf16),
            pltpu.VMEM((positions, 2 * head_cols), bf16),
            pltpu.VMEM((heads, DK, DK), f32),
            pltpu.VMEM((heads, DK, DK), f32),
            pltpu.VMEM((rounds, heads, DK, DK), bf16),
            pltpu.VMEM((rounds, padded, DK), f32),
            pltpu.VMEM((rounds, heads, DK, DK), bf16),
            pltpu.VMEM((rounds, padded, DK), f32),
            pltpu.VMEM((16, head_cols), bf16),
            pltpu.VMEM((16, head_cols), bf16),
            pltpu.VMEM((owned, model), f32),
            pltpu.VMEM((n_tp, owned, model), bf16),
            pltpu.VMEM((n_tp, owned, model), bf16),
            dma((2, steps, PIECES)),
            dma((2, steps, PIECES)),
            dma((2 * steps, PIECES)),
            dma((2 * steps, PIECES)),
            dma((rounds, 2)),
            dma((rounds, 2)),
            dma((2,)),
            dma,
            dma((n_tp, 4)),
            dma((n_tp, 4)),
        ],
        compiler_params=pltpu.CompilerParams(
            collective_id=1, has_side_effects=True, vmem_limit_bytes=56 * 1024 * 1024
        ),
        cost_estimate=pl.CostEstimate(
            flops=2 * positions * depth * model, bytes_accessed=4 * depth * width, transcendentals=0
        ),
    )(proj, keep, extra, sgain, pool_mix, pgain, shard, post)


def pair_kernel(
    tok_hbm,
    gain_ref,
    w0,
    w1,
    w2,
    w3,
    w4,
    w5,
    rate_ref,
    extra_hbm,
    sgain_ref,
    mix_hbm,
    pgain_ref,
    orec_hbm,
    opool_hbm,
    post_ref,
    out_ref,
    wide,
    scaled,
    inv_rms,
    w_own,
    w_all,
    o_all,
    extra,
    mix_own,
    proj,
    local,
    reach,
    faded,
    kept,
    scored,
    state,
    state_go,
    state_come,
    decay_go,
    decay_come,
    tail_go,
    tail_come,
    total_go,
    total_come,
    last_come,
    y_all,
    y_go,
    part_go,
    part_come,
    mine,
    done,
    own_sem,
    tok_send,
    tok_recv,
    extra_send,
    extra_recv,
    w_send,
    w_recv,
    wy_send,
    wy_recv,
    o_send,
    o_recv,
    oy_send,
    oy_recv,
    scan_send,
    scan_recv,
    y_send,
    y_recv,
    part_send,
    part_recv,
):
    f32, bf16 = jnp.float32, jnp.bfloat16
    me = lax.axis_index("sp")
    x = lax.axis_index("tp")
    z, y, c = me // 4, (me // 2) % 2, me % 2
    odd = z % 2
    pair = z // 2
    head = odd * 2 + c
    is_mid = (z == 1) | (z == 2)
    is_end = jnp.logical_not(is_mid)
    slabs = [z, z + 1 - 2 * odd, 2 - pair, 3 * (1 - pair)]
    my_slot = jnp.where(is_mid, 2, 3)
    rows, feats = tok_hbm.shape
    shard = w0.shape[0]
    parts = (w0, w1, w2, w3, w4, w5)
    units = len(parts)
    positions = wide.shape[0]
    half = positions // 2
    block = rows
    blocks = positions // block
    n_rows = w_all.shape[1]
    tok_pieces = 4
    piece = rows // tok_pieces

    def peer(zz, yy, cc):
        return {"sp": zz * 4 + yy * 2 + cc}

    def peer_x(cc):
        return {"sp": z * 4 + y * 2 + cc, "tp": 1 - x}

    other_c = peer(z, y, 1 - c)
    other_y = peer(z, 1 - y, c)

    def lanes(i, n=1):
        return pl.ds(pl.multiple_of(i * DK, DK), n * DK)

    def own_rows(base, size):
        return pl.ds(pl.multiple_of(base, 16), size)

    def tok_at(zq, cc, xx, q):
        start = zq * half + cc * rows + q * piece
        return wide.at[own_rows(start, piece), pl.ds(pl.multiple_of(xx * feats, 128), feats)]

    owns = {}

    def own_copy(name, src, dst):
        copy = pltpu.make_async_copy(src, dst, own_sem.at[len(owns)])
        copy.start()
        owns[name] = copy

    own_tok = wide.at[
        own_rows(odd * half + c * rows, rows), pl.ds(pl.multiple_of(x * feats, 128), feats)
    ]
    own_copy("tok", tok_hbm, own_tok)
    own_copy("extra", extra_hbm, extra.at[odd * 2 + c])
    here = z * 2 + y
    w_landed = own_sem.at[2]
    for u, part in enumerate(parts):
        pltpu.make_async_copy(part, w_own.at[u], w_landed).start()
    o_landed = own_sem.at[3]
    pltpu.make_async_copy(orec_hbm, o_all.at[here, pl.ds(0, 4 * DK)], o_landed).start()
    pltpu.make_async_copy(opool_hbm, o_all.at[here, pl.ds(4 * DK, 4 * DK)], o_landed).start()
    mix_copy = pltpu.make_async_copy(mix_hbm.at[head], mix_own, own_sem.at[4])
    mix_copy.start()

    barrier = pltpu.get_barrier_semaphore()
    across = peer((z + 2) % 4, y, c)
    across_y = peer((z + 2) % 4, 1 - y, c)
    peers = [other_c, other_y, peer_x(c), peer_x(1 - c), across_y]
    for k in range(1, 4):
        peers += [peer(slabs[k], y, c), peer(slabs[k], y, 1 - c)]
    for to in peers:
        pl.semaphore_signal(barrier, inc=1, device_id=to)
    pl.semaphore_wait(barrier, len(peers))

    def send(src, dst, send_sem, recv_sem, to):
        pltpu.make_async_remote_copy(
            src_ref=src, dst_ref=dst, send_sem=send_sem, recv_sem=recv_sem, device_id=to
        ).start()

    def sent(ref, send_sem):
        pltpu.make_async_remote_copy(
            src_ref=ref, dst_ref=ref, send_sem=send_sem, recv_sem=send_sem, device_id=other_c
        ).wait_send()

    def arrive(ref, recv_sem):
        pltpu.make_async_remote_copy(
            src_ref=ref, dst_ref=ref, send_sem=recv_sem, recv_sem=recv_sem, device_id=other_c
        ).wait_recv()

    def tok_rows(zq, cc, xx):
        start = zq * half + cc * rows
        return wide.at[own_rows(start, rows), pl.ds(pl.multiple_of(xx * feats, 128), feats)]

    def tok_share(at, near):
        send(at, at, tok_send.at[1], tok_recv.at[9 if near else 10], other_c)

    owns["extra"].wait()
    for e, to in enumerate([other_c, peer(slabs[1], y, c), peer(slabs[1], y, 1 - c)]):
        at = extra.at[odd * 2 + c]
        send(at, at, extra_send.at[0], extra_recv.at[e], to)
    owns["tok"].wait()
    for q in range(tok_pieces):
        at = tok_at(odd, c, x, q)
        send(at, at, tok_send.at[0], tok_recv.at[q], peer(slabs[1], y, c))
    send(own_tok, own_tok, tok_send.at[1], tok_recv.at[8], peer_x(c))
    tok_share(own_tok, True)

    def w_piece(slab, cc, n=1):
        return own_rows((slab * 4 + y * 2 + cc) * shard, n * shard)

    def send_copy(src, dst, send_sem, recv_sem, to):
        return pltpu.make_async_remote_copy(
            src_ref=src, dst_ref=dst, send_sem=send_sem, recv_sem=recv_sem, device_id=to
        )

    def w_send_to(u, k, only=None):
        copies = []
        for e in range(2):
            cc = c if e == 0 else 1 - c
            slot = 1 if k == 1 else my_slot
            copies.append(
                send_copy(
                    w_own.at[u, :, lanes((slabs[k] % 2) * 2 + cc)],
                    w_all.at[u, w_piece(z, c)],
                    w_send.at[0],
                    w_recv.at[u, slot],
                    peer(slabs[k], y, cc),
                )
            )
        issue(copies, only)

    def issue(copies, only=None):
        if only is None:
            for copy in copies:
                copy.start()
        else:

            @pl.when(only)
            def _():
                for copy in copies:
                    copy.start()

    pltpu.make_async_copy(w_own, w_own, w_landed).wait()
    for u in range(units):
        pltpu.make_async_copy(
            w_own.at[u, :, lanes(head)], w_all.at[u, w_piece(z, c)], w_recv.at[u, 0]
        ).start()
        send(
            w_own.at[u, :, lanes(odd * 2 + 1 - c)],
            w_all.at[u, w_piece(z, c)],
            w_send.at[0],
            w_recv.at[u, 0],
            other_c,
        )
        w_send_to(u, 1, None if u == 0 else is_mid)
        w_send_to(u, 2, is_mid)

    def w_relay(u, k):
        at = w_all.at[u, w_piece(slabs[k], 0, 2)]
        arrive(at, w_recv.at[u, k])
        send(at, at, wy_send.at[0], wy_recv.at[u], other_y)

    def w_late_end():
        for u in range(units):
            w_send_to(u, 3, is_end)
            w_send_to(u, 2, is_end)
            if u > 0:
                w_send_to(u, 1, is_end)

    def w_late_mid():
        for u in range(units):
            w_send_to(u, 3, is_mid)

    def w_need(u):
        arrive(w_all.at[u, pl.ds(0, n_rows // 2)], wy_recv.at[u])

    pieces = 4
    depth = o_all.shape[1] // pieces

    def o_at(slab, yy, part):
        return o_all.at[slab * 2 + yy, pl.ds(part * depth, depth)]

    def o_copy(route, part, held, slot, to):
        at = o_at(held, y, part)
        return send_copy(
            at, at, o_send.at[min(route, 1)], o_recv.at[slot - 1, part], peer(to, y, c)
        )

    def o_near():
        for part in range(pieces):
            o_copy(0, part, z, 1, slabs[1]).start()

    def o_across(which):
        @pl.when(is_mid)
        def _():
            for part in which:
                o_copy(1, part, z, 2, slabs[2]).start()

    def o_relay(k, part):
        at = o_at(slabs[k], y, part)
        if k > 0:
            arrive(at, o_recv.at[k - 1, part])
        send(at, at, oy_send.at[0], oy_recv.at[k], other_y)

    def o_onward(k, part):
        if k == 1:
            o_copy(2, part, slabs[1], 3, slabs[2]).start()
        else:
            o_copy(k + 1, part, slabs[k], k, slabs[1]).start()

    def o_near_relays(which):
        for part in which:
            o_relay(1, part)

            @pl.when(is_mid)
            def _():
                o_onward(1, part)

    def o_mid_relays(k, which):
        @pl.when(is_mid)
        def _():
            for part in which:
                o_relay(k, part)
                o_onward(k, part)

    def o_end_relays(k, which):
        @pl.when(is_end)
        def _():
            for part in which:
                o_relay(k, part)

    def o_need(k):
        arrive(o_all.at[slabs[k] * 2 + 1 - y], oy_recv.at[k])

    for u in range(units):
        w_relay(u, 0)
    pltpu.make_async_copy(o_all.at[here], o_all.at[here], o_landed).wait()

    def tok_z(q):
        at = tok_at(1 - odd, c, x, q)
        arrive(at, tok_recv.at[q])
        send(at, at, tok_send.at[1], tok_recv.at[4 + q], peer_x(c))
        tok_share(at, False)

    def tok_x():
        at = tok_rows(odd, c, 1 - x)
        arrive(at, tok_recv.at[8])
        tok_share(at, True)

    def tok_diagonal(q):
        at = tok_at(1 - odd, c, 1 - x, q)
        arrive(at, tok_recv.at[4 + q])
        tok_share(at, False)

    def tok_shared(zq, near):
        arrive(wide.at[own_rows(zq * half + (1 - c) * rows, rows)], tok_recv.at[9 if near else 10])

    def scale(zq, cc):
        at = own_rows(zq * half + cc * rows, rows)
        values = wide[at, :].astype(f32)
        scaled[at, :] = (values * gain_ref[...]).astype(bf16)
        squares = jnp.sum(values * values, axis=1, keepdims=True)
        inv_rms[at, :] = jnp.broadcast_to(
            lax.rsqrt(squares / wide.shape[1] + eps), (rows, DK)
        )

    def w_relays(u):
        w_relay(u, 1)
        w_relay(u, 2)
        w_relay(u, 3)

    tok_z(0)
    tok_z(1)
    w_late_end()
    for part in range(pieces):
        o_relay(0, part)
    tok_z(2)
    sent(own_tok, tok_send.at[0])
    w_late_mid()
    tok_z(3)
    tok_x()
    scale(odd, c)
    tok_shared(odd, True)
    scale(odd, 1 - c)
    w_relay(0, 2)
    w_relay(0, 1)
    w_relay(0, 3)
    tok_diagonal(0)
    tok_diagonal(1)
    w_relays(1)
    tok_diagonal(2)
    tok_diagonal(3)
    scale(1 - odd, c)
    tok_shared(1 - odd, False)
    scale(1 - odd, 1 - c)
    w_relays(2)

    def project_units(first, count):
        def one(i, _):
            at = own_rows(i * block, block)
            right = [w_all[u] for u in range(first, first + count)]
            right = right[0] if count == 1 else jnp.concatenate(right, axis=1)
            acc = jnp.dot(scaled[at, :], right, preferred_element_type=f32)
            norm = inv_rms[at, :]
            for j in range(count):
                proj[first + j, at, :] = (acc[:, j * DK : (j + 1) * DK] * norm).astype(bf16)
            return 0

        lax.fori_loop(0, blocks, one, 0)

    w_need(0)
    w_need(1)
    project_units(0, 2)
    for e, (zq, cc) in enumerate([(odd, 1 - c), (1 - odd, c), (1 - odd, 1 - c)]):
        arrive(extra.at[zq * 2 + cc], extra_recv.at[e])

    rate = rate_ref[:, lanes(head)]
    series = jnp.ones_like(rate)
    for n in range(10, 1, -1):
        series = 1.0 - series * rate / n
    keep = jnp.where(rate < 0.5, rate * series, 1.0 - jnp.exp(-rate))

    row = lax.broadcasted_iota(jnp.int32, (block, block), 0)
    col = lax.broadcasted_iota(jnp.int32, (block, block), 1)
    lower = jnp.where(row >= col, 1.0, 0.0).astype(f32)
    line = lax.broadcasted_iota(jnp.int32, (block, DK), 0)
    eighths = block // 8
    sub = lax.broadcasted_iota(jnp.int32, (eighths, 8, DK), 1)
    over_last = (((1,), (1,)), ((), ()))
    decays = []

    def score_block(b):
        at = slice(b * block, (b + 1) * block)
        q = proj[1, at, :].astype(f32) * DK ** (-0.5)
        kg = keep * jax.nn.sigmoid(-proj[0, at, :].astype(f32))
        added = jnp.broadcast_to(extra[b, pl.ds(head, 1), :], (DK, block)).T
        logs = jnp.log1p(-kg) + added
        cum = jnp.dot(lower, logs, precision=coarsest_scale_depth, preferred_element_type=f32)
        last = cum[block - 1 :, :]
        faded[at, :] = (kg * jnp.exp(last - cum)).astype(bf16)
        decays.append(jnp.exp(last))
        reach[at, :] = (q * jnp.exp(cum)).astype(bf16)
        kept[0, at, :] = cum
        kept[1, at, :] = kg
        scores = jnp.zeros((block, block), f32)
        span = 8
        while span < block:
            twice = 2 * span
            c3 = cum.reshape(block // twice, twice, DK)
            middle = jnp.broadcast_to(c3[:, span - 1 : span, :], c3.shape).reshape(cum.shape)
            fade = jnp.exp(-jnp.abs(cum - middle))
            later = (line // span) % 2 == 1
            probe = jnp.where(later, q * fade, 0.0).astype(bf16)
            keyed = jnp.where(later, 0.0, kg * fade).astype(bf16)
            found = lax.dot_general(probe, keyed, over_last, preferred_element_type=f32)
            scores = scores + jnp.where(row // twice == col // twice, found, 0.0)
            span = twice
        scored[b] = scores.astype(bf16)

    def value_block(b):
        at = slice(b * block, (b + 1) * block)
        q = proj[1, at, :].astype(f32) * DK ** (-0.5)
        v = proj[2, at, :]
        state[b] = lax.dot_general(
            v, faded[at, :], (((0,), (0,)), ((), ())), preferred_element_type=f32
        )
        result = jnp.dot(scored[b], v, preferred_element_type=f32)
        c3 = kept[0, at, :].reshape(eighths, 8, DK)
        q3 = q.reshape(eighths, 8, DK)
        k3 = kept[1, at, :].reshape(eighths, 8, DK)
        v3 = v.astype(f32).reshape(eighths, 8, DK)
        near = result.reshape(eighths, 8, DK)
        for s in range(8):
            weight = jnp.exp(jnp.minimum(c3 - c3[:, s : s + 1, :], 0.0))
            score = jnp.sum(q3 * k3[:, s : s + 1, :] * weight, axis=2, keepdims=True)
            near = near + jnp.where(sub >= s, score * v3[:, s : s + 1, :], 0.0)
        local[at, :] = near.reshape(block, DK)

    score_block(0)
    w_relays(3)
    score_block(1)
    score_block(2)
    score_block(3)
    w_relays(4)
    o_near()
    o_across(range(2))
    w_need(2)
    project_units(2, 1)
    for b in range(blocks):
        value_block(b)
        if b == 2:
            w_relays(5)

    sums = [decays[2 * i + 1] * state[2 * i] + state[2 * i + 1] for i in range(2)]
    fades = [decays[2 * i] * decays[2 * i + 1] for i in range(2)]
    for i in range(2):
        state_go[i] = sums[i].astype(bf16)
        decay_go[i : i + 1, :] = fades[i]
    send(state_go, state_come, scan_send.at[0], scan_recv.at[0], other_y)
    send(decay_go, decay_come, scan_send.at[1], scan_recv.at[1], other_y)
    w_need(3)
    project_units(3, 1)
    for i in range(2):
        tail_go[i] = proj[3, (i + 1) * half - 16 : (i + 1) * half, :]
    send(tail_go, tail_come, scan_send.at[2], scan_recv.at[2], other_y)
    send(tail_go.at[1], last_come, scan_send.at[4], scan_recv.at[4], across_y)
    w_need(4)
    project_units(4, 1)

    arrive(state_come, scan_recv.at[0])
    arrive(decay_come, scan_recv.at[1])
    first_y = y == 0
    theirs = [state_come[i].astype(f32) for i in range(2)]
    their_fades = [decay_come[i : i + 1, :] for i in range(2)]
    order = []
    for i in range(2):
        order.append(
            (jnp.where(first_y, sums[i], theirs[i]), jnp.where(first_y, fades[i], their_fades[i]))
        )
        order.append(
            (jnp.where(first_y, theirs[i], sums[i]), jnp.where(first_y, their_fades[i], fades[i]))
        )
    total = order[0][0]
    for add, fade in order[1:]:
        total = fade * total + add
    total_go[...] = total.astype(bf16)
    send(total_go, total_come, scan_send.at[3], scan_recv.at[3], across)
    o_across(range(2, pieces))
    o_near_relays(range(2))
    o_mid_relays(2, range(2))
    mix_copy.wait()
    arrive(tail_come, scan_recv.at[2])
    arrive(last_come, scan_recv.at[4])

    later_pair = pair > 0
    at_head = lanes(head)
    level = (x * 4 + head) % 4
    window = 2
    for k in range(1, 4):
        window = jnp.where(level == k, 2 ** (1 + k), window)
    line_half = lax.broadcasted_iota(jnp.int32, (half, DK), 0)
    far = [jnp.where(later_pair, last_come[...].astype(f32), 0.0), tail_come[0].astype(f32)]
    their_tails = [tail_come[i].astype(f32) for i in range(2)]
    is_odd = odd == 1

    def pool_half(i):
        at_static = slice(i * half, (i + 1) * half)
        xin = proj[3, at_static, :].astype(f32)
        prior = jnp.where(first_y, far[i], their_tails[i])
        sums_in = jnp.concatenate([prior, xin], axis=0)
        chosen = jnp.zeros((half, DK), f32)
        for k in range(4):
            sums_in = sums_in + pltpu.roll(sums_in, 2**k, 0)
            chosen = jnp.where(level == k, sums_in[16:, :], chosen)
        begins = (4 * pair + 2 * i + y) * half
        count = jnp.minimum(begins + line_half + 1, window).astype(f32)
        mixed = (chosen / count - xin).astype(bf16)
        mapped = jnp.dot(mixed, mix_own[...], preferred_element_type=f32)
        gate = proj[4, at_static, :].astype(f32)
        return mapped * pgain_ref[:, at_head] * (gate * jax.nn.sigmoid(gate))

    z_peer = peer(slabs[1], y, c)
    their_head = (1 - odd) * 2 + c

    def y_at(part, hd, ch):
        return y_all.at[part * 4 + hd, pl.ds(ch * block, block)]

    def y_put(part, ch, low, high):
        at = slice(ch * block, (ch + 1) * block)
        y_go[part, at, :] = jnp.where(is_odd, low, high).astype(bf16)
        y_all[part * 4 + head, at, :] = jnp.where(is_odd, high, low).astype(bf16)
        send(
            y_go.at[part, pl.ds(ch * block, block)],
            y_at(part, head, ch),
            y_send.at[0],
            y_recv.at[part * 2 + ch],
            z_peer,
        )
        at = y_at(part, head, ch)
        send(at, at, y_send.at[0], y_recv.at[4 + ch], other_c)

    def y_pass(part, ch):
        at = y_at(part, their_head, ch)
        arrive(at, y_recv.at[part * 2 + ch])
        send(at, at, y_send.at[0], y_recv.at[4 + ch], other_c)

    def y_need(ch):
        arrive(y_all.at[pl.ds(0, 2)], y_recv.at[4 + ch])

    pooled = [pool_half(i) for i in range(2)]
    for ch in range(2):
        rows_ch = slice(ch * block, (ch + 1) * block)
        y_put(1, ch, pooled[0][rows_ch], pooled[1][rows_ch])
    o_near_relays(range(2, pieces))
    w_need(5)
    project_units(5, 1)
    arrive(total_come, scan_recv.at[3])
    befores = []
    running = jnp.where(later_pair, total_come[...].astype(f32), 0.0)
    for i in range(2):
        after_first = order[2 * i][1] * running + order[2 * i][0]
        befores.append(jnp.where(first_y, running, after_first))
        running = order[2 * i + 1][1] * after_first + order[2 * i + 1][0]

    def rec_rows(b, before):
        rows_b = slice(b * block, (b + 1) * block)
        rec = local[rows_b, :] + lax.dot_general(
            reach[rows_b, :], before.astype(bf16), over_last, preferred_element_type=f32
        )
        normed = rec * lax.rsqrt(jnp.mean(rec * rec, axis=1, keepdims=True) + eps)
        gate = proj[5, rows_b, :].astype(f32)
        return normed * sgain_ref[:, at_head] * (gate * jax.nn.sigmoid(gate))

    for ch in range(2):
        recs = []
        for i in range(2):
            b = 2 * i + ch
            recs.append(rec_rows(b, befores[i]))
            befores[i] = decays[b] * befores[i] + state[b]
        y_put(0, ch, recs[0], recs[1])
    o_mid_relays(2, range(2, pieces))
    for ch in range(2):
        y_pass(1, ch)
    o_mid_relays(3, range(2))
    o_end_relays(2, range(2))
    y_pass(0, 0)
    o_mid_relays(3, range(2, pieces))
    o_end_relays(2, range(2, pieces))
    y_pass(0, 1)

    owned = part_come.shape[2]

    def rows_for(xx, cc):
        return own_rows(cc * rows + xx * owned, owned)

    def part_copies(k, ch):
        over_x = send_copy(
            part_go.at[k, rows_for(1 - x, ch)],
            part_come.at[k, c],
            part_send.at[0],
            part_recv.at[k],
            peer_x(ch),
        )
        over_c = send_copy(
            part_go.at[k, rows_for(x, ch)],
            part_come.at[k, 2],
            part_send.at[0],
            part_recv.at[k],
            other_c,
        )
        return over_x, over_c

    def out_chunk(k, ch):
        left = jnp.concatenate(
            [y_all[i, ch * block : (ch + 1) * block, :] for i in range(8)], axis=1
        )
        right = jnp.concatenate([o_all[slabs[k] * 2], o_all[slabs[k] * 2 + 1]], axis=1)
        part_go[k, ch * block : (ch + 1) * block, :] = jnp.dot(
            left, right, preferred_element_type=f32
        ).astype(bf16)
        over_x, over_c = part_copies(k, ch)
        over_x.start()

        @pl.when(c != ch)
        def _():
            over_c.start()

    def gather_chunk(k):
        arrive(part_come.at[k], part_recv.at[k])
        ours = part_go[k, rows_for(x, c), :].astype(f32) + part_come[k, c].astype(f32)
        others = part_come[k, 2].astype(f32) + part_come[k, 1 - c].astype(f32)
        for yy in range(2):
            cols = slice(yy * DK, (yy + 1) * DK)
            mine[:, lanes(slabs[k] * 4 + yy * 2 + c)] = ours[:, cols]
            mine[:, lanes(slabs[k] * 4 + yy * 2 + 1 - c)] = others[:, cols]

    for ch in range(2):
        y_need(ch)
        for k in range(2):
            if ch == 0:
                o_need(k)
            out_chunk(k, ch)
    o_need(2)
    for ch in range(2):
        o_end_relays(3, range(ch, ch + 1))
        out_chunk(2, ch)
    for k in range(2):
        gather_chunk(k)
        o_end_relays(3, range(k + 2, k + 3))
    gather_chunk(2)
    o_need(3)
    for ch in range(2):
        out_chunk(3, ch)
    gather_chunk(3)

    def finish():
        summed = mine[...]
        done[...] = (
            summed
            * lax.rsqrt(jnp.mean(summed * summed, axis=1, keepdims=True) + eps)
            * post_ref[...]
        ).astype(bf16)
        copy = pltpu.make_async_copy(done, out_ref, own_sem.at[0])
        copy.start()
        copy.wait()

    finish()
    def drain():
        sent(wide.at[pl.ds(0, 6 * rows // 2)], tok_send.at[1])
        sent(extra.at[pl.ds(0, 3)], extra_send.at[0])
        sent(w_all.at[pl.ds(0, 3), pl.ds(0, 14 * shard)], w_send.at[0])
        sent(w_all.at[pl.ds(0, 3)], wy_send.at[0])
        sent(o_all.at[0], o_send.at[0])
        sent(o_all.at[pl.ds(0, 4)], oy_send.at[0])

        @pl.when(is_mid)
        def _():
            sent(o_all.at[pl.ds(0, 4)], o_send.at[1])

        for i, ref in enumerate([state_go, decay_go, tail_go, total_go, tail_go.at[1]]):
            sent(ref, scan_send.at[i])
        sent(y_all.at[pl.ds(0, 6)], y_send.at[0])
        sent(part_go.at[pl.ds(0, 3)], part_send.at[0])

    drain()


def pair_layer(
    tokens,
    gain,
    shards,
    rate,
    extra,
    sgain,
    pool_mix,
    pgain,
    out_rec,
    out_pool,
    post,
):
    n = lax.axis_size("sp")
    n_tp = lax.axis_size("tp")
    rows, feats = tokens.shape
    shard, cols = shards[0].shape
    heads = cols // DK
    depth, width = out_rec.shape
    slabs = n // 4
    positions = 4 * rows
    half = 2 * rows
    owned = rows // n_tp
    model = n * width
    f32, bf16, dma = jnp.float32, jnp.bfloat16, pltpu.SemaphoreType.DMA
    units = len(shards)
    vmem, hbm = pl.BlockSpec(memory_space=pltpu.VMEM), pl.BlockSpec(memory_space=pl.ANY)
    return pl.pallas_call(
        pair_kernel,
        out_shape=jax.ShapeDtypeStruct((owned, model), bf16),
        in_specs=[hbm, vmem] + [hbm] * 6 + [vmem, hbm, vmem, hbm, vmem, hbm, hbm, vmem],
        out_specs=hbm,
        scratch_shapes=[
            pltpu.VMEM((positions, n_tp * feats), bf16),
            pltpu.VMEM((positions, n_tp * feats), bf16),
            pltpu.VMEM((positions, DK), f32),
            pltpu.VMEM((units, shard, cols), bf16),
            pltpu.VMEM((units, n * shard, DK), bf16),
            pltpu.VMEM((2 * slabs, 2 * depth, width), bf16),
            pltpu.VMEM((4, heads, rows), f32),
            pltpu.VMEM((DK, DK), bf16),
            pltpu.VMEM((units, positions, DK), bf16),
            pltpu.VMEM((positions, DK), f32),
            pltpu.VMEM((positions, DK), bf16),
            pltpu.VMEM((positions, DK), bf16),
            pltpu.VMEM((2, positions, DK), f32),
            pltpu.VMEM((4, rows, rows), bf16),
            pltpu.VMEM((4, DK, DK), f32),
            pltpu.VMEM((2, DK, DK), bf16),
            pltpu.VMEM((2, DK, DK), bf16),
            pltpu.VMEM((8, DK), f32),
            pltpu.VMEM((8, DK), f32),
            pltpu.VMEM((2, 16, DK), bf16),
            pltpu.VMEM((2, 16, DK), bf16),
            pltpu.VMEM((DK, DK), bf16),
            pltpu.VMEM((DK, DK), bf16),
            pltpu.VMEM((16, DK), bf16),
            pltpu.VMEM((2 * heads, half, DK), bf16),
            pltpu.VMEM((2, half, DK), bf16),
            pltpu.VMEM((slabs, half, 2 * width), bf16),
            pltpu.VMEM((slabs, 3, owned, 2 * width), bf16),
            pltpu.VMEM((owned, model), f32),
            pltpu.VMEM((owned, model), bf16),
            dma((5,)),
            dma((2,)),
            dma((11,)),
            dma((1,)),
            dma((3,)),
            dma((1,)),
            dma((units, slabs)),
            dma((1,)),
            dma((units,)),
            dma((2,)),
            dma((3, 4)),
            dma((1,)),
            dma((slabs,)),
            dma((5,)),
            dma((5,)),
            dma((1,)),
            dma((6,)),
            dma((1,)),
            dma((slabs,)),
        ],
        compiler_params=pltpu.CompilerParams(
            collective_id=0, has_side_effects=True, vmem_limit_bytes=56 * 1024 * 1024
        ),
        cost_estimate=pl.CostEstimate(
            flops=2 * positions * n * shard * units * DK,
            bytes_accessed=4 * units * shard * cols,
            transcendentals=0,
        ),
    )(
        tokens,
        gain[None, :],
        *shards,
        rate[None, :],
        extra.T,
        sgain[None, :],
        pool_mix,
        pgain[None, :],
        out_rec,
        out_pool,
        post[None, :],
    )


def per_device(
    tokens_in,
    norm_gain,
    w_query,
    w_forget,
    w_input,
    w_rgate,
    w_pool_in,
    w_pgate,
    floor_rate,
    extra_logdecay,
    state_gain,
    pool_mix,
    pool_gain,
    out_rec,
    out_pool,
    post_gain,
):
    n, n_tp, heads = lax.axis_size("sp"), lax.axis_size("tp"), extra_logdecay.shape[1]
    if n == 16 and n_tp == 2 and heads == 4:
        return pair_layer(
            tokens_in,
            norm_gain,
            [w_forget, w_query, w_input, w_pool_in, w_pgate, w_rgate],
            floor_rate,
            extra_logdecay,
            state_gain,
            pool_mix,
            pool_gain,
            out_rec,
            out_pool,
            post_gain,
        )
    shards = [w_query, w_forget, w_input, w_rgate, w_pool_in, w_pgate]
    proj = project(tokens_in, norm_gain, shards)
    return mix(
        proj,
        -jnp.expm1(-floor_rate)[None, :],
        extra_logdecay,
        state_gain[None, :],
        pool_mix,
        pool_gain[None, :],
        jnp.concatenate([out_rec, out_pool], axis=0),
        post_gain[None, :],
    )


def solution(mesh):
    placed = (
        P("sp", "tp"),
        P(),
        P("sp", "tp"),
        P("sp", "tp"),
        P("sp", "tp"),
        P("sp", "tp"),
        P("sp", "tp"),
        P("sp", "tp"),
        P("tp"),
        P("sp", "tp"),
        P("tp"),
        P("tp", None, None),
        P("tp"),
        P("tp", "sp"),
        P("tp", "sp"),
        P(),
    )
    return jax.shard_map(
        per_device, mesh=mesh, in_specs=placed, out_specs=P(("sp", "tp"), None), check_vma=False
    )
```

```python
import functools

import jax
import jax.numpy as jnp
from jax import lax
from jax.experimental import pallas as pl
from jax.experimental.pallas import tpu as pltpu
from jax.sharding import PartitionSpec as P

DK = 128


eps = 1e-06
coarsest_scale_depth = lax.Precision.HIGHEST


PIECES = 4


def ring_place(chip, chips):
    odd = chip % 2
    return (1 - odd) * (chip // 2) + odd * (chips - 1 - chip // 2)


def ring_chip(place, chips):
    back = place // (chips // 2)
    return (1 - back) * (2 * place) + back * (2 * (chips - 1 - place) + 1)


def project_kernel(
    n,
    n_tp,
    tok_ref,
    gain_ref,
    w0,
    w1,
    w2,
    w3,
    w4,
    w5,
    proj_ref,
    wide,
    scaled,
    weights,
    acc,
    tok_send,
    tok_recv,
    own_sem,
    ring_send,
    ring_recv,
    core_send,
    core_recv,
):
    chips = n // 2
    steps = chips // 2
    me = lax.axis_index("sp")
    tp = lax.axis_index("tp")
    core = me % 2
    place = ring_place(me // 2, chips)

    def chip_at(offset):
        return ring_chip((place + offset + chips) % chips, chips)

    following = 2 * chip_at(1) + core
    preceding = 2 * chip_at(-1) + core
    partner = 2 * (me // 2) + 1 - core
    parts = (w0, w1, w2, w3, w4, w5)
    rows, part_cols = w0.shape
    my_rows = pl.ds(pl.multiple_of(me * rows, 16), rows)
    owns = []
    for i, part in enumerate(parts):
        block = weights.at[my_rows, pl.ds(i * part_cols, part_cols)]
        owns.append(pltpu.make_async_copy(part, block, own_sem.at[i]))
        owns[-1].start()
    piece = rows // PIECES
    features = tok_ref.shape[1]

    barrier = pltpu.get_barrier_semaphore()
    for peer in (following, preceding, partner):
        pl.semaphore_signal(barrier, inc=1, device_id={"sp": peer})
    for turn in range(1, n_tp):
        pl.semaphore_signal(barrier, inc=1, device_id={"tp": (tp + turn) % n_tp})
    pl.semaphore_wait(barrier, 3 + n_tp - 1)

    def rows_of(chip, which, q):
        start = (2 * chip + which) * rows + q * piece
        return pl.ds(pl.multiple_of(start, 8), piece)

    sends = []

    def to_core(offset, q, source):
        slot = offset + steps - 1
        copy = pltpu.make_async_remote_copy(
            src_ref=source,
            dst_ref=weights.at[rows_of(chip_at(offset), core, q)],
            send_sem=core_send.at[slot, q],
            recv_sem=core_recv.at[slot, q],
            device_id={"sp": partner},
        )
        copy.start()
        sends.append(copy)

    def from_core(offset, q):
        slot = offset + steps - 1
        dst = weights.at[rows_of(chip_at(offset), 1 - core, q)]
        pltpu.make_async_remote_copy(
            src_ref=dst,
            dst_ref=dst,
            send_sem=core_send.at[slot, q],
            recv_sem=core_recv.at[slot, q],
            device_id={"sp": partner},
        ).wait_recv()

    def pieces_of(direction, step):
        if step < steps - 1:
            return range(PIECES)
        half = PIECES // 2
        return range(half) if direction == 0 else range(half, PIECES)

    def ring_copy(direction, step, q, source):
        offset = -step if direction == 0 else step
        dst = weights.at[rows_of(chip_at(offset), core, q)]
        return pltpu.make_async_remote_copy(
            src_ref=dst if source is None else source,
            dst_ref=dst,
            send_sem=ring_send.at[direction, step, q],
            recv_sem=ring_recv.at[direction, step, q],
            device_id={"sp": following if direction == 0 else preceding},
        )

    def ring_arrival(direction, step, q):
        offset = -(step + 1) if direction == 0 else step + 1
        dst = weights.at[rows_of(chip_at(offset), core, q)]
        pltpu.make_async_remote_copy(
            src_ref=dst,
            dst_ref=dst,
            send_sem=ring_send.at[direction, step, q],
            recv_sem=ring_recv.at[direction, step, q],
            device_id={"sp": following if direction == 0 else preceding},
        ).wait_recv()

    for own in owns:
        own.wait()
    for q in range(PIECES):
        mine = weights.at[rows_of(me // 2, core, q)]
        for direction in range(2):
            if q in pieces_of(direction, 0):
                copy = ring_copy(direction, 0, q, mine)
                copy.start()
                sends.append(copy)
        to_core(0, q, mine)
    tokens_at = pl.ds(pl.multiple_of(tp * features, 128), features)
    for turn in range(1, n_tp):
        copy = pltpu.make_async_remote_copy(
            src_ref=tok_ref,
            dst_ref=wide.at[:, tokens_at],
            send_sem=tok_send.at[turn - 1],
            recv_sem=tok_recv.at[turn - 1],
            device_id={"tp": (tp + turn) % n_tp},
        )
        copy.start()
        sends.append(copy)
    acc[...] = jnp.zeros_like(acc)
    wide[:, tokens_at] = tok_ref[...]
    for turn in range(1, n_tp):
        theirs = pl.ds(
            pl.multiple_of((tp - turn + n_tp) % n_tp * features, 128), features
        )
        pltpu.make_async_remote_copy(
            src_ref=tok_ref,
            dst_ref=wide.at[:, theirs],
            send_sem=tok_send.at[turn - 1],
            recv_sem=tok_recv.at[turn - 1],
            device_id={"tp": (tp + turn) % n_tp},
        ).wait_recv()
    scaled[...] = (wide[...].astype(jnp.float32) * gain_ref[...]).astype(jnp.bfloat16)

    cols = weights.shape[1]
    tile = cols // 6

    by_chip = (2 * rows) % 128 == 0

    def multiply(offset):
        if not by_chip:
            return
        multiply_rows(pl.ds(pl.multiple_of(chip_at(offset) * 2 * rows, 2 * rows), 2 * rows))

    def multiply_rows(depth):
        def one(i, _):
            at = pl.ds(pl.multiple_of(i * tile, 128), tile)
            acc[:, at] += jnp.dot(
                scaled[:, depth], weights[depth, at], preferred_element_type=jnp.float32
            )
            return 0

        lax.fori_loop(0, 6, one, 0)

    for step in range(steps):
        for q in range(PIECES):
            for direction in range(2):
                if q not in pieces_of(direction, step):
                    continue
                offset = -(step + 1) if direction == 0 else step + 1
                ring_arrival(direction, step, q)
                if step + 1 < steps and q in pieces_of(direction, step + 1):
                    copy = ring_copy(direction, step + 1, q, None)
                    copy.start()
                    sends.append(copy)
                last = offset if abs(offset) < steps else steps
                dst = weights.at[rows_of(chip_at(last), core, q)]
                to_core(last, q, dst)
        for offset in [0] if step == 0 else [-step, step]:
            for q in range(PIECES):
                from_core(offset, q)
            multiply(offset)
    for q in range(PIECES):
        from_core(steps, q)
    multiply(steps)
    if not by_chip:
        multiply_rows(slice(None))
    values = wide[...].astype(jnp.float32)
    squares = jnp.sum(values * values, axis=1, keepdims=True)
    inv_rms = lax.rsqrt(squares / wide.shape[1] + eps)
    proj_ref[...] = (acc[...] * inv_rms).astype(jnp.bfloat16)
    for copy in sends:
        copy.wait_send()


def project(tokens, gain, shards):
    n = lax.axis_size("sp")
    n_tp = lax.axis_size("tp")
    positions, features = tokens.shape
    rows = shards[0].shape[0]
    cols = sum(shard.shape[1] for shard in shards)
    width = n * rows
    steps = n // 4
    dma = pltpu.SemaphoreType.DMA
    return pl.pallas_call(
        functools.partial(project_kernel, n, n_tp),
        out_shape=jax.ShapeDtypeStruct((positions, cols), jnp.bfloat16),
        in_specs=[pl.BlockSpec(memory_space=pltpu.VMEM)] * 2
        + [pl.BlockSpec(memory_space=pl.ANY)] * 6,
        out_specs=pl.BlockSpec(memory_space=pltpu.VMEM),
        scratch_shapes=[
            pltpu.VMEM((positions, width), jnp.bfloat16),
            pltpu.VMEM((positions, width), jnp.bfloat16),
            pltpu.VMEM((width, cols), jnp.bfloat16),
            pltpu.VMEM((positions, cols), jnp.float32),
            dma((n_tp,)),
            dma((n_tp,)),
            dma((6,)),
            dma((2, steps, PIECES)),
            dma((2, steps, PIECES)),
            dma((2 * steps, PIECES)),
            dma((2 * steps, PIECES)),
        ],
        compiler_params=pltpu.CompilerParams(
            collective_id=0, has_side_effects=True, vmem_limit_bytes=56 * 1024 * 1024
        ),
        cost_estimate=pl.CostEstimate(
            flops=2 * positions * width * cols, bytes_accessed=4 * rows * cols, transcendentals=0
        ),
    )(tokens, gain[None, :], *shards)


def mix_kernel(
    n,
    n_tp,
    proj_ref,
    keep_ref,
    extra_ref,
    sgain_ref,
    mix_ref,
    pgain_ref,
    w_ref,
    post_ref,
    out_ref,
    weights,
    local,
    reach,
    both,
    state,
    before,
    gone_state,
    gone_decay,
    come_state,
    come_decay,
    tail,
    tail_in,
    mine,
    gone_out,
    come_out,
    ring_send,
    ring_recv,
    core_send,
    core_recv,
    scan_send,
    scan_recv,
    tail_sem,
    own_sem,
    out_send,
    out_recv,
):
    f32, bf16 = jnp.float32, jnp.bfloat16
    chips = n // 2
    steps = chips // 2
    rounds = (n - 1).bit_length()
    me = lax.axis_index("sp")
    tp = lax.axis_index("tp")
    core = me % 2
    place = ring_place(me // 2, chips)

    def chip_at(offset):
        return ring_chip((place + offset + chips) % chips, chips)

    following = 2 * chip_at(1) + core
    preceding = 2 * chip_at(-1) + core
    partner = 2 * (me // 2) + 1 - core
    piece = w_ref.shape[0] // PIECES

    barrier = pltpu.get_barrier_semaphore()
    for peer in (following, preceding, partner):
        pl.semaphore_signal(barrier, inc=1, device_id={"sp": peer})
    for r in range(rounds):
        pl.semaphore_signal(barrier, inc=1, device_id={"sp": (me + 2**r) % n})
        pl.semaphore_signal(barrier, inc=1, device_id={"sp": (me - 2**r + n) % n})
    for turn in range(1, n_tp):
        pl.semaphore_signal(barrier, inc=1, device_id={"tp": (tp + turn) % n_tp})
    pl.semaphore_wait(barrier, 3 + 2 * rounds + n_tp - 1)

    sends = []

    def spot(chip, which, q):
        return weights.at[2 * chip + which, pl.ds(q * piece, piece)]

    def to_core(offset, q, source):
        slot = offset + steps - 1
        copy = pltpu.make_async_remote_copy(
            src_ref=source,
            dst_ref=spot(chip_at(offset), core, q),
            send_sem=core_send.at[slot, q],
            recv_sem=core_recv.at[slot, q],
            device_id={"sp": partner},
        )
        copy.start()
        sends.append(copy)

    def from_core(offset, q):
        slot = offset + steps - 1
        dst = spot(chip_at(offset), 1 - core, q)
        pltpu.make_async_remote_copy(
            src_ref=dst,
            dst_ref=dst,
            send_sem=core_send.at[slot, q],
            recv_sem=core_recv.at[slot, q],
            device_id={"sp": partner},
        ).wait_recv()

    def pieces_of(direction, step):
        if step < steps - 1:
            return range(PIECES)
        half = PIECES // 2
        return range(half) if direction == 0 else range(half, PIECES)

    def ring_copy(direction, step, q, source, offset):
        dst = spot(chip_at(offset), core, q)
        return pltpu.make_async_remote_copy(
            src_ref=dst if source is None else source,
            dst_ref=dst,
            send_sem=ring_send.at[direction, step, q],
            recv_sem=ring_recv.at[direction, step, q],
            device_id={"sp": following if direction == 0 else preceding},
        )

    def ring_step(step):
        for q in range(PIECES):
            for direction in range(2):
                if q not in pieces_of(direction, step):
                    continue
                offset = -(step + 1) if direction == 0 else step + 1
                ring_copy(direction, step, q, None, offset).wait_recv()
                if step + 1 < steps and q in pieces_of(direction, step + 1):
                    copy = ring_copy(direction, step + 1, q, None, offset)
                    copy.start()
                    sends.append(copy)
                last = offset if abs(offset) < steps else steps
                to_core(last, q, spot(chip_at(last), core, q))

    pending = list(range(steps))

    def advance_ring():
        if pending:
            ring_step(pending.pop(0))

    positions = proj_ref.shape[0]
    head_cols = proj_ref.shape[1] // 6
    heads = head_cols // DK
    reach_back = tail.shape[0]

    tail[...] = proj_ref[positions - reach_back :, 4 * head_cols : 5 * head_cols]
    for q in range(PIECES):
        own_piece = w_ref.at[pl.ds(q * piece, piece)]
        for direction in range(2):
            if q in pieces_of(direction, 0):
                copy = ring_copy(direction, 0, q, own_piece, 0)
                copy.start()
                sends.append(copy)
        to_core(0, q, own_piece)
    own = pltpu.make_async_copy(w_ref, weights.at[me], own_sem)
    own.start()
    tail_copy = pltpu.make_async_remote_copy(
        src_ref=tail,
        dst_ref=tail_in,
        send_sem=tail_sem.at[0],
        recv_sem=tail_sem.at[1],
        device_id={"sp": (me + 1) % n},
    )
    tail_copy.start()

    row = lax.broadcasted_iota(jnp.int32, (positions, positions), 0)
    col = lax.broadcasted_iota(jnp.int32, (positions, positions), 1)
    lower = jnp.where(row >= col, 1.0, 0.0).astype(f32)
    line = lax.broadcasted_iota(jnp.int32, (positions, DK), 0)
    units = positions // 8
    sub = lax.broadcasted_iota(jnp.int32, (units, 8, DK), 1)
    over_last = (((1,), (1,)), ((), ()))

    decay_now = []
    for h in range(heads):
        at = slice(h * DK, (h + 1) * DK)
        part = lambda i: proj_ref[:, i * head_cols + h * DK : i * head_cols + (h + 1) * DK]
        q = part(0).astype(f32) * DK ** (-0.5)
        kg = keep_ref[:, at] * jax.nn.sigmoid(-part(1).astype(f32))
        v = part(2)
        logs = jnp.log1p(-kg) + extra_ref[:, h : h + 1]
        c = jnp.dot(
            lower, logs, precision=coarsest_scale_depth, preferred_element_type=f32
        )
        last = c[positions - 1 :, :]
        state[h] = lax.dot_general(
            v,
            (kg * jnp.exp(last - c)).astype(bf16),
            (((0,), (0,)), ((), ())),
            preferred_element_type=f32,
        )
        gone_decay[0, h : h + 1, :] = jnp.exp(last)
        reach[:, at] = (q * jnp.exp(c)).astype(bf16)
        scores = jnp.zeros((positions, positions), f32)
        span = 8
        while span < positions:
            pair = 2 * span
            c3 = c.reshape(positions // pair, pair, DK)
            middle = jnp.broadcast_to(c3[:, span - 1 : span, :], c3.shape).reshape(c.shape)
            fade = jnp.exp(-jnp.abs(c - middle))
            later = (line // span) % 2 == 1
            probe = jnp.where(later, q * fade, 0.0).astype(bf16)
            keyed = jnp.where(later, 0.0, kg * fade).astype(bf16)
            found = lax.dot_general(probe, keyed, over_last, preferred_element_type=f32)
            scores = scores + jnp.where(row // pair == col // pair, found, 0.0)
            span = pair
        result = jnp.dot(scores.astype(bf16), v, preferred_element_type=f32)
        c3 = c.reshape(units, 8, DK)
        q3 = q.reshape(units, 8, DK)
        k3 = kg.reshape(units, 8, DK)
        v3 = v.astype(f32).reshape(units, 8, DK)
        near = result.reshape(units, 8, DK)
        for s in range(8):
            weight = jnp.exp(jnp.minimum(c3 - c3[:, s : s + 1, :], 0.0))
            score = jnp.sum(q3 * k3[:, s : s + 1, :] * weight, axis=2, keepdims=True)
            near = near + jnp.where(sub >= s, score * v3[:, s : s + 1, :], 0.0)
        local[:, at] = near.reshape(positions, DK)
        if h % 2 == 1:
            advance_ring()

    def scan_copies(r):
        target = {"sp": (me + 2**r) % n}
        return [
            pltpu.make_async_remote_copy(
                src_ref=gone.at[r],
                dst_ref=come.at[r],
                send_sem=scan_send.at[r, i],
                recv_sem=scan_recv.at[r, i],
                device_id=target,
            )
            for i, (gone, come) in enumerate(
                [(gone_state, come_state), (gone_decay, come_decay)]
            )
        ]

    before[...] = jnp.zeros_like(before)
    decay_w = [gone_decay[0, h : h + 1, :] for h in range(heads)]
    decay_e = [jnp.ones((1, DK), f32) for h in range(heads)]

    def pool(h):
        at = slice(h * DK, (h + 1) * DK)
        x = proj_ref[:, 4 * head_cols + h * DK : 4 * head_cols + (h + 1) * DK].astype(f32)
        prior = jnp.where(me > 0, tail_in[:, at].astype(f32), 0.0)
        level = (tp * heads + h) % 4
        total = jnp.concatenate([prior, x], axis=0)
        chosen = jnp.zeros((positions, DK), f32)
        for k in range(4):
            total = total + pltpu.roll(total, 2**k, 0)
            chosen = jnp.where(level == k, total[reach_back:, :], chosen)
        window = 2
        for k in range(1, 4):
            window = jnp.where(level == k, 2 ** (1 + k), window)
        count = jnp.minimum(me * positions + line + 1, window).astype(f32)
        mixed = (chosen / count - x).astype(bf16)
        mapped = jnp.dot(mixed, mix_ref[h], preferred_element_type=f32)
        gate = proj_ref[:, 5 * head_cols + h * DK : 5 * head_cols + (h + 1) * DK].astype(f32)
        both[:, head_cols + h * DK : head_cols + (h + 1) * DK] = (
            mapped * pgain_ref[:, at] * (gate * jax.nn.sigmoid(gate))
        ).astype(bf16)

    pools = list(range(heads))
    for r in range(rounds):
        gone_state[r] = state[...].astype(bf16)
        if r > 0:
            for h in range(heads):
                gone_decay[r, h : h + 1, :] = decay_w[h]
        for copy in scan_copies(r):
            copy.start()
            sends.append(copy)
        if r == 0:
            tail_copy.wait_recv()
        if pools:
            pool(pools.pop(0))
        advance_ring()
        for copy in scan_copies(r):
            copy.wait_recv()
        valid = me >= 2**r
        for h in range(heads):
            came = jnp.where(valid, come_state[r, h].astype(f32), 0.0)
            came_decay = jnp.where(valid, come_decay[r, h : h + 1, :], 1.0)
            before[h] = before[h] + decay_e[h] * came
            decay_e[h] = decay_e[h] * came_decay
            if r + 1 < rounds:
                state[h] = state[h] + decay_w[h] * came
                decay_w[h] = decay_w[h] * came_decay
    for h in pools:
        pool(h)
    while pending:
        advance_ring()

    for h in range(heads):
        at = slice(h * DK, (h + 1) * DK)
        rec = local[:, at] + lax.dot_general(
            reach[:, at], before[h].astype(bf16), over_last, preferred_element_type=f32
        )
        normed = rec * lax.rsqrt(jnp.mean(rec * rec, axis=1, keepdims=True) + eps)
        gate = proj_ref[:, 3 * head_cols + h * DK : 3 * head_cols + (h + 1) * DK].astype(f32)
        both[:, at] = (normed * sgain_ref[:, at] * (gate * jax.nn.sigmoid(gate))).astype(bf16)

    own.wait()
    for offset in range(-(steps - 1), steps + 1):
        for q in range(PIECES):
            from_core(offset, q)

    owned = positions // n_tp
    width = w_ref.shape[1]
    quarter = n // 4

    def share(rows, group):
        left = both[rows, :]
        for slot in range(group * quarter, (group + 1) * quarter, 2):
            right = jnp.concatenate([weights[slot], weights[slot + 1]], axis=1)
            yield slot, jnp.dot(left, right, preferred_element_type=f32).astype(bf16)

    def out_copy(turn, group):
        cols = pl.ds(group * quarter * width, quarter * width)
        return pltpu.make_async_remote_copy(
            src_ref=gone_out.at[turn - 1, :, cols],
            dst_ref=come_out.at[turn - 1, :, cols],
            send_sem=out_send.at[turn - 1, group],
            recv_sem=out_recv.at[turn - 1, group],
            device_id={"tp": (tp + turn) % n_tp},
        )

    for turn in range(1, n_tp):
        target = (tp + turn) % n_tp
        rows = pl.ds(pl.multiple_of(target * owned, owned), owned)
        for group in range(4):
            for slot, value in share(rows, group):
                gone_out[turn - 1, :, slot * width : (slot + 2) * width] = value
            copy = out_copy(turn, group)
            copy.start()
            sends.append(copy)
    rows = pl.ds(pl.multiple_of(tp * owned, owned), owned)
    for group in range(4):
        for slot, value in share(rows, group):
            mine[:, slot * width : (slot + 2) * width] = value.astype(f32)
    for turn in range(1, n_tp):
        for group in range(4):
            out_copy(turn, group).wait_recv()
        mine[...] += come_out[turn - 1].astype(f32)
    summed = mine[...]
    out_ref[...] = (
        summed
        * lax.rsqrt(jnp.mean(summed * summed, axis=1, keepdims=True) + eps)
        * post_ref[...]
    ).astype(bf16)
    tail_copy.wait_send()
    for copy in sends:
        copy.wait_send()


def mix(proj, keep, extra, sgain, pool_mix, pgain, shard, post):
    n = lax.axis_size("sp")
    n_tp = lax.axis_size("tp")
    positions, heads = extra.shape
    head_cols = heads * DK
    depth, width = shard.shape
    steps = n // 4
    rounds = (n - 1).bit_length()
    owned = positions // n_tp
    model = n * width
    padded = -(-heads // 8) * 8
    f32, bf16, dma = jnp.float32, jnp.bfloat16, pltpu.SemaphoreType.DMA
    return pl.pallas_call(
        functools.partial(mix_kernel, n, n_tp),
        out_shape=jax.ShapeDtypeStruct((owned, model), bf16),
        in_specs=[pl.BlockSpec(memory_space=pltpu.VMEM)] * 8,
        out_specs=pl.BlockSpec(memory_space=pltpu.VMEM),
        scratch_shapes=[
            pltpu.VMEM((n, depth, width), bf16),
            pltpu.VMEM((positions, head_cols), f32),
            pltpu.VMEM((positions, head_cols), bf16),
            pltpu.VMEM((positions, 2 * head_cols), bf16),
            pltpu.VMEM((heads, DK, DK), f32),
            pltpu.VMEM((heads, DK, DK), f32),
            pltpu.VMEM((rounds, heads, DK, DK), bf16),
            pltpu.VMEM((rounds, padded, DK), f32),
            pltpu.VMEM((rounds, heads, DK, DK), bf16),
            pltpu.VMEM((rounds, padded, DK), f32),
            pltpu.VMEM((16, head_cols), bf16),
            pltpu.VMEM((16, head_cols), bf16),
            pltpu.VMEM((owned, model), f32),
            pltpu.VMEM((n_tp, owned, model), bf16),
            pltpu.VMEM((n_tp, owned, model), bf16),
            dma((2, steps, PIECES)),
            dma((2, steps, PIECES)),
            dma((2 * steps, PIECES)),
            dma((2 * steps, PIECES)),
            dma((rounds, 2)),
            dma((rounds, 2)),
            dma((2,)),
            dma,
            dma((n_tp, 4)),
            dma((n_tp, 4)),
        ],
        compiler_params=pltpu.CompilerParams(
            collective_id=1, has_side_effects=True, vmem_limit_bytes=56 * 1024 * 1024
        ),
        cost_estimate=pl.CostEstimate(
            flops=2 * positions * depth * model, bytes_accessed=4 * depth * width, transcendentals=0
        ),
    )(proj, keep, extra, sgain, pool_mix, pgain, shard, post)


def pair_kernel(
    tok_hbm,
    gain_ref,
    w0,
    w1,
    w2,
    w3,
    w4,
    w5,
    rate_ref,
    extra_hbm,
    sgain_ref,
    mix_hbm,
    pgain_ref,
    orec_hbm,
    opool_hbm,
    post_ref,
    out_ref,
    wide,
    scaled,
    inv_rms,
    w_own,
    w_all,
    o_all,
    extra,
    mix_own,
    proj,
    local,
    reach,
    faded,
    kept,
    scored,
    state,
    state_go,
    state_come,
    decay_go,
    decay_come,
    tail_go,
    tail_come,
    total_go,
    total_come,
    last_come,
    y_all,
    y_go,
    part_go,
    part_come,
    mine,
    done,
    own_sem,
    tok_send,
    tok_recv,
    extra_send,
    extra_recv,
    w_send,
    w_recv,
    wy_send,
    wy_recv,
    o_send,
    o_recv,
    oy_send,
    oy_recv,
    scan_send,
    scan_recv,
    y_send,
    y_recv,
    part_send,
    part_recv,
):
    f32, bf16 = jnp.float32, jnp.bfloat16
    me = lax.axis_index("sp")
    x = lax.axis_index("tp")
    z, y, c = me // 4, (me // 2) % 2, me % 2
    odd = z % 2
    pair = z // 2
    head = odd * 2 + c
    is_mid = (z == 1) | (z == 2)
    is_end = jnp.logical_not(is_mid)
    slabs = [z, z + 1 - 2 * odd, 2 - pair, 3 * (1 - pair)]
    my_slot = jnp.where(is_mid, 2, 3)
    rows, feats = tok_hbm.shape
    shard = w0.shape[0]
    parts = (w0, w1, w2, w3, w4, w5)
    units = len(parts)
    positions = wide.shape[0]
    half = positions // 2
    block = rows
    blocks = positions // block
    n_rows = w_all.shape[1]
    tok_pieces = 4
    piece = rows // tok_pieces

    def peer(zz, yy, cc):
        return {"sp": zz * 4 + yy * 2 + cc}

    def peer_x(cc):
        return {"sp": z * 4 + y * 2 + cc, "tp": 1 - x}

    other_c = peer(z, y, 1 - c)
    other_y = peer(z, 1 - y, c)

    def lanes(i, n=1):
        return pl.ds(pl.multiple_of(i * DK, DK), n * DK)

    def own_rows(base, size):
        return pl.ds(pl.multiple_of(base, 16), size)

    def tok_at(zq, cc, xx, q):
        start = zq * half + cc * rows + q * piece
        return wide.at[own_rows(start, piece), pl.ds(pl.multiple_of(xx * feats, 128), feats)]

    owns = {}

    def own_copy(name, src, dst):
        copy = pltpu.make_async_copy(src, dst, own_sem.at[len(owns)])
        copy.start()
        owns[name] = copy

    own_tok = wide.at[
        own_rows(odd * half + c * rows, rows), pl.ds(pl.multiple_of(x * feats, 128), feats)
    ]
    own_copy("tok", tok_hbm, own_tok)
    own_copy("extra", extra_hbm, extra.at[odd * 2 + c])
    here = z * 2 + y
    w_landed = own_sem.at[2]
    for u, part in enumerate(parts):
        pltpu.make_async_copy(part, w_own.at[u], w_landed).start()
    o_landed = own_sem.at[3]
    pltpu.make_async_copy(orec_hbm, o_all.at[here, pl.ds(0, 4 * DK)], o_landed).start()
    pltpu.make_async_copy(opool_hbm, o_all.at[here, pl.ds(4 * DK, 4 * DK)], o_landed).start()
    mix_copy = pltpu.make_async_copy(mix_hbm.at[head], mix_own, own_sem.at[4])
    mix_copy.start()

    barrier = pltpu.get_barrier_semaphore()
    across = peer((z + 2) % 4, y, c)
    across_y = peer((z + 2) % 4, 1 - y, c)
    peers = [other_c, other_y, peer_x(c), peer_x(1 - c), across_y]
    for k in range(1, 4):
        peers += [peer(slabs[k], y, c), peer(slabs[k], y, 1 - c)]
    for to in peers:
        pl.semaphore_signal(barrier, inc=1, device_id=to)
    pl.semaphore_wait(barrier, len(peers))

    def send(src, dst, send_sem, recv_sem, to):
        pltpu.make_async_remote_copy(
            src_ref=src, dst_ref=dst, send_sem=send_sem, recv_sem=recv_sem, device_id=to
        ).start()

    def sent(ref, send_sem):
        pltpu.make_async_remote_copy(
            src_ref=ref, dst_ref=ref, send_sem=send_sem, recv_sem=send_sem, device_id=other_c
        ).wait_send()

    def arrive(ref, recv_sem):
        pltpu.make_async_remote_copy(
            src_ref=ref, dst_ref=ref, send_sem=recv_sem, recv_sem=recv_sem, device_id=other_c
        ).wait_recv()

    def tok_rows(zq, cc, xx):
        start = zq * half + cc * rows
        return wide.at[own_rows(start, rows), pl.ds(pl.multiple_of(xx * feats, 128), feats)]

    def tok_share(at, near):
        send(at, at, tok_send.at[1], tok_recv.at[9 if near else 10], other_c)

    owns["extra"].wait()
    for e, to in enumerate([other_c, peer(slabs[1], y, c), peer(slabs[1], y, 1 - c)]):
        at = extra.at[odd * 2 + c]
        send(at, at, extra_send.at[0], extra_recv.at[e], to)
    owns["tok"].wait()
    for q in range(tok_pieces):
        at = tok_at(odd, c, x, q)
        send(at, at, tok_send.at[0], tok_recv.at[q], peer(slabs[1], y, c))
    send(own_tok, own_tok, tok_send.at[1], tok_recv.at[8], peer_x(c))
    tok_share(own_tok, True)

    def w_piece(slab, cc, n=1):
        return own_rows((slab * 4 + y * 2 + cc) * shard, n * shard)

    def send_copy(src, dst, send_sem, recv_sem, to):
        return pltpu.make_async_remote_copy(
            src_ref=src, dst_ref=dst, send_sem=send_sem, recv_sem=recv_sem, device_id=to
        )

    def w_send_to(u, k, only=None):
        copies = []
        for e in range(2):
            cc = c if e == 0 else 1 - c
            slot = 1 if k == 1 else my_slot
            copies.append(
                send_copy(
                    w_own.at[u, :, lanes((slabs[k] % 2) * 2 + cc)],
                    w_all.at[u, w_piece(z, c)],
                    w_send.at[0],
                    w_recv.at[u, slot],
                    peer(slabs[k], y, cc),
                )
            )
        issue(copies, only)

    def issue(copies, only=None):
        if only is None:
            for copy in copies:
                copy.start()
        else:

            @pl.when(only)
            def _():
                for copy in copies:
                    copy.start()

    pltpu.make_async_copy(w_own, w_own, w_landed).wait()
    for u in range(units):
        pltpu.make_async_copy(
            w_own.at[u, :, lanes(head)], w_all.at[u, w_piece(z, c)], w_recv.at[u, 0]
        ).start()
        send(
            w_own.at[u, :, lanes(odd * 2 + 1 - c)],
            w_all.at[u, w_piece(z, c)],
            w_send.at[0],
            w_recv.at[u, 0],
            other_c,
        )
        w_send_to(u, 1, None if u == 0 else is_mid)
        w_send_to(u, 2, is_mid)

    def w_relay(u, k):
        at = w_all.at[u, w_piece(slabs[k], 0, 2)]
        arrive(at, w_recv.at[u, k])
        send(at, at, wy_send.at[0], wy_recv.at[u], other_y)

    def w_late_end():
        for u in range(units):
            w_send_to(u, 3, is_end)
            w_send_to(u, 2, is_end)
            if u > 0:
                w_send_to(u, 1, is_end)

    def w_late_mid():
        for u in range(units):
            w_send_to(u, 3, is_mid)

    def w_need(u):
        arrive(w_all.at[u, pl.ds(0, n_rows // 2)], wy_recv.at[u])

    pieces = 4
    depth = o_all.shape[1] // pieces

    def o_at(slab, yy, part):
        return o_all.at[slab * 2 + yy, pl.ds(part * depth, depth)]

    def o_copy(route, part, held, slot, to):
        at = o_at(held, y, part)
        return send_copy(
            at, at, o_send.at[min(route, 1)], o_recv.at[slot - 1, part], peer(to, y, c)
        )

    def o_near():
        for part in range(pieces):
            o_copy(0, part, z, 1, slabs[1]).start()

    def o_across(which):
        @pl.when(is_mid)
        def _():
            for part in which:
                o_copy(1, part, z, 2, slabs[2]).start()

    def o_relay(k, part):
        at = o_at(slabs[k], y, part)
        if k > 0:
            arrive(at, o_recv.at[k - 1, part])
        send(at, at, oy_send.at[0], oy_recv.at[k], other_y)

    def o_onward(k, part):
        if k == 1:
            o_copy(2, part, slabs[1], 3, slabs[2]).start()
        else:
            o_copy(k + 1, part, slabs[k], k, slabs[1]).start()

    def o_near_relays(which):
        for part in which:
            o_relay(1, part)

            @pl.when(is_mid)
            def _():
                o_onward(1, part)

    def o_mid_relays(k, which):
        @pl.when(is_mid)
        def _():
            for part in which:
                o_relay(k, part)
                o_onward(k, part)

    def o_end_relays(k, which):
        @pl.when(is_end)
        def _():
            for part in which:
                o_relay(k, part)

    def o_need(k):
        arrive(o_all.at[slabs[k] * 2 + 1 - y], oy_recv.at[k])

    for u in range(units):
        w_relay(u, 0)
    pltpu.make_async_copy(o_all.at[here], o_all.at[here], o_landed).wait()

    def tok_z(q):
        at = tok_at(1 - odd, c, x, q)
        arrive(at, tok_recv.at[q])
        send(at, at, tok_send.at[1], tok_recv.at[4 + q], peer_x(c))
        tok_share(at, False)

    def tok_x():
        at = tok_rows(odd, c, 1 - x)
        arrive(at, tok_recv.at[8])
        tok_share(at, True)

    def tok_diagonal(q):
        at = tok_at(1 - odd, c, 1 - x, q)
        arrive(at, tok_recv.at[4 + q])
        tok_share(at, False)

    def tok_shared(zq, near):
        arrive(wide.at[own_rows(zq * half + (1 - c) * rows, rows)], tok_recv.at[9 if near else 10])

    def scale(zq, cc):
        at = own_rows(zq * half + cc * rows, rows)
        values = wide[at, :].astype(f32)
        scaled[at, :] = (values * gain_ref[...]).astype(bf16)
        squares = jnp.sum(values * values, axis=1, keepdims=True)
        inv_rms[at, :] = jnp.broadcast_to(
            lax.rsqrt(squares / wide.shape[1] + eps), (rows, DK)
        )

    def w_relays(u):
        w_relay(u, 1)
        w_relay(u, 2)
        w_relay(u, 3)

    tok_z(0)
    tok_z(1)
    w_late_end()
    for part in range(pieces):
        o_relay(0, part)
    tok_z(2)
    sent(own_tok, tok_send.at[0])
    w_late_mid()
    tok_z(3)
    tok_x()
    scale(odd, c)
    tok_shared(odd, True)
    scale(odd, 1 - c)
    w_relay(0, 2)
    w_relay(0, 1)
    w_relay(0, 3)
    tok_diagonal(0)
    tok_diagonal(1)
    w_relay(1, 1)
    tok_diagonal(2)
    w_relay(1, 2)
    tok_diagonal(3)
    w_relay(1, 3)
    scale(1 - odd, c)
    tok_shared(1 - odd, False)
    scale(1 - odd, 1 - c)
    w_relays(2)

    def project_units(first, count):
        def one(i, _):
            at = own_rows(i * block, block)
            right = [w_all[u] for u in range(first, first + count)]
            right = right[0] if count == 1 else jnp.concatenate(right, axis=1)
            acc = jnp.dot(scaled[at, :], right, preferred_element_type=f32)
            norm = inv_rms[at, :]
            for j in range(count):
                proj[first + j, at, :] = (acc[:, j * DK : (j + 1) * DK] * norm).astype(bf16)
            return 0

        lax.fori_loop(0, blocks, one, 0)

    w_need(0)
    w_need(1)
    project_units(0, 2)
    for e, (zq, cc) in enumerate([(odd, 1 - c), (1 - odd, c), (1 - odd, 1 - c)]):
        arrive(extra.at[zq * 2 + cc], extra_recv.at[e])

    rate = rate_ref[:, lanes(head)]
    series = jnp.ones_like(rate)
    for n in range(10, 1, -1):
        series = 1.0 - series * rate / n
    keep = jnp.where(rate < 0.5, rate * series, 1.0 - jnp.exp(-rate))

    row = lax.broadcasted_iota(jnp.int32, (block, block), 0)
    col = lax.broadcasted_iota(jnp.int32, (block, block), 1)
    lower = jnp.where(row >= col, 1.0, 0.0).astype(f32)
    line = lax.broadcasted_iota(jnp.int32, (block, DK), 0)
    eighths = block // 8
    sub = lax.broadcasted_iota(jnp.int32, (eighths, 8, DK), 1)
    over_last = (((1,), (1,)), ((), ()))
    decays = []

    def score_block(b):
        at = slice(b * block, (b + 1) * block)
        q = proj[1, at, :].astype(f32) * DK ** (-0.5)
        kg = keep * jax.nn.sigmoid(-proj[0, at, :].astype(f32))
        added = jnp.broadcast_to(extra[b, pl.ds(head, 1), :], (DK, block)).T
        logs = jnp.log1p(-kg) + added
        cum = jnp.dot(lower, logs, precision=coarsest_scale_depth, preferred_element_type=f32)
        last = cum[block - 1 :, :]
        faded[at, :] = (kg * jnp.exp(last - cum)).astype(bf16)
        decays.append(jnp.exp(last))
        reach[at, :] = (q * jnp.exp(cum)).astype(bf16)
        kept[0, at, :] = cum
        kept[1, at, :] = kg
        scores = jnp.zeros((block, block), f32)
        span = 8
        while span < block:
            twice = 2 * span
            c3 = cum.reshape(block // twice, twice, DK)
            middle = jnp.broadcast_to(c3[:, span - 1 : span, :], c3.shape).reshape(cum.shape)
            fade = jnp.exp(-jnp.abs(cum - middle))
            later = (line // span) % 2 == 1
            probe = jnp.where(later, q * fade, 0.0).astype(bf16)
            keyed = jnp.where(later, 0.0, kg * fade).astype(bf16)
            found = lax.dot_general(probe, keyed, over_last, preferred_element_type=f32)
            scores = scores + jnp.where(row // twice == col // twice, found, 0.0)
            span = twice
        scored[b] = scores.astype(bf16)

    def value_block(b):
        at = slice(b * block, (b + 1) * block)
        q = proj[1, at, :].astype(f32) * DK ** (-0.5)
        v = proj[2, at, :]
        state[b] = lax.dot_general(
            v, faded[at, :], (((0,), (0,)), ((), ())), preferred_element_type=f32
        )
        result = jnp.dot(scored[b], v, preferred_element_type=f32)
        c3 = kept[0, at, :].reshape(eighths, 8, DK)
        q3 = q.reshape(eighths, 8, DK)
        k3 = kept[1, at, :].reshape(eighths, 8, DK)
        v3 = v.astype(f32).reshape(eighths, 8, DK)
        near = result.reshape(eighths, 8, DK)
        for s in range(8):
            weight = jnp.exp(jnp.minimum(c3 - c3[:, s : s + 1, :], 0.0))
            score = jnp.sum(q3 * k3[:, s : s + 1, :] * weight, axis=2, keepdims=True)
            near = near + jnp.where(sub >= s, score * v3[:, s : s + 1, :], 0.0)
        local[at, :] = near.reshape(block, DK)

    score_block(0)
    w_relays(3)
    score_block(1)
    score_block(2)
    score_block(3)
    w_relays(4)
    o_near()
    o_across(range(pieces))
    w_need(2)
    project_units(2, 1)
    for b in range(blocks):
        value_block(b)

    sums = [decays[2 * i + 1] * state[2 * i] + state[2 * i + 1] for i in range(2)]
    fades = [decays[2 * i] * decays[2 * i + 1] for i in range(2)]
    for i in range(2):
        state_go[i] = sums[i].astype(bf16)
        decay_go[i : i + 1, :] = fades[i]
    send(state_go, state_come, scan_send.at[0], scan_recv.at[0], other_y)
    send(decay_go, decay_come, scan_send.at[1], scan_recv.at[1], other_y)
    w_need(3)
    project_units(3, 1)
    for i in range(2):
        tail_go[i] = proj[3, (i + 1) * half - 16 : (i + 1) * half, :]
    send(tail_go, tail_come, scan_send.at[2], scan_recv.at[2], other_y)
    send(tail_go.at[1], last_come, scan_send.at[4], scan_recv.at[4], across_y)
    w_relays(5)
    w_need(4)
    project_units(4, 1)
    o_near_relays(range(2))
    o_mid_relays(2, range(2))

    arrive(state_come, scan_recv.at[0])
    arrive(decay_come, scan_recv.at[1])
    first_y = y == 0
    theirs = [state_come[i].astype(f32) for i in range(2)]
    their_fades = [decay_come[i : i + 1, :] for i in range(2)]
    order = []
    for i in range(2):
        order.append(
            (jnp.where(first_y, sums[i], theirs[i]), jnp.where(first_y, fades[i], their_fades[i]))
        )
        order.append(
            (jnp.where(first_y, theirs[i], sums[i]), jnp.where(first_y, their_fades[i], fades[i]))
        )
    total = order[0][0]
    for add, fade in order[1:]:
        total = fade * total + add
    total_go[...] = total.astype(bf16)
    send(total_go, total_come, scan_send.at[3], scan_recv.at[3], across)
    mix_copy.wait()
    arrive(tail_come, scan_recv.at[2])
    arrive(last_come, scan_recv.at[4])

    later_pair = pair > 0
    at_head = lanes(head)
    level = (x * 4 + head) % 4
    window = 2
    for k in range(1, 4):
        window = jnp.where(level == k, 2 ** (1 + k), window)
    line_half = lax.broadcasted_iota(jnp.int32, (half, DK), 0)
    far = [jnp.where(later_pair, last_come[...].astype(f32), 0.0), tail_come[0].astype(f32)]
    their_tails = [tail_come[i].astype(f32) for i in range(2)]
    is_odd = odd == 1

    def pool_half(i):
        at_static = slice(i * half, (i + 1) * half)
        xin = proj[3, at_static, :].astype(f32)
        prior = jnp.where(first_y, far[i], their_tails[i])
        sums_in = jnp.concatenate([prior, xin], axis=0)
        chosen = jnp.zeros((half, DK), f32)
        for k in range(4):
            sums_in = sums_in + pltpu.roll(sums_in, 2**k, 0)
            chosen = jnp.where(level == k, sums_in[16:, :], chosen)
        begins = (4 * pair + 2 * i + y) * half
        count = jnp.minimum(begins + line_half + 1, window).astype(f32)
        mixed = (chosen / count - xin).astype(bf16)
        mapped = jnp.dot(mixed, mix_own[...], preferred_element_type=f32)
        gate = proj[4, at_static, :].astype(f32)
        return mapped * pgain_ref[:, at_head] * (gate * jax.nn.sigmoid(gate))

    z_peer = peer(slabs[1], y, c)
    their_head = (1 - odd) * 2 + c

    def y_at(part, hd, ch):
        return y_all.at[part * 4 + hd, pl.ds(ch * block, block)]

    def y_put(part, ch, low, high):
        at = slice(ch * block, (ch + 1) * block)
        y_go[part, at, :] = jnp.where(is_odd, low, high).astype(bf16)
        y_all[part * 4 + head, at, :] = jnp.where(is_odd, high, low).astype(bf16)
        send(
            y_go.at[part, pl.ds(ch * block, block)],
            y_at(part, head, ch),
            y_send.at[0],
            y_recv.at[part * 2 + ch],
            z_peer,
        )
        at = y_at(part, head, ch)
        send(at, at, y_send.at[0], y_recv.at[4 + ch], other_c)

    def y_pass(part, ch):
        at = y_at(part, their_head, ch)
        arrive(at, y_recv.at[part * 2 + ch])
        send(at, at, y_send.at[0], y_recv.at[4 + ch], other_c)

    def y_need(ch):
        arrive(y_all.at[pl.ds(0, 2)], y_recv.at[4 + ch])

    pooled = [pool_half(i) for i in range(2)]
    for ch in range(2):
        rows_ch = slice(ch * block, (ch + 1) * block)
        y_put(1, ch, pooled[0][rows_ch], pooled[1][rows_ch])
    o_near_relays(range(2, pieces))
    w_need(5)
    project_units(5, 1)
    arrive(total_come, scan_recv.at[3])
    befores = []
    running = jnp.where(later_pair, total_come[...].astype(f32), 0.0)
    for i in range(2):
        after_first = order[2 * i][1] * running + order[2 * i][0]
        befores.append(jnp.where(first_y, running, after_first))
        running = order[2 * i + 1][1] * after_first + order[2 * i + 1][0]

    def rec_rows(b, before):
        rows_b = slice(b * block, (b + 1) * block)
        rec = local[rows_b, :] + lax.dot_general(
            reach[rows_b, :], before.astype(bf16), over_last, preferred_element_type=f32
        )
        normed = rec * lax.rsqrt(jnp.mean(rec * rec, axis=1, keepdims=True) + eps)
        gate = proj[5, rows_b, :].astype(f32)
        return normed * sgain_ref[:, at_head] * (gate * jax.nn.sigmoid(gate))

    for ch in range(2):
        recs = []
        for i in range(2):
            b = 2 * i + ch
            recs.append(rec_rows(b, befores[i]))
            befores[i] = decays[b] * befores[i] + state[b]
        y_put(0, ch, recs[0], recs[1])
    o_mid_relays(2, range(2, pieces))
    for ch in range(2):
        y_pass(1, ch)
    o_mid_relays(3, range(2))
    o_end_relays(2, range(2))
    y_pass(0, 0)
    o_mid_relays(3, range(2, pieces))
    o_end_relays(2, range(2, pieces))
    y_pass(0, 1)

    owned = part_come.shape[2]

    def rows_for(xx, cc):
        return own_rows(cc * rows + xx * owned, owned)

    def part_copies(k, ch):
        over_x = send_copy(
            part_go.at[k, rows_for(1 - x, ch)],
            part_come.at[k, c],
            part_send.at[0],
            part_recv.at[k],
            peer_x(ch),
        )
        over_c = send_copy(
            part_go.at[k, rows_for(x, ch)],
            part_come.at[k, 2],
            part_send.at[0],
            part_recv.at[k],
            other_c,
        )
        return over_x, over_c

    def out_chunk(k, ch):
        left = jnp.concatenate(
            [y_all[i, ch * block : (ch + 1) * block, :] for i in range(8)], axis=1
        )
        right = jnp.concatenate([o_all[slabs[k] * 2], o_all[slabs[k] * 2 + 1]], axis=1)
        part_go[k, ch * block : (ch + 1) * block, :] = jnp.dot(
            left, right, preferred_element_type=f32
        ).astype(bf16)
        over_x, over_c = part_copies(k, ch)
        over_x.start()

        @pl.when(c != ch)
        def _():
            over_c.start()

    def drain():
        sent(wide.at[pl.ds(0, 6 * rows // 2)], tok_send.at[1])
        sent(extra.at[pl.ds(0, 3)], extra_send.at[0])
        sent(w_all.at[pl.ds(0, 3), pl.ds(0, 14 * shard)], w_send.at[0])
        sent(w_all.at[pl.ds(0, 3)], wy_send.at[0])
        sent(o_all.at[0], o_send.at[0])
        sent(o_all.at[pl.ds(0, 4)], oy_send.at[0])

        @pl.when(is_mid)
        def _():
            sent(o_all.at[pl.ds(0, 4)], o_send.at[1])

        for i, ref in enumerate([state_go, decay_go, tail_go, total_go, tail_go.at[1]]):
            sent(ref, scan_send.at[i])
        sent(y_all.at[pl.ds(0, 6)], y_send.at[0])

    def gather_chunk(k):
        arrive(part_come.at[k], part_recv.at[k])
        ours = part_go[k, rows_for(x, c), :].astype(f32) + part_come[k, c].astype(f32)
        others = part_come[k, 2].astype(f32) + part_come[k, 1 - c].astype(f32)
        for yy in range(2):
            cols = slice(yy * DK, (yy + 1) * DK)
            mine[:, lanes(slabs[k] * 4 + yy * 2 + c)] = ours[:, cols]
            mine[:, lanes(slabs[k] * 4 + yy * 2 + 1 - c)] = others[:, cols]

    for ch in range(2):
        y_need(ch)
        for k in range(2):
            if ch == 0:
                o_need(k)
            out_chunk(k, ch)
    o_need(2)
    for ch in range(2):
        o_end_relays(3, range(ch, ch + 1))
        out_chunk(2, ch)
    o_end_relays(3, range(2, pieces))
    o_need(3)
    for ch in range(2):
        out_chunk(3, ch)
    drain()
    for k in range(len(slabs)):
        gather_chunk(k)

    def finish():
        summed = mine[...]
        done[...] = (
            summed
            * lax.rsqrt(jnp.mean(summed * summed, axis=1, keepdims=True) + eps)
            * post_ref[...]
        ).astype(bf16)
        copy = pltpu.make_async_copy(done, out_ref, own_sem.at[0])
        copy.start()
        copy.wait()

    finish()
    sent(part_go.at[pl.ds(0, 3)], part_send.at[0])


def pair_layer(
    tokens,
    gain,
    shards,
    rate,
    extra,
    sgain,
    pool_mix,
    pgain,
    out_rec,
    out_pool,
    post,
):
    n = lax.axis_size("sp")
    n_tp = lax.axis_size("tp")
    rows, feats = tokens.shape
    shard, cols = shards[0].shape
    heads = cols // DK
    depth, width = out_rec.shape
    slabs = n // 4
    positions = 4 * rows
    half = 2 * rows
    owned = rows // n_tp
    model = n * width
    f32, bf16, dma = jnp.float32, jnp.bfloat16, pltpu.SemaphoreType.DMA
    units = len(shards)
    vmem, hbm = pl.BlockSpec(memory_space=pltpu.VMEM), pl.BlockSpec(memory_space=pl.ANY)
    return pl.pallas_call(
        pair_kernel,
        out_shape=jax.ShapeDtypeStruct((owned, model), bf16),
        in_specs=[hbm, vmem] + [hbm] * 6 + [vmem, hbm, vmem, hbm, vmem, hbm, hbm, vmem],
        out_specs=hbm,
        scratch_shapes=[
            pltpu.VMEM((positions, n_tp * feats), bf16),
            pltpu.VMEM((positions, n_tp * feats), bf16),
            pltpu.VMEM((positions, DK), f32),
            pltpu.VMEM((units, shard, cols), bf16),
            pltpu.VMEM((units, n * shard, DK), bf16),
            pltpu.VMEM((2 * slabs, 2 * depth, width), bf16),
            pltpu.VMEM((4, heads, rows), f32),
            pltpu.VMEM((DK, DK), bf16),
            pltpu.VMEM((units, positions, DK), bf16),
            pltpu.VMEM((positions, DK), f32),
            pltpu.VMEM((positions, DK), bf16),
            pltpu.VMEM((positions, DK), bf16),
            pltpu.VMEM((2, positions, DK), f32),
            pltpu.VMEM((4, rows, rows), bf16),
            pltpu.VMEM((4, DK, DK), f32),
            pltpu.VMEM((2, DK, DK), bf16),
            pltpu.VMEM((2, DK, DK), bf16),
            pltpu.VMEM((8, DK), f32),
            pltpu.VMEM((8, DK), f32),
            pltpu.VMEM((2, 16, DK), bf16),
            pltpu.VMEM((2, 16, DK), bf16),
            pltpu.VMEM((DK, DK), bf16),
            pltpu.VMEM((DK, DK), bf16),
            pltpu.VMEM((16, DK), bf16),
            pltpu.VMEM((2 * heads, half, DK), bf16),
            pltpu.VMEM((2, half, DK), bf16),
            pltpu.VMEM((slabs, half, 2 * width), bf16),
            pltpu.VMEM((slabs, 3, owned, 2 * width), bf16),
            pltpu.VMEM((owned, model), f32),
            pltpu.VMEM((owned, model), bf16),
            dma((5,)),
            dma((2,)),
            dma((11,)),
            dma((1,)),
            dma((3,)),
            dma((1,)),
            dma((units, slabs)),
            dma((1,)),
            dma((units,)),
            dma((2,)),
            dma((3, 4)),
            dma((1,)),
            dma((slabs,)),
            dma((5,)),
            dma((5,)),
            dma((1,)),
            dma((6,)),
            dma((1,)),
            dma((slabs,)),
        ],
        compiler_params=pltpu.CompilerParams(
            collective_id=0, has_side_effects=True, vmem_limit_bytes=56 * 1024 * 1024
        ),
        cost_estimate=pl.CostEstimate(
            flops=2 * positions * n * shard * units * DK,
            bytes_accessed=4 * units * shard * cols,
            transcendentals=0,
        ),
    )(
        tokens,
        gain[None, :],
        *shards,
        rate[None, :],
        extra.T,
        sgain[None, :],
        pool_mix,
        pgain[None, :],
        out_rec,
        out_pool,
        post[None, :],
    )


def per_device(
    tokens_in,
    norm_gain,
    w_query,
    w_forget,
    w_input,
    w_rgate,
    w_pool_in,
    w_pgate,
    floor_rate,
    extra_logdecay,
    state_gain,
    pool_mix,
    pool_gain,
    out_rec,
    out_pool,
    post_gain,
):
    n, n_tp, heads = lax.axis_size("sp"), lax.axis_size("tp"), extra_logdecay.shape[1]
    if n == 16 and n_tp == 2 and heads == 4:
        return pair_layer(
            tokens_in,
            norm_gain,
            [w_forget, w_query, w_input, w_pool_in, w_pgate, w_rgate],
            floor_rate,
            extra_logdecay,
            state_gain,
            pool_mix,
            pool_gain,
            out_rec,
            out_pool,
            post_gain,
        )
    shards = [w_query, w_forget, w_input, w_rgate, w_pool_in, w_pgate]
    proj = project(tokens_in, norm_gain, shards)
    return mix(
        proj,
        -jnp.expm1(-floor_rate)[None, :],
        extra_logdecay,
        state_gain[None, :],
        pool_mix,
        pool_gain[None, :],
        jnp.concatenate([out_rec, out_pool], axis=0),
        post_gain[None, :],
    )


def solution(mesh):
    placed = (
        P("sp", "tp"),
        P(),
        P("sp", "tp"),
        P("sp", "tp"),
        P("sp", "tp"),
        P("sp", "tp"),
        P("sp", "tp"),
        P("sp", "tp"),
        P("tp"),
        P("sp", "tp"),
        P("tp"),
        P("tp", None, None),
        P("tp"),
        P("tp", "sp"),
        P("tp", "sp"),
        P(),
    )
    return jax.shard_map(
        per_device, mesh=mesh, in_specs=placed, out_specs=P(("sp", "tp"), None), check_vma=False
    )
```

```python
import functools

import jax
import jax.numpy as jnp
from jax import lax
from jax.experimental import pallas as pl
from jax.experimental.pallas import tpu as pltpu
from jax.sharding import PartitionSpec as P

DK = 128


eps = 1e-06
coarsest_scale_depth = lax.Precision.HIGHEST


PIECES = 4


def ring_place(chip, chips):
    odd = chip % 2
    return (1 - odd) * (chip // 2) + odd * (chips - 1 - chip // 2)


def ring_chip(place, chips):
    back = place // (chips // 2)
    return (1 - back) * (2 * place) + back * (2 * (chips - 1 - place) + 1)


def project_kernel(
    n,
    n_tp,
    tok_ref,
    gain_ref,
    w0,
    w1,
    w2,
    w3,
    w4,
    w5,
    proj_ref,
    wide,
    scaled,
    weights,
    acc,
    tok_send,
    tok_recv,
    own_sem,
    ring_send,
    ring_recv,
    core_send,
    core_recv,
):
    chips = n // 2
    steps = chips // 2
    me = lax.axis_index("sp")
    tp = lax.axis_index("tp")
    core = me % 2
    place = ring_place(me // 2, chips)

    def chip_at(offset):
        return ring_chip((place + offset + chips) % chips, chips)

    following = 2 * chip_at(1) + core
    preceding = 2 * chip_at(-1) + core
    partner = 2 * (me // 2) + 1 - core
    parts = (w0, w1, w2, w3, w4, w5)
    rows, part_cols = w0.shape
    my_rows = pl.ds(pl.multiple_of(me * rows, 16), rows)
    owns = []
    for i, part in enumerate(parts):
        block = weights.at[my_rows, pl.ds(i * part_cols, part_cols)]
        owns.append(pltpu.make_async_copy(part, block, own_sem.at[i]))
        owns[-1].start()
    piece = rows // PIECES
    features = tok_ref.shape[1]

    barrier = pltpu.get_barrier_semaphore()
    for peer in (following, preceding, partner):
        pl.semaphore_signal(barrier, inc=1, device_id={"sp": peer})
    for turn in range(1, n_tp):
        pl.semaphore_signal(barrier, inc=1, device_id={"tp": (tp + turn) % n_tp})
    pl.semaphore_wait(barrier, 3 + n_tp - 1)

    def rows_of(chip, which, q):
        start = (2 * chip + which) * rows + q * piece
        return pl.ds(pl.multiple_of(start, 8), piece)

    sends = []

    def to_core(offset, q, source):
        slot = offset + steps - 1
        copy = pltpu.make_async_remote_copy(
            src_ref=source,
            dst_ref=weights.at[rows_of(chip_at(offset), core, q)],
            send_sem=core_send.at[slot, q],
            recv_sem=core_recv.at[slot, q],
            device_id={"sp": partner},
        )
        copy.start()
        sends.append(copy)

    def from_core(offset, q):
        slot = offset + steps - 1
        dst = weights.at[rows_of(chip_at(offset), 1 - core, q)]
        pltpu.make_async_remote_copy(
            src_ref=dst,
            dst_ref=dst,
            send_sem=core_send.at[slot, q],
            recv_sem=core_recv.at[slot, q],
            device_id={"sp": partner},
        ).wait_recv()

    def pieces_of(direction, step):
        if step < steps - 1:
            return range(PIECES)
        half = PIECES // 2
        return range(half) if direction == 0 else range(half, PIECES)

    def ring_copy(direction, step, q, source):
        offset = -step if direction == 0 else step
        dst = weights.at[rows_of(chip_at(offset), core, q)]
        return pltpu.make_async_remote_copy(
            src_ref=dst if source is None else source,
            dst_ref=dst,
            send_sem=ring_send.at[direction, step, q],
            recv_sem=ring_recv.at[direction, step, q],
            device_id={"sp": following if direction == 0 else preceding},
        )

    def ring_arrival(direction, step, q):
        offset = -(step + 1) if direction == 0 else step + 1
        dst = weights.at[rows_of(chip_at(offset), core, q)]
        pltpu.make_async_remote_copy(
            src_ref=dst,
            dst_ref=dst,
            send_sem=ring_send.at[direction, step, q],
            recv_sem=ring_recv.at[direction, step, q],
            device_id={"sp": following if direction == 0 else preceding},
        ).wait_recv()

    for own in owns:
        own.wait()
    for q in range(PIECES):
        mine = weights.at[rows_of(me // 2, core, q)]
        for direction in range(2):
            if q in pieces_of(direction, 0):
                copy = ring_copy(direction, 0, q, mine)
                copy.start()
                sends.append(copy)
        to_core(0, q, mine)
    tokens_at = pl.ds(pl.multiple_of(tp * features, 128), features)
    for turn in range(1, n_tp):
        copy = pltpu.make_async_remote_copy(
            src_ref=tok_ref,
            dst_ref=wide.at[:, tokens_at],
            send_sem=tok_send.at[turn - 1],
            recv_sem=tok_recv.at[turn - 1],
            device_id={"tp": (tp + turn) % n_tp},
        )
        copy.start()
        sends.append(copy)
    acc[...] = jnp.zeros_like(acc)
    wide[:, tokens_at] = tok_ref[...]
    for turn in range(1, n_tp):
        theirs = pl.ds(
            pl.multiple_of((tp - turn + n_tp) % n_tp * features, 128), features
        )
        pltpu.make_async_remote_copy(
            src_ref=tok_ref,
            dst_ref=wide.at[:, theirs],
            send_sem=tok_send.at[turn - 1],
            recv_sem=tok_recv.at[turn - 1],
            device_id={"tp": (tp + turn) % n_tp},
        ).wait_recv()
    scaled[...] = (wide[...].astype(jnp.float32) * gain_ref[...]).astype(jnp.bfloat16)

    cols = weights.shape[1]
    tile = cols // 6

    by_chip = (2 * rows) % 128 == 0

    def multiply(offset):
        if not by_chip:
            return
        multiply_rows(pl.ds(pl.multiple_of(chip_at(offset) * 2 * rows, 2 * rows), 2 * rows))

    def multiply_rows(depth):
        def one(i, _):
            at = pl.ds(pl.multiple_of(i * tile, 128), tile)
            acc[:, at] += jnp.dot(
                scaled[:, depth], weights[depth, at], preferred_element_type=jnp.float32
            )
            return 0

        lax.fori_loop(0, 6, one, 0)

    for step in range(steps):
        for q in range(PIECES):
            for direction in range(2):
                if q not in pieces_of(direction, step):
                    continue
                offset = -(step + 1) if direction == 0 else step + 1
                ring_arrival(direction, step, q)
                if step + 1 < steps and q in pieces_of(direction, step + 1):
                    copy = ring_copy(direction, step + 1, q, None)
                    copy.start()
                    sends.append(copy)
                last = offset if abs(offset) < steps else steps
                dst = weights.at[rows_of(chip_at(last), core, q)]
                to_core(last, q, dst)
        for offset in [0] if step == 0 else [-step, step]:
            for q in range(PIECES):
                from_core(offset, q)
            multiply(offset)
    for q in range(PIECES):
        from_core(steps, q)
    multiply(steps)
    if not by_chip:
        multiply_rows(slice(None))
    values = wide[...].astype(jnp.float32)
    squares = jnp.sum(values * values, axis=1, keepdims=True)
    inv_rms = lax.rsqrt(squares / wide.shape[1] + eps)
    proj_ref[...] = (acc[...] * inv_rms).astype(jnp.bfloat16)
    for copy in sends:
        copy.wait_send()


def project(tokens, gain, shards):
    n = lax.axis_size("sp")
    n_tp = lax.axis_size("tp")
    positions, features = tokens.shape
    rows = shards[0].shape[0]
    cols = sum(shard.shape[1] for shard in shards)
    width = n * rows
    steps = n // 4
    dma = pltpu.SemaphoreType.DMA
    return pl.pallas_call(
        functools.partial(project_kernel, n, n_tp),
        out_shape=jax.ShapeDtypeStruct((positions, cols), jnp.bfloat16),
        in_specs=[pl.BlockSpec(memory_space=pltpu.VMEM)] * 2
        + [pl.BlockSpec(memory_space=pl.ANY)] * 6,
        out_specs=pl.BlockSpec(memory_space=pltpu.VMEM),
        scratch_shapes=[
            pltpu.VMEM((positions, width), jnp.bfloat16),
            pltpu.VMEM((positions, width), jnp.bfloat16),
            pltpu.VMEM((width, cols), jnp.bfloat16),
            pltpu.VMEM((positions, cols), jnp.float32),
            dma((n_tp,)),
            dma((n_tp,)),
            dma((6,)),
            dma((2, steps, PIECES)),
            dma((2, steps, PIECES)),
            dma((2 * steps, PIECES)),
            dma((2 * steps, PIECES)),
        ],
        compiler_params=pltpu.CompilerParams(
            collective_id=0, has_side_effects=True, vmem_limit_bytes=56 * 1024 * 1024
        ),
        cost_estimate=pl.CostEstimate(
            flops=2 * positions * width * cols, bytes_accessed=4 * rows * cols, transcendentals=0
        ),
    )(tokens, gain[None, :], *shards)


def mix_kernel(
    n,
    n_tp,
    proj_ref,
    keep_ref,
    extra_ref,
    sgain_ref,
    mix_ref,
    pgain_ref,
    w_ref,
    post_ref,
    out_ref,
    weights,
    local,
    reach,
    both,
    state,
    before,
    gone_state,
    gone_decay,
    come_state,
    come_decay,
    tail,
    tail_in,
    mine,
    gone_out,
    come_out,
    ring_send,
    ring_recv,
    core_send,
    core_recv,
    scan_send,
    scan_recv,
    tail_sem,
    own_sem,
    out_send,
    out_recv,
):
    f32, bf16 = jnp.float32, jnp.bfloat16
    chips = n // 2
    steps = chips // 2
    rounds = (n - 1).bit_length()
    me = lax.axis_index("sp")
    tp = lax.axis_index("tp")
    core = me % 2
    place = ring_place(me // 2, chips)

    def chip_at(offset):
        return ring_chip((place + offset + chips) % chips, chips)

    following = 2 * chip_at(1) + core
    preceding = 2 * chip_at(-1) + core
    partner = 2 * (me // 2) + 1 - core
    piece = w_ref.shape[0] // PIECES

    barrier = pltpu.get_barrier_semaphore()
    for peer in (following, preceding, partner):
        pl.semaphore_signal(barrier, inc=1, device_id={"sp": peer})
    for r in range(rounds):
        pl.semaphore_signal(barrier, inc=1, device_id={"sp": (me + 2**r) % n})
        pl.semaphore_signal(barrier, inc=1, device_id={"sp": (me - 2**r + n) % n})
    for turn in range(1, n_tp):
        pl.semaphore_signal(barrier, inc=1, device_id={"tp": (tp + turn) % n_tp})
    pl.semaphore_wait(barrier, 3 + 2 * rounds + n_tp - 1)

    sends = []

    def spot(chip, which, q):
        return weights.at[2 * chip + which, pl.ds(q * piece, piece)]

    def to_core(offset, q, source):
        slot = offset + steps - 1
        copy = pltpu.make_async_remote_copy(
            src_ref=source,
            dst_ref=spot(chip_at(offset), core, q),
            send_sem=core_send.at[slot, q],
            recv_sem=core_recv.at[slot, q],
            device_id={"sp": partner},
        )
        copy.start()
        sends.append(copy)

    def from_core(offset, q):
        slot = offset + steps - 1
        dst = spot(chip_at(offset), 1 - core, q)
        pltpu.make_async_remote_copy(
            src_ref=dst,
            dst_ref=dst,
            send_sem=core_send.at[slot, q],
            recv_sem=core_recv.at[slot, q],
            device_id={"sp": partner},
        ).wait_recv()

    def pieces_of(direction, step):
        if step < steps - 1:
            return range(PIECES)
        half = PIECES // 2
        return range(half) if direction == 0 else range(half, PIECES)

    def ring_copy(direction, step, q, source, offset):
        dst = spot(chip_at(offset), core, q)
        return pltpu.make_async_remote_copy(
            src_ref=dst if source is None else source,
            dst_ref=dst,
            send_sem=ring_send.at[direction, step, q],
            recv_sem=ring_recv.at[direction, step, q],
            device_id={"sp": following if direction == 0 else preceding},
        )

    def ring_step(step):
        for q in range(PIECES):
            for direction in range(2):
                if q not in pieces_of(direction, step):
                    continue
                offset = -(step + 1) if direction == 0 else step + 1
                ring_copy(direction, step, q, None, offset).wait_recv()
                if step + 1 < steps and q in pieces_of(direction, step + 1):
                    copy = ring_copy(direction, step + 1, q, None, offset)
                    copy.start()
                    sends.append(copy)
                last = offset if abs(offset) < steps else steps
                to_core(last, q, spot(chip_at(last), core, q))

    pending = list(range(steps))

    def advance_ring():
        if pending:
            ring_step(pending.pop(0))

    positions = proj_ref.shape[0]
    head_cols = proj_ref.shape[1] // 6
    heads = head_cols // DK
    reach_back = tail.shape[0]

    tail[...] = proj_ref[positions - reach_back :, 4 * head_cols : 5 * head_cols]
    for q in range(PIECES):
        own_piece = w_ref.at[pl.ds(q * piece, piece)]
        for direction in range(2):
            if q in pieces_of(direction, 0):
                copy = ring_copy(direction, 0, q, own_piece, 0)
                copy.start()
                sends.append(copy)
        to_core(0, q, own_piece)
    own = pltpu.make_async_copy(w_ref, weights.at[me], own_sem)
    own.start()
    tail_copy = pltpu.make_async_remote_copy(
        src_ref=tail,
        dst_ref=tail_in,
        send_sem=tail_sem.at[0],
        recv_sem=tail_sem.at[1],
        device_id={"sp": (me + 1) % n},
    )
    tail_copy.start()

    row = lax.broadcasted_iota(jnp.int32, (positions, positions), 0)
    col = lax.broadcasted_iota(jnp.int32, (positions, positions), 1)
    lower = jnp.where(row >= col, 1.0, 0.0).astype(f32)
    line = lax.broadcasted_iota(jnp.int32, (positions, DK), 0)
    units = positions // 8
    sub = lax.broadcasted_iota(jnp.int32, (units, 8, DK), 1)
    over_last = (((1,), (1,)), ((), ()))

    decay_now = []
    for h in range(heads):
        at = slice(h * DK, (h + 1) * DK)
        part = lambda i: proj_ref[:, i * head_cols + h * DK : i * head_cols + (h + 1) * DK]
        q = part(0).astype(f32) * DK ** (-0.5)
        kg = keep_ref[:, at] * jax.nn.sigmoid(-part(1).astype(f32))
        v = part(2)
        logs = jnp.log1p(-kg) + extra_ref[:, h : h + 1]
        c = jnp.dot(
            lower, logs, precision=coarsest_scale_depth, preferred_element_type=f32
        )
        last = c[positions - 1 :, :]
        state[h] = lax.dot_general(
            v,
            (kg * jnp.exp(last - c)).astype(bf16),
            (((0,), (0,)), ((), ())),
            preferred_element_type=f32,
        )
        gone_decay[0, h : h + 1, :] = jnp.exp(last)
        reach[:, at] = (q * jnp.exp(c)).astype(bf16)
        scores = jnp.zeros((positions, positions), f32)
        span = 8
        while span < positions:
            pair = 2 * span
            c3 = c.reshape(positions // pair, pair, DK)
            middle = jnp.broadcast_to(c3[:, span - 1 : span, :], c3.shape).reshape(c.shape)
            fade = jnp.exp(-jnp.abs(c - middle))
            later = (line // span) % 2 == 1
            probe = jnp.where(later, q * fade, 0.0).astype(bf16)
            keyed = jnp.where(later, 0.0, kg * fade).astype(bf16)
            found = lax.dot_general(probe, keyed, over_last, preferred_element_type=f32)
            scores = scores + jnp.where(row // pair == col // pair, found, 0.0)
            span = pair
        result = jnp.dot(scores.astype(bf16), v, preferred_element_type=f32)
        c3 = c.reshape(units, 8, DK)
        q3 = q.reshape(units, 8, DK)
        k3 = kg.reshape(units, 8, DK)
        v3 = v.astype(f32).reshape(units, 8, DK)
        near = result.reshape(units, 8, DK)
        for s in range(8):
            weight = jnp.exp(jnp.minimum(c3 - c3[:, s : s + 1, :], 0.0))
            score = jnp.sum(q3 * k3[:, s : s + 1, :] * weight, axis=2, keepdims=True)
            near = near + jnp.where(sub >= s, score * v3[:, s : s + 1, :], 0.0)
        local[:, at] = near.reshape(positions, DK)
        if h % 2 == 1:
            advance_ring()

    def scan_copies(r):
        target = {"sp": (me + 2**r) % n}
        return [
            pltpu.make_async_remote_copy(
                src_ref=gone.at[r],
                dst_ref=come.at[r],
                send_sem=scan_send.at[r, i],
                recv_sem=scan_recv.at[r, i],
                device_id=target,
            )
            for i, (gone, come) in enumerate(
                [(gone_state, come_state), (gone_decay, come_decay)]
            )
        ]

    before[...] = jnp.zeros_like(before)
    decay_w = [gone_decay[0, h : h + 1, :] for h in range(heads)]
    decay_e = [jnp.ones((1, DK), f32) for h in range(heads)]

    def pool(h):
        at = slice(h * DK, (h + 1) * DK)
        x = proj_ref[:, 4 * head_cols + h * DK : 4 * head_cols + (h + 1) * DK].astype(f32)
        prior = jnp.where(me > 0, tail_in[:, at].astype(f32), 0.0)
        level = (tp * heads + h) % 4
        total = jnp.concatenate([prior, x], axis=0)
        chosen = jnp.zeros((positions, DK), f32)
        for k in range(4):
            total = total + pltpu.roll(total, 2**k, 0)
            chosen = jnp.where(level == k, total[reach_back:, :], chosen)
        window = 2
        for k in range(1, 4):
            window = jnp.where(level == k, 2 ** (1 + k), window)
        count = jnp.minimum(me * positions + line + 1, window).astype(f32)
        mixed = (chosen / count - x).astype(bf16)
        mapped = jnp.dot(mixed, mix_ref[h], preferred_element_type=f32)
        gate = proj_ref[:, 5 * head_cols + h * DK : 5 * head_cols + (h + 1) * DK].astype(f32)
        both[:, head_cols + h * DK : head_cols + (h + 1) * DK] = (
            mapped * pgain_ref[:, at] * (gate * jax.nn.sigmoid(gate))
        ).astype(bf16)

    pools = list(range(heads))
    for r in range(rounds):
        gone_state[r] = state[...].astype(bf16)
        if r > 0:
            for h in range(heads):
                gone_decay[r, h : h + 1, :] = decay_w[h]
        for copy in scan_copies(r):
            copy.start()
            sends.append(copy)
        if r == 0:
            tail_copy.wait_recv()
        if pools:
            pool(pools.pop(0))
        advance_ring()
        for copy in scan_copies(r):
            copy.wait_recv()
        valid = me >= 2**r
        for h in range(heads):
            came = jnp.where(valid, come_state[r, h].astype(f32), 0.0)
            came_decay = jnp.where(valid, come_decay[r, h : h + 1, :], 1.0)
            before[h] = before[h] + decay_e[h] * came
            decay_e[h] = decay_e[h] * came_decay
            if r + 1 < rounds:
                state[h] = state[h] + decay_w[h] * came
                decay_w[h] = decay_w[h] * came_decay
    for h in pools:
        pool(h)
    while pending:
        advance_ring()

    for h in range(heads):
        at = slice(h * DK, (h + 1) * DK)
        rec = local[:, at] + lax.dot_general(
            reach[:, at], before[h].astype(bf16), over_last, preferred_element_type=f32
        )
        normed = rec * lax.rsqrt(jnp.mean(rec * rec, axis=1, keepdims=True) + eps)
        gate = proj_ref[:, 3 * head_cols + h * DK : 3 * head_cols + (h + 1) * DK].astype(f32)
        both[:, at] = (normed * sgain_ref[:, at] * (gate * jax.nn.sigmoid(gate))).astype(bf16)

    own.wait()
    for offset in range(-(steps - 1), steps + 1):
        for q in range(PIECES):
            from_core(offset, q)

    owned = positions // n_tp
    width = w_ref.shape[1]
    quarter = n // 4

    def share(rows, group):
        left = both[rows, :]
        for slot in range(group * quarter, (group + 1) * quarter, 2):
            right = jnp.concatenate([weights[slot], weights[slot + 1]], axis=1)
            yield slot, jnp.dot(left, right, preferred_element_type=f32).astype(bf16)

    def out_copy(turn, group):
        cols = pl.ds(group * quarter * width, quarter * width)
        return pltpu.make_async_remote_copy(
            src_ref=gone_out.at[turn - 1, :, cols],
            dst_ref=come_out.at[turn - 1, :, cols],
            send_sem=out_send.at[turn - 1, group],
            recv_sem=out_recv.at[turn - 1, group],
            device_id={"tp": (tp + turn) % n_tp},
        )

    for turn in range(1, n_tp):
        target = (tp + turn) % n_tp
        rows = pl.ds(pl.multiple_of(target * owned, owned), owned)
        for group in range(4):
            for slot, value in share(rows, group):
                gone_out[turn - 1, :, slot * width : (slot + 2) * width] = value
            copy = out_copy(turn, group)
            copy.start()
            sends.append(copy)
    rows = pl.ds(pl.multiple_of(tp * owned, owned), owned)
    for group in range(4):
        for slot, value in share(rows, group):
            mine[:, slot * width : (slot + 2) * width] = value.astype(f32)
    for turn in range(1, n_tp):
        for group in range(4):
            out_copy(turn, group).wait_recv()
        mine[...] += come_out[turn - 1].astype(f32)
    summed = mine[...]
    out_ref[...] = (
        summed
        * lax.rsqrt(jnp.mean(summed * summed, axis=1, keepdims=True) + eps)
        * post_ref[...]
    ).astype(bf16)
    tail_copy.wait_send()
    for copy in sends:
        copy.wait_send()


def mix(proj, keep, extra, sgain, pool_mix, pgain, shard, post):
    n = lax.axis_size("sp")
    n_tp = lax.axis_size("tp")
    positions, heads = extra.shape
    head_cols = heads * DK
    depth, width = shard.shape
    steps = n // 4
    rounds = (n - 1).bit_length()
    owned = positions // n_tp
    model = n * width
    padded = -(-heads // 8) * 8
    f32, bf16, dma = jnp.float32, jnp.bfloat16, pltpu.SemaphoreType.DMA
    return pl.pallas_call(
        functools.partial(mix_kernel, n, n_tp),
        out_shape=jax.ShapeDtypeStruct((owned, model), bf16),
        in_specs=[pl.BlockSpec(memory_space=pltpu.VMEM)] * 8,
        out_specs=pl.BlockSpec(memory_space=pltpu.VMEM),
        scratch_shapes=[
            pltpu.VMEM((n, depth, width), bf16),
            pltpu.VMEM((positions, head_cols), f32),
            pltpu.VMEM((positions, head_cols), bf16),
            pltpu.VMEM((positions, 2 * head_cols), bf16),
            pltpu.VMEM((heads, DK, DK), f32),
            pltpu.VMEM((heads, DK, DK), f32),
            pltpu.VMEM((rounds, heads, DK, DK), bf16),
            pltpu.VMEM((rounds, padded, DK), f32),
            pltpu.VMEM((rounds, heads, DK, DK), bf16),
            pltpu.VMEM((rounds, padded, DK), f32),
            pltpu.VMEM((16, head_cols), bf16),
            pltpu.VMEM((16, head_cols), bf16),
            pltpu.VMEM((owned, model), f32),
            pltpu.VMEM((n_tp, owned, model), bf16),
            pltpu.VMEM((n_tp, owned, model), bf16),
            dma((2, steps, PIECES)),
            dma((2, steps, PIECES)),
            dma((2 * steps, PIECES)),
            dma((2 * steps, PIECES)),
            dma((rounds, 2)),
            dma((rounds, 2)),
            dma((2,)),
            dma,
            dma((n_tp, 4)),
            dma((n_tp, 4)),
        ],
        compiler_params=pltpu.CompilerParams(
            collective_id=1, has_side_effects=True, vmem_limit_bytes=56 * 1024 * 1024
        ),
        cost_estimate=pl.CostEstimate(
            flops=2 * positions * depth * model, bytes_accessed=4 * depth * width, transcendentals=0
        ),
    )(proj, keep, extra, sgain, pool_mix, pgain, shard, post)


def pair_kernel(
    tok_hbm,
    gain_ref,
    w0,
    w1,
    w2,
    w3,
    w4,
    w5,
    rate_ref,
    extra_hbm,
    sgain_ref,
    mix_hbm,
    pgain_ref,
    orec_hbm,
    opool_hbm,
    post_ref,
    out_ref,
    wide,
    scaled,
    inv_rms,
    w_own,
    w_all,
    o_all,
    extra,
    mix_own,
    proj,
    local,
    reach,
    faded,
    kept,
    scored,
    state,
    state_go,
    state_come,
    decay_go,
    decay_come,
    tail_go,
    tail_come,
    total_go,
    total_come,
    last_come,
    y_all,
    y_go,
    part_go,
    part_come,
    mine,
    done,
    own_sem,
    tok_send,
    tok_recv,
    extra_send,
    extra_recv,
    w_send,
    w_recv,
    wy_send,
    wy_recv,
    o_send,
    o_recv,
    oy_send,
    oy_recv,
    scan_send,
    scan_recv,
    y_send,
    y_recv,
    part_send,
    part_recv,
):
    f32, bf16 = jnp.float32, jnp.bfloat16
    me = lax.axis_index("sp")
    x = lax.axis_index("tp")
    z, y, c = me // 4, (me // 2) % 2, me % 2
    odd = z % 2
    pair = z // 2
    head = odd * 2 + c
    is_mid = (z == 1) | (z == 2)
    is_end = jnp.logical_not(is_mid)
    slabs = [z, z + 1 - 2 * odd, 2 - pair, 3 * (1 - pair)]
    my_slot = jnp.where(is_mid, 2, 3)
    rows, feats = tok_hbm.shape
    shard = w0.shape[0]
    parts = (w0, w1, w2, w3, w4, w5)
    units = len(parts)
    positions = wide.shape[0]
    half = positions // 2
    block = rows
    blocks = positions // block
    n_rows = w_all.shape[1]
    tok_pieces = 4
    piece = rows // tok_pieces

    def peer(zz, yy, cc):
        return {"sp": zz * 4 + yy * 2 + cc}

    def peer_x(cc):
        return {"sp": z * 4 + y * 2 + cc, "tp": 1 - x}

    other_c = peer(z, y, 1 - c)
    other_y = peer(z, 1 - y, c)

    def lanes(i, n=1):
        return pl.ds(pl.multiple_of(i * DK, DK), n * DK)

    def own_rows(base, size):
        return pl.ds(pl.multiple_of(base, 16), size)

    def tok_at(zq, cc, xx, q):
        start = zq * half + cc * rows + q * piece
        return wide.at[own_rows(start, piece), pl.ds(pl.multiple_of(xx * feats, 128), feats)]

    owns = {}

    def own_copy(name, src, dst):
        copy = pltpu.make_async_copy(src, dst, own_sem.at[len(owns)])
        copy.start()
        owns[name] = copy

    own_tok = wide.at[
        own_rows(odd * half + c * rows, rows), pl.ds(pl.multiple_of(x * feats, 128), feats)
    ]
    own_copy("tok", tok_hbm, own_tok)
    own_copy("extra", extra_hbm, extra.at[odd * 2 + c])
    here = z * 2 + y
    w_landed = own_sem.at[2]
    for u, part in enumerate(parts):
        pltpu.make_async_copy(part, w_own.at[u], w_landed).start()
    o_landed = own_sem.at[3]
    pltpu.make_async_copy(orec_hbm, o_all.at[here, pl.ds(0, 4 * DK)], o_landed).start()
    pltpu.make_async_copy(opool_hbm, o_all.at[here, pl.ds(4 * DK, 4 * DK)], o_landed).start()
    mix_copy = pltpu.make_async_copy(mix_hbm.at[head], mix_own, own_sem.at[4])
    mix_copy.start()

    barrier = pltpu.get_barrier_semaphore()
    across = peer((z + 2) % 4, y, c)
    across_y = peer((z + 2) % 4, 1 - y, c)
    peers = [other_c, other_y, peer_x(c), peer_x(1 - c), across_y]
    for k in range(1, 4):
        peers += [peer(slabs[k], y, c), peer(slabs[k], y, 1 - c)]
    for to in peers:
        pl.semaphore_signal(barrier, inc=1, device_id=to)
    pl.semaphore_wait(barrier, len(peers))

    def send(src, dst, send_sem, recv_sem, to):
        pltpu.make_async_remote_copy(
            src_ref=src, dst_ref=dst, send_sem=send_sem, recv_sem=recv_sem, device_id=to
        ).start()

    def sent(ref, send_sem):
        pltpu.make_async_remote_copy(
            src_ref=ref, dst_ref=ref, send_sem=send_sem, recv_sem=send_sem, device_id=other_c
        ).wait_send()

    def arrive(ref, recv_sem):
        pltpu.make_async_remote_copy(
            src_ref=ref, dst_ref=ref, send_sem=recv_sem, recv_sem=recv_sem, device_id=other_c
        ).wait_recv()

    def tok_rows(zq, cc, xx):
        start = zq * half + cc * rows
        return wide.at[own_rows(start, rows), pl.ds(pl.multiple_of(xx * feats, 128), feats)]

    def tok_share(at, near):
        send(at, at, tok_send.at[1], tok_recv.at[9 if near else 10], other_c)

    owns["extra"].wait()
    for e, to in enumerate([other_c, peer(slabs[1], y, c), peer(slabs[1], y, 1 - c)]):
        at = extra.at[odd * 2 + c]
        send(at, at, extra_send.at[0], extra_recv.at[e], to)
    owns["tok"].wait()
    for q in range(tok_pieces):
        at = tok_at(odd, c, x, q)
        send(at, at, tok_send.at[0], tok_recv.at[q], peer(slabs[1], y, c))
    send(own_tok, own_tok, tok_send.at[1], tok_recv.at[8], peer_x(c))
    tok_share(own_tok, True)

    def w_piece(slab, cc, n=1):
        return own_rows((slab * 4 + y * 2 + cc) * shard, n * shard)

    def send_copy(src, dst, send_sem, recv_sem, to):
        return pltpu.make_async_remote_copy(
            src_ref=src, dst_ref=dst, send_sem=send_sem, recv_sem=recv_sem, device_id=to
        )

    ahead = 1

    def w_send_to(u, k, only=None):
        copies = []
        for e in range(2):
            cc = c if e == 0 else 1 - c
            slot = 1 if k == 1 else my_slot
            copies.append(
                send_copy(
                    w_own.at[u, :, lanes((slabs[k] % 2) * 2 + cc)],
                    w_all.at[u, w_piece(z, c)],
                    w_send.at[0],
                    w_recv.at[u, slot],
                    peer(slabs[k], y, cc),
                )
            )
        issue(copies, only)

    def issue(copies, only=None):
        if only is None:
            for copy in copies:
                copy.start()
        else:

            @pl.when(only)
            def _():
                for copy in copies:
                    copy.start()

    pltpu.make_async_copy(w_own, w_own, w_landed).wait()
    for u in range(units):
        pltpu.make_async_copy(
            w_own.at[u, :, lanes(head)], w_all.at[u, w_piece(z, c)], w_recv.at[u, 0]
        ).start()
        send(
            w_own.at[u, :, lanes(odd * 2 + 1 - c)],
            w_all.at[u, w_piece(z, c)],
            w_send.at[0],
            w_recv.at[u, 0],
            other_c,
        )
        w_send_to(u, 1, None if u == 0 else is_mid)
        w_send_to(u, 2, is_mid)
        if u < ahead:
            w_send_to(u, 3, is_mid)

    def w_relay(u, k):
        at = w_all.at[u, w_piece(slabs[k], 0, 2)]
        arrive(at, w_recv.at[u, k])
        send(at, at, wy_send.at[0], wy_recv.at[u], other_y)

    def w_late_end():
        for u in range(units):
            w_send_to(u, 3, is_end)
            w_send_to(u, 2, is_end)
            if u > 0:
                w_send_to(u, 1, is_end)

    def w_late_mid():
        for u in range(ahead, units):
            w_send_to(u, 3, is_mid)

    def w_need(u):
        arrive(w_all.at[u, pl.ds(0, n_rows // 2)], wy_recv.at[u])

    pieces = 4
    depth = o_all.shape[1] // pieces

    def o_at(slab, yy, part):
        return o_all.at[slab * 2 + yy, pl.ds(part * depth, depth)]

    def o_copy(route, part, held, slot, to):
        at = o_at(held, y, part)
        return send_copy(
            at, at, o_send.at[min(route, 1)], o_recv.at[slot - 1, part], peer(to, y, c)
        )

    def o_near():
        for part in range(pieces):
            o_copy(0, part, z, 1, slabs[1]).start()

    def o_across(which):
        @pl.when(is_mid)
        def _():
            for part in which:
                o_copy(1, part, z, 2, slabs[2]).start()

    def o_relay(k, part):
        at = o_at(slabs[k], y, part)
        if k > 0:
            arrive(at, o_recv.at[k - 1, part])
        send(at, at, oy_send.at[0], oy_recv.at[k], other_y)

    def o_onward(k, part):
        if k == 1:
            o_copy(2, part, slabs[1], 3, slabs[2]).start()
        else:
            o_copy(k + 1, part, slabs[k], k, slabs[1]).start()

    def o_near_relays(which):
        for part in which:
            o_relay(1, part)

            @pl.when(is_mid)
            def _():
                o_onward(1, part)

    def o_mid_relays(k, which):
        @pl.when(is_mid)
        def _():
            for part in which:
                o_relay(k, part)
                o_onward(k, part)

    def o_end_relays(k, which):
        @pl.when(is_end)
        def _():
            for part in which:
                o_relay(k, part)

    def o_need(k):
        arrive(o_all.at[slabs[k] * 2 + 1 - y], oy_recv.at[k])

    for u in range(units):
        w_relay(u, 0)
    pltpu.make_async_copy(o_all.at[here], o_all.at[here], o_landed).wait()

    def tok_z(q):
        at = tok_at(1 - odd, c, x, q)
        arrive(at, tok_recv.at[q])
        send(at, at, tok_send.at[1], tok_recv.at[4 + q], peer_x(c))
        tok_share(at, False)

    def tok_x():
        at = tok_rows(odd, c, 1 - x)
        arrive(at, tok_recv.at[8])
        tok_share(at, True)

    def tok_diagonal(q):
        at = tok_at(1 - odd, c, 1 - x, q)
        arrive(at, tok_recv.at[4 + q])
        tok_share(at, False)

    def tok_shared(zq, near):
        arrive(wide.at[own_rows(zq * half + (1 - c) * rows, rows)], tok_recv.at[9 if near else 10])

    def scale(zq, cc):
        at = own_rows(zq * half + cc * rows, rows)
        values = wide[at, :].astype(f32)
        scaled[at, :] = (values * gain_ref[...]).astype(bf16)
        squares = jnp.sum(values * values, axis=1, keepdims=True)
        inv_rms[at, :] = jnp.broadcast_to(
            lax.rsqrt(squares / wide.shape[1] + eps), (rows, DK)
        )

    def w_relays(u):
        w_relay(u, 1)
        w_relay(u, 2)
        w_relay(u, 3)

    tok_z(0)
    tok_z(1)
    w_late_end()
    for part in range(pieces):
        o_relay(0, part)
    tok_z(2)
    sent(own_tok, tok_send.at[0])
    w_late_mid()
    tok_z(3)
    tok_x()
    scale(odd, c)
    tok_shared(odd, True)
    scale(odd, 1 - c)
    w_relay(0, 2)
    w_relay(0, 1)
    w_relay(0, 3)
    tok_diagonal(0)
    tok_diagonal(1)
    tok_diagonal(2)
    w_relay(1, 1)
    w_relay(1, 2)
    tok_diagonal(3)
    w_relay(1, 3)
    scale(1 - odd, c)
    tok_shared(1 - odd, False)
    scale(1 - odd, 1 - c)
    w_relays(2)

    def project_units(first, count):
        def one(i, _):
            at = own_rows(i * block, block)
            right = [w_all[u] for u in range(first, first + count)]
            right = right[0] if count == 1 else jnp.concatenate(right, axis=1)
            acc = jnp.dot(scaled[at, :], right, preferred_element_type=f32)
            norm = inv_rms[at, :]
            for j in range(count):
                proj[first + j, at, :] = (acc[:, j * DK : (j + 1) * DK] * norm).astype(bf16)
            return 0

        lax.fori_loop(0, blocks, one, 0)

    w_need(0)
    w_need(1)
    project_units(0, 2)
    for e, (zq, cc) in enumerate([(odd, 1 - c), (1 - odd, c), (1 - odd, 1 - c)]):
        arrive(extra.at[zq * 2 + cc], extra_recv.at[e])

    rate = rate_ref[:, lanes(head)]
    series = jnp.ones_like(rate)
    for n in range(10, 1, -1):
        series = 1.0 - series * rate / n
    keep = jnp.where(rate < 0.5, rate * series, 1.0 - jnp.exp(-rate))

    row = lax.broadcasted_iota(jnp.int32, (block, block), 0)
    col = lax.broadcasted_iota(jnp.int32, (block, block), 1)
    lower = jnp.where(row >= col, 1.0, 0.0).astype(f32)
    line = lax.broadcasted_iota(jnp.int32, (block, DK), 0)
    eighths = block // 8
    sub = lax.broadcasted_iota(jnp.int32, (eighths, 8, DK), 1)
    over_last = (((1,), (1,)), ((), ()))
    decays = []

    def score_block(b):
        at = slice(b * block, (b + 1) * block)
        q = proj[1, at, :].astype(f32) * DK ** (-0.5)
        kg = keep * jax.nn.sigmoid(-proj[0, at, :].astype(f32))
        added = jnp.broadcast_to(extra[b, pl.ds(head, 1), :], (DK, block)).T
        logs = jnp.log1p(-kg) + added
        cum = jnp.dot(lower, logs, precision=coarsest_scale_depth, preferred_element_type=f32)
        last = cum[block - 1 :, :]
        faded[at, :] = (kg * jnp.exp(last - cum)).astype(bf16)
        decays.append(jnp.exp(last))
        reach[at, :] = (q * jnp.exp(cum)).astype(bf16)
        kept[0, at, :] = cum
        kept[1, at, :] = kg
        scores = jnp.zeros((block, block), f32)
        span = 8
        while span < block:
            twice = 2 * span
            c3 = cum.reshape(block // twice, twice, DK)
            middle = jnp.broadcast_to(c3[:, span - 1 : span, :], c3.shape).reshape(cum.shape)
            fade = jnp.exp(-jnp.abs(cum - middle))
            later = (line // span) % 2 == 1
            probe = jnp.where(later, q * fade, 0.0).astype(bf16)
            keyed = jnp.where(later, 0.0, kg * fade).astype(bf16)
            found = lax.dot_general(probe, keyed, over_last, preferred_element_type=f32)
            scores = scores + jnp.where(row // twice == col // twice, found, 0.0)
            span = twice
        scored[b] = scores.astype(bf16)

    def value_block(b):
        at = slice(b * block, (b + 1) * block)
        q = proj[1, at, :].astype(f32) * DK ** (-0.5)
        v = proj[2, at, :]
        state[b] = lax.dot_general(
            v, faded[at, :], (((0,), (0,)), ((), ())), preferred_element_type=f32
        )
        result = jnp.dot(scored[b], v, preferred_element_type=f32)
        c3 = kept[0, at, :].reshape(eighths, 8, DK)
        q3 = q.reshape(eighths, 8, DK)
        k3 = kept[1, at, :].reshape(eighths, 8, DK)
        v3 = v.astype(f32).reshape(eighths, 8, DK)
        near = result.reshape(eighths, 8, DK)
        for s in range(8):
            weight = jnp.exp(jnp.minimum(c3 - c3[:, s : s + 1, :], 0.0))
            score = jnp.sum(q3 * k3[:, s : s + 1, :] * weight, axis=2, keepdims=True)
            near = near + jnp.where(sub >= s, score * v3[:, s : s + 1, :], 0.0)
        local[at, :] = near.reshape(block, DK)

    score_block(0)
    w_relays(3)
    score_block(1)
    score_block(2)
    score_block(3)
    w_relays(4)
    o_near()
    o_across(range(pieces))
    w_need(2)
    project_units(2, 1)
    for b in range(blocks):
        value_block(b)

    sums = [decays[2 * i + 1] * state[2 * i] + state[2 * i + 1] for i in range(2)]
    fades = [decays[2 * i] * decays[2 * i + 1] for i in range(2)]
    for i in range(2):
        state_go[i] = sums[i].astype(bf16)
        decay_go[i : i + 1, :] = fades[i]
    send(state_go, state_come, scan_send.at[0], scan_recv.at[0], other_y)
    send(decay_go, decay_come, scan_send.at[1], scan_recv.at[1], other_y)
    w_need(3)
    project_units(3, 1)
    for i in range(2):
        tail_go[i] = proj[3, (i + 1) * half - 16 : (i + 1) * half, :]
    send(tail_go, tail_come, scan_send.at[2], scan_recv.at[2], other_y)
    send(tail_go.at[1], last_come, scan_send.at[4], scan_recv.at[4], across_y)
    w_relays(5)
    w_need(4)
    project_units(4, 1)
    o_near_relays(range(2))
    o_mid_relays(2, range(2))

    arrive(state_come, scan_recv.at[0])
    arrive(decay_come, scan_recv.at[1])
    first_y = y == 0
    theirs = [state_come[i].astype(f32) for i in range(2)]
    their_fades = [decay_come[i : i + 1, :] for i in range(2)]
    order = []
    for i in range(2):
        order.append(
            (jnp.where(first_y, sums[i], theirs[i]), jnp.where(first_y, fades[i], their_fades[i]))
        )
        order.append(
            (jnp.where(first_y, theirs[i], sums[i]), jnp.where(first_y, their_fades[i], fades[i]))
        )
    total = order[0][0]
    for add, fade in order[1:]:
        total = fade * total + add
    total_go[...] = total.astype(bf16)
    send(total_go, total_come, scan_send.at[3], scan_recv.at[3], across)
    mix_copy.wait()
    arrive(tail_come, scan_recv.at[2])
    arrive(last_come, scan_recv.at[4])

    later_pair = pair > 0
    at_head = lanes(head)
    level = (x * 4 + head) % 4
    window = 2
    for k in range(1, 4):
        window = jnp.where(level == k, 2 ** (1 + k), window)
    line_half = lax.broadcasted_iota(jnp.int32, (half, DK), 0)
    far = [jnp.where(later_pair, last_come[...].astype(f32), 0.0), tail_come[0].astype(f32)]
    their_tails = [tail_come[i].astype(f32) for i in range(2)]
    is_odd = odd == 1

    def pool_half(i):
        at_static = slice(i * half, (i + 1) * half)
        xin = proj[3, at_static, :].astype(f32)
        prior = jnp.where(first_y, far[i], their_tails[i])
        sums_in = jnp.concatenate([prior, xin], axis=0)
        chosen = jnp.zeros((half, DK), f32)
        for k in range(4):
            sums_in = sums_in + pltpu.roll(sums_in, 2**k, 0)
            chosen = jnp.where(level == k, sums_in[16:, :], chosen)
        begins = (4 * pair + 2 * i + y) * half
        count = jnp.minimum(begins + line_half + 1, window).astype(f32)
        mixed = (chosen / count - xin).astype(bf16)
        mapped = jnp.dot(mixed, mix_own[...], preferred_element_type=f32)
        gate = proj[4, at_static, :].astype(f32)
        return mapped * pgain_ref[:, at_head] * (gate * jax.nn.sigmoid(gate))

    z_peer = peer(slabs[1], y, c)
    their_head = (1 - odd) * 2 + c

    def y_at(part, hd, ch):
        return y_all.at[part * 4 + hd, pl.ds(ch * block, block)]

    def y_put(part, ch, low, high):
        at = slice(ch * block, (ch + 1) * block)
        y_go[part, at, :] = jnp.where(is_odd, low, high).astype(bf16)
        y_all[part * 4 + head, at, :] = jnp.where(is_odd, high, low).astype(bf16)
        send(
            y_go.at[part, pl.ds(ch * block, block)],
            y_at(part, head, ch),
            y_send.at[0],
            y_recv.at[part * 2 + ch],
            z_peer,
        )
        at = y_at(part, head, ch)
        send(at, at, y_send.at[0], y_recv.at[4 + ch], other_c)

    def y_pass(part, ch):
        at = y_at(part, their_head, ch)
        arrive(at, y_recv.at[part * 2 + ch])
        send(at, at, y_send.at[0], y_recv.at[4 + ch], other_c)

    def y_need(ch):
        arrive(y_all.at[pl.ds(0, 2)], y_recv.at[4 + ch])

    pooled = [pool_half(i) for i in range(2)]
    for ch in range(2):
        rows_ch = slice(ch * block, (ch + 1) * block)
        y_put(1, ch, pooled[0][rows_ch], pooled[1][rows_ch])
    o_near_relays(range(2, pieces))
    w_need(5)
    project_units(5, 1)
    arrive(total_come, scan_recv.at[3])
    befores = []
    running = jnp.where(later_pair, total_come[...].astype(f32), 0.0)
    for i in range(2):
        after_first = order[2 * i][1] * running + order[2 * i][0]
        befores.append(jnp.where(first_y, running, after_first))
        running = order[2 * i + 1][1] * after_first + order[2 * i + 1][0]

    def rec_rows(b, before):
        rows_b = slice(b * block, (b + 1) * block)
        rec = local[rows_b, :] + lax.dot_general(
            reach[rows_b, :], before.astype(bf16), over_last, preferred_element_type=f32
        )
        normed = rec * lax.rsqrt(jnp.mean(rec * rec, axis=1, keepdims=True) + eps)
        gate = proj[5, rows_b, :].astype(f32)
        return normed * sgain_ref[:, at_head] * (gate * jax.nn.sigmoid(gate))

    for ch in range(2):
        recs = []
        for i in range(2):
            b = 2 * i + ch
            recs.append(rec_rows(b, befores[i]))
            befores[i] = decays[b] * befores[i] + state[b]
        y_put(0, ch, recs[0], recs[1])
    o_mid_relays(2, range(2, pieces))
    for ch in range(2):
        y_pass(1, ch)
    o_mid_relays(3, range(2))
    o_end_relays(2, range(2))
    y_pass(0, 0)
    o_mid_relays(3, range(2, pieces))
    y_pass(0, 1)

    owned = part_come.shape[2]

    def rows_for(xx, cc):
        return own_rows(cc * rows + xx * owned, owned)

    def part_copies(k, ch, cols):
        over_x = send_copy(
            part_go.at[k, rows_for(1 - x, ch), cols],
            part_come.at[k, c, :, cols],
            part_send.at[0],
            part_recv.at[k],
            peer_x(ch),
        )
        over_c = send_copy(
            part_go.at[k, rows_for(x, ch), cols],
            part_come.at[k, 2, :, cols],
            part_send.at[0],
            part_recv.at[k],
            other_c,
        )
        return over_x, over_c

    def out_chunk(k, ch, yy=None):
        left = jnp.concatenate(
            [y_all[i, ch * block : (ch + 1) * block, :] for i in range(8)], axis=1
        )
        if yy is None:
            right = jnp.concatenate([o_all[slabs[k] * 2], o_all[slabs[k] * 2 + 1]], axis=1)
            cols = pl.ds(0, 2 * DK)
        else:
            right = o_all[slabs[k] * 2 + yy]
            cols = lanes(yy)
        part_go[k, ch * block : (ch + 1) * block, cols] = jnp.dot(
            left, right, preferred_element_type=f32
        ).astype(bf16)
        over_x, over_c = part_copies(k, ch, cols)
        over_x.start()

        @pl.when(c != ch)
        def _():
            over_c.start()

    def drain():
        sent(wide.at[pl.ds(0, 6 * rows // 2)], tok_send.at[1])
        sent(extra.at[pl.ds(0, 3)], extra_send.at[0])
        sent(w_all.at[pl.ds(0, 3), pl.ds(0, 14 * shard)], w_send.at[0])
        sent(w_all.at[pl.ds(0, 3)], wy_send.at[0])
        sent(o_all.at[0], o_send.at[0])
        sent(o_all.at[pl.ds(0, 4)], oy_send.at[0])

        @pl.when(is_mid)
        def _():
            sent(o_all.at[pl.ds(0, 4)], o_send.at[1])

        for i, ref in enumerate([state_go, decay_go, tail_go, total_go, tail_go.at[1]]):
            sent(ref, scan_send.at[i])
        sent(y_all.at[pl.ds(0, 6)], y_send.at[0])

    def gather_chunk(k):
        arrive(part_come.at[k], part_recv.at[k])
        ours = part_go[k, rows_for(x, c), :].astype(f32) + part_come[k, c].astype(f32)
        others = part_come[k, 2].astype(f32) + part_come[k, 1 - c].astype(f32)
        for yy in range(2):
            cols = slice(yy * DK, (yy + 1) * DK)
            mine[:, lanes(slabs[k] * 4 + yy * 2 + c)] = ours[:, cols]
            mine[:, lanes(slabs[k] * 4 + yy * 2 + 1 - c)] = others[:, cols]

    late = [(2, 2), (2, 3), (3, 0), (3, 1), (3, 2), (3, 3)]

    def late_relay():
        k, part = late.pop(0)
        o_end_relays(k, [part])

    for ch in range(2):
        y_need(ch)
        for k in range(2):
            if ch == 0:
                o_need(k)
            out_chunk(k, ch)
            late_relay()
    o_need(2)
    for ch in range(2):
        out_chunk(2, ch)
        late_relay()
    for ch in range(2):
        out_chunk(3, ch, y)
    o_need(3)
    for ch in range(2):
        out_chunk(3, ch, 1 - y)
    drain()
    for k in range(len(slabs)):
        gather_chunk(k)

    def finish():
        summed = mine[...]
        done[...] = (
            summed
            * lax.rsqrt(jnp.mean(summed * summed, axis=1, keepdims=True) + eps)
            * post_ref[...]
        ).astype(bf16)
        copy = pltpu.make_async_copy(done, out_ref, own_sem.at[0])
        copy.start()
        copy.wait()

    finish()
    sent(part_go.at[pl.ds(0, 3)], part_send.at[0])


def pair_layer(
    tokens,
    gain,
    shards,
    rate,
    extra,
    sgain,
    pool_mix,
    pgain,
    out_rec,
    out_pool,
    post,
):
    n = lax.axis_size("sp")
    n_tp = lax.axis_size("tp")
    rows, feats = tokens.shape
    shard, cols = shards[0].shape
    heads = cols // DK
    depth, width = out_rec.shape
    slabs = n // 4
    positions = 4 * rows
    half = 2 * rows
    owned = rows // n_tp
    model = n * width
    f32, bf16, dma = jnp.float32, jnp.bfloat16, pltpu.SemaphoreType.DMA
    units = len(shards)
    vmem, hbm = pl.BlockSpec(memory_space=pltpu.VMEM), pl.BlockSpec(memory_space=pl.ANY)
    return pl.pallas_call(
        pair_kernel,
        out_shape=jax.ShapeDtypeStruct((owned, model), bf16),
        in_specs=[hbm, vmem] + [hbm] * 6 + [vmem, hbm, vmem, hbm, vmem, hbm, hbm, vmem],
        out_specs=hbm,
        scratch_shapes=[
            pltpu.VMEM((positions, n_tp * feats), bf16),
            pltpu.VMEM((positions, n_tp * feats), bf16),
            pltpu.VMEM((positions, DK), f32),
            pltpu.VMEM((units, shard, cols), bf16),
            pltpu.VMEM((units, n * shard, DK), bf16),
            pltpu.VMEM((2 * slabs, 2 * depth, width), bf16),
            pltpu.VMEM((4, heads, rows), f32),
            pltpu.VMEM((DK, DK), bf16),
            pltpu.VMEM((units, positions, DK), bf16),
            pltpu.VMEM((positions, DK), f32),
            pltpu.VMEM((positions, DK), bf16),
            pltpu.VMEM((positions, DK), bf16),
            pltpu.VMEM((2, positions, DK), f32),
            pltpu.VMEM((4, rows, rows), bf16),
            pltpu.VMEM((4, DK, DK), f32),
            pltpu.VMEM((2, DK, DK), bf16),
            pltpu.VMEM((2, DK, DK), bf16),
            pltpu.VMEM((8, DK), f32),
            pltpu.VMEM((8, DK), f32),
            pltpu.VMEM((2, 16, DK), bf16),
            pltpu.VMEM((2, 16, DK), bf16),
            pltpu.VMEM((DK, DK), bf16),
            pltpu.VMEM((DK, DK), bf16),
            pltpu.VMEM((16, DK), bf16),
            pltpu.VMEM((2 * heads, half, DK), bf16),
            pltpu.VMEM((2, half, DK), bf16),
            pltpu.VMEM((slabs, half, 2 * width), bf16),
            pltpu.VMEM((slabs, 3, owned, 2 * width), bf16),
            pltpu.VMEM((owned, model), f32),
            pltpu.VMEM((owned, model), bf16),
            dma((5,)),
            dma((2,)),
            dma((11,)),
            dma((1,)),
            dma((3,)),
            dma((1,)),
            dma((units, slabs)),
            dma((1,)),
            dma((units,)),
            dma((2,)),
            dma((3, 4)),
            dma((1,)),
            dma((slabs,)),
            dma((5,)),
            dma((5,)),
            dma((1,)),
            dma((6,)),
            dma((1,)),
            dma((slabs,)),
        ],
        compiler_params=pltpu.CompilerParams(
            collective_id=0, has_side_effects=True, vmem_limit_bytes=56 * 1024 * 1024
        ),
        cost_estimate=pl.CostEstimate(
            flops=2 * positions * n * shard * units * DK,
            bytes_accessed=4 * units * shard * cols,
            transcendentals=0,
        ),
    )(
        tokens,
        gain[None, :],
        *shards,
        rate[None, :],
        extra.T,
        sgain[None, :],
        pool_mix,
        pgain[None, :],
        out_rec,
        out_pool,
        post[None, :],
    )


def per_device(
    tokens_in,
    norm_gain,
    w_query,
    w_forget,
    w_input,
    w_rgate,
    w_pool_in,
    w_pgate,
    floor_rate,
    extra_logdecay,
    state_gain,
    pool_mix,
    pool_gain,
    out_rec,
    out_pool,
    post_gain,
):
    n, n_tp, heads = lax.axis_size("sp"), lax.axis_size("tp"), extra_logdecay.shape[1]
    if n == 16 and n_tp == 2 and heads == 4:
        return pair_layer(
            tokens_in,
            norm_gain,
            [w_forget, w_query, w_input, w_pool_in, w_pgate, w_rgate],
            floor_rate,
            extra_logdecay,
            state_gain,
            pool_mix,
            pool_gain,
            out_rec,
            out_pool,
            post_gain,
        )
    shards = [w_query, w_forget, w_input, w_rgate, w_pool_in, w_pgate]
    proj = project(tokens_in, norm_gain, shards)
    return mix(
        proj,
        -jnp.expm1(-floor_rate)[None, :],
        extra_logdecay,
        state_gain[None, :],
        pool_mix,
        pool_gain[None, :],
        jnp.concatenate([out_rec, out_pool], axis=0),
        post_gain[None, :],
    )


def solution(mesh):
    placed = (
        P("sp", "tp"),
        P(),
        P("sp", "tp"),
        P("sp", "tp"),
        P("sp", "tp"),
        P("sp", "tp"),
        P("sp", "tp"),
        P("sp", "tp"),
        P("tp"),
        P("sp", "tp"),
        P("tp"),
        P("tp", None, None),
        P("tp"),
        P("tp", "sp"),
        P("tp", "sp"),
        P(),
    )
    return jax.shard_map(
        per_device, mesh=mesh, in_specs=placed, out_specs=P(("sp", "tp"), None), check_vma=False
    )
```

```python
import functools

import jax
import jax.numpy as jnp
from jax import lax
from jax.experimental import pallas as pl
from jax.experimental.pallas import tpu as pltpu
from jax.sharding import PartitionSpec as P

DK = 128


eps = 1e-06
coarsest_scale_depth = lax.Precision.HIGHEST


PIECES = 4


def ring_place(chip, chips):
    odd = chip % 2
    return (1 - odd) * (chip // 2) + odd * (chips - 1 - chip // 2)


def ring_chip(place, chips):
    back = place // (chips // 2)
    return (1 - back) * (2 * place) + back * (2 * (chips - 1 - place) + 1)


def project_kernel(
    n,
    n_tp,
    tok_ref,
    gain_ref,
    w0,
    w1,
    w2,
    w3,
    w4,
    w5,
    proj_ref,
    wide,
    scaled,
    weights,
    acc,
    tok_send,
    tok_recv,
    own_sem,
    ring_send,
    ring_recv,
    core_send,
    core_recv,
):
    chips = n // 2
    steps = chips // 2
    me = lax.axis_index("sp")
    tp = lax.axis_index("tp")
    core = me % 2
    place = ring_place(me // 2, chips)

    def chip_at(offset):
        return ring_chip((place + offset + chips) % chips, chips)

    following = 2 * chip_at(1) + core
    preceding = 2 * chip_at(-1) + core
    partner = 2 * (me // 2) + 1 - core
    parts = (w0, w1, w2, w3, w4, w5)
    rows, part_cols = w0.shape
    my_rows = pl.ds(pl.multiple_of(me * rows, 16), rows)
    owns = []
    for i, part in enumerate(parts):
        block = weights.at[my_rows, pl.ds(i * part_cols, part_cols)]
        owns.append(pltpu.make_async_copy(part, block, own_sem.at[i]))
        owns[-1].start()
    piece = rows // PIECES
    features = tok_ref.shape[1]

    barrier = pltpu.get_barrier_semaphore()
    for peer in (following, preceding, partner):
        pl.semaphore_signal(barrier, inc=1, device_id={"sp": peer})
    for turn in range(1, n_tp):
        pl.semaphore_signal(barrier, inc=1, device_id={"tp": (tp + turn) % n_tp})
    pl.semaphore_wait(barrier, 3 + n_tp - 1)

    def rows_of(chip, which, q):
        start = (2 * chip + which) * rows + q * piece
        return pl.ds(pl.multiple_of(start, 8), piece)

    sends = []

    def to_core(offset, q, source):
        slot = offset + steps - 1
        copy = pltpu.make_async_remote_copy(
            src_ref=source,
            dst_ref=weights.at[rows_of(chip_at(offset), core, q)],
            send_sem=core_send.at[slot, q],
            recv_sem=core_recv.at[slot, q],
            device_id={"sp": partner},
        )
        copy.start()
        sends.append(copy)

    def from_core(offset, q):
        slot = offset + steps - 1
        dst = weights.at[rows_of(chip_at(offset), 1 - core, q)]
        pltpu.make_async_remote_copy(
            src_ref=dst,
            dst_ref=dst,
            send_sem=core_send.at[slot, q],
            recv_sem=core_recv.at[slot, q],
            device_id={"sp": partner},
        ).wait_recv()

    def pieces_of(direction, step):
        if step < steps - 1:
            return range(PIECES)
        half = PIECES // 2
        return range(half) if direction == 0 else range(half, PIECES)

    def ring_copy(direction, step, q, source):
        offset = -step if direction == 0 else step
        dst = weights.at[rows_of(chip_at(offset), core, q)]
        return pltpu.make_async_remote_copy(
            src_ref=dst if source is None else source,
            dst_ref=dst,
            send_sem=ring_send.at[direction, step, q],
            recv_sem=ring_recv.at[direction, step, q],
            device_id={"sp": following if direction == 0 else preceding},
        )

    def ring_arrival(direction, step, q):
        offset = -(step + 1) if direction == 0 else step + 1
        dst = weights.at[rows_of(chip_at(offset), core, q)]
        pltpu.make_async_remote_copy(
            src_ref=dst,
            dst_ref=dst,
            send_sem=ring_send.at[direction, step, q],
            recv_sem=ring_recv.at[direction, step, q],
            device_id={"sp": following if direction == 0 else preceding},
        ).wait_recv()

    for own in owns:
        own.wait()
    for q in range(PIECES):
        mine = weights.at[rows_of(me // 2, core, q)]
        for direction in range(2):
            if q in pieces_of(direction, 0):
                copy = ring_copy(direction, 0, q, mine)
                copy.start()
                sends.append(copy)
        to_core(0, q, mine)
    tokens_at = pl.ds(pl.multiple_of(tp * features, 128), features)
    for turn in range(1, n_tp):
        copy = pltpu.make_async_remote_copy(
            src_ref=tok_ref,
            dst_ref=wide.at[:, tokens_at],
            send_sem=tok_send.at[turn - 1],
            recv_sem=tok_recv.at[turn - 1],
            device_id={"tp": (tp + turn) % n_tp},
        )
        copy.start()
        sends.append(copy)
    acc[...] = jnp.zeros_like(acc)
    wide[:, tokens_at] = tok_ref[...]
    for turn in range(1, n_tp):
        theirs = pl.ds(
            pl.multiple_of((tp - turn + n_tp) % n_tp * features, 128), features
        )
        pltpu.make_async_remote_copy(
            src_ref=tok_ref,
            dst_ref=wide.at[:, theirs],
            send_sem=tok_send.at[turn - 1],
            recv_sem=tok_recv.at[turn - 1],
            device_id={"tp": (tp + turn) % n_tp},
        ).wait_recv()
    scaled[...] = (wide[...].astype(jnp.float32) * gain_ref[...]).astype(jnp.bfloat16)

    cols = weights.shape[1]
    tile = cols // 6

    by_chip = (2 * rows) % 128 == 0

    def multiply(offset):
        if not by_chip:
            return
        multiply_rows(pl.ds(pl.multiple_of(chip_at(offset) * 2 * rows, 2 * rows), 2 * rows))

    def multiply_rows(depth):
        def one(i, _):
            at = pl.ds(pl.multiple_of(i * tile, 128), tile)
            acc[:, at] += jnp.dot(
                scaled[:, depth], weights[depth, at], preferred_element_type=jnp.float32
            )
            return 0

        lax.fori_loop(0, 6, one, 0)

    for step in range(steps):
        for q in range(PIECES):
            for direction in range(2):
                if q not in pieces_of(direction, step):
                    continue
                offset = -(step + 1) if direction == 0 else step + 1
                ring_arrival(direction, step, q)
                if step + 1 < steps and q in pieces_of(direction, step + 1):
                    copy = ring_copy(direction, step + 1, q, None)
                    copy.start()
                    sends.append(copy)
                last = offset if abs(offset) < steps else steps
                dst = weights.at[rows_of(chip_at(last), core, q)]
                to_core(last, q, dst)
        for offset in [0] if step == 0 else [-step, step]:
            for q in range(PIECES):
                from_core(offset, q)
            multiply(offset)
    for q in range(PIECES):
        from_core(steps, q)
    multiply(steps)
    if not by_chip:
        multiply_rows(slice(None))
    values = wide[...].astype(jnp.float32)
    squares = jnp.sum(values * values, axis=1, keepdims=True)
    inv_rms = lax.rsqrt(squares / wide.shape[1] + eps)
    proj_ref[...] = (acc[...] * inv_rms).astype(jnp.bfloat16)
    for copy in sends:
        copy.wait_send()


def project(tokens, gain, shards):
    n = lax.axis_size("sp")
    n_tp = lax.axis_size("tp")
    positions, features = tokens.shape
    rows = shards[0].shape[0]
    cols = sum(shard.shape[1] for shard in shards)
    width = n * rows
    steps = n // 4
    dma = pltpu.SemaphoreType.DMA
    return pl.pallas_call(
        functools.partial(project_kernel, n, n_tp),
        out_shape=jax.ShapeDtypeStruct((positions, cols), jnp.bfloat16),
        in_specs=[pl.BlockSpec(memory_space=pltpu.VMEM)] * 2
        + [pl.BlockSpec(memory_space=pl.ANY)] * 6,
        out_specs=pl.BlockSpec(memory_space=pltpu.VMEM),
        scratch_shapes=[
            pltpu.VMEM((positions, width), jnp.bfloat16),
            pltpu.VMEM((positions, width), jnp.bfloat16),
            pltpu.VMEM((width, cols), jnp.bfloat16),
            pltpu.VMEM((positions, cols), jnp.float32),
            dma((n_tp,)),
            dma((n_tp,)),
            dma((6,)),
            dma((2, steps, PIECES)),
            dma((2, steps, PIECES)),
            dma((2 * steps, PIECES)),
            dma((2 * steps, PIECES)),
        ],
        compiler_params=pltpu.CompilerParams(
            collective_id=0, has_side_effects=True, vmem_limit_bytes=56 * 1024 * 1024
        ),
        cost_estimate=pl.CostEstimate(
            flops=2 * positions * width * cols, bytes_accessed=4 * rows * cols, transcendentals=0
        ),
    )(tokens, gain[None, :], *shards)


def mix_kernel(
    n,
    n_tp,
    proj_ref,
    keep_ref,
    extra_ref,
    sgain_ref,
    mix_ref,
    pgain_ref,
    w_ref,
    post_ref,
    out_ref,
    weights,
    local,
    reach,
    both,
    state,
    before,
    gone_state,
    gone_decay,
    come_state,
    come_decay,
    tail,
    tail_in,
    mine,
    gone_out,
    come_out,
    ring_send,
    ring_recv,
    core_send,
    core_recv,
    scan_send,
    scan_recv,
    tail_sem,
    own_sem,
    out_send,
    out_recv,
):
    f32, bf16 = jnp.float32, jnp.bfloat16
    chips = n // 2
    steps = chips // 2
    rounds = (n - 1).bit_length()
    me = lax.axis_index("sp")
    tp = lax.axis_index("tp")
    core = me % 2
    place = ring_place(me // 2, chips)

    def chip_at(offset):
        return ring_chip((place + offset + chips) % chips, chips)

    following = 2 * chip_at(1) + core
    preceding = 2 * chip_at(-1) + core
    partner = 2 * (me // 2) + 1 - core
    piece = w_ref.shape[0] // PIECES

    barrier = pltpu.get_barrier_semaphore()
    for peer in (following, preceding, partner):
        pl.semaphore_signal(barrier, inc=1, device_id={"sp": peer})
    for r in range(rounds):
        pl.semaphore_signal(barrier, inc=1, device_id={"sp": (me + 2**r) % n})
        pl.semaphore_signal(barrier, inc=1, device_id={"sp": (me - 2**r + n) % n})
    for turn in range(1, n_tp):
        pl.semaphore_signal(barrier, inc=1, device_id={"tp": (tp + turn) % n_tp})
    pl.semaphore_wait(barrier, 3 + 2 * rounds + n_tp - 1)

    sends = []

    def spot(chip, which, q):
        return weights.at[2 * chip + which, pl.ds(q * piece, piece)]

    def to_core(offset, q, source):
        slot = offset + steps - 1
        copy = pltpu.make_async_remote_copy(
            src_ref=source,
            dst_ref=spot(chip_at(offset), core, q),
            send_sem=core_send.at[slot, q],
            recv_sem=core_recv.at[slot, q],
            device_id={"sp": partner},
        )
        copy.start()
        sends.append(copy)

    def from_core(offset, q):
        slot = offset + steps - 1
        dst = spot(chip_at(offset), 1 - core, q)
        pltpu.make_async_remote_copy(
            src_ref=dst,
            dst_ref=dst,
            send_sem=core_send.at[slot, q],
            recv_sem=core_recv.at[slot, q],
            device_id={"sp": partner},
        ).wait_recv()

    def pieces_of(direction, step):
        if step < steps - 1:
            return range(PIECES)
        half = PIECES // 2
        return range(half) if direction == 0 else range(half, PIECES)

    def ring_copy(direction, step, q, source, offset):
        dst = spot(chip_at(offset), core, q)
        return pltpu.make_async_remote_copy(
            src_ref=dst if source is None else source,
            dst_ref=dst,
            send_sem=ring_send.at[direction, step, q],
            recv_sem=ring_recv.at[direction, step, q],
            device_id={"sp": following if direction == 0 else preceding},
        )

    def ring_step(step):
        for q in range(PIECES):
            for direction in range(2):
                if q not in pieces_of(direction, step):
                    continue
                offset = -(step + 1) if direction == 0 else step + 1
                ring_copy(direction, step, q, None, offset).wait_recv()
                if step + 1 < steps and q in pieces_of(direction, step + 1):
                    copy = ring_copy(direction, step + 1, q, None, offset)
                    copy.start()
                    sends.append(copy)
                last = offset if abs(offset) < steps else steps
                to_core(last, q, spot(chip_at(last), core, q))

    pending = list(range(steps))

    def advance_ring():
        if pending:
            ring_step(pending.pop(0))

    positions = proj_ref.shape[0]
    head_cols = proj_ref.shape[1] // 6
    heads = head_cols // DK
    reach_back = tail.shape[0]

    tail[...] = proj_ref[positions - reach_back :, 4 * head_cols : 5 * head_cols]
    for q in range(PIECES):
        own_piece = w_ref.at[pl.ds(q * piece, piece)]
        for direction in range(2):
            if q in pieces_of(direction, 0):
                copy = ring_copy(direction, 0, q, own_piece, 0)
                copy.start()
                sends.append(copy)
        to_core(0, q, own_piece)
    own = pltpu.make_async_copy(w_ref, weights.at[me], own_sem)
    own.start()
    tail_copy = pltpu.make_async_remote_copy(
        src_ref=tail,
        dst_ref=tail_in,
        send_sem=tail_sem.at[0],
        recv_sem=tail_sem.at[1],
        device_id={"sp": (me + 1) % n},
    )
    tail_copy.start()

    row = lax.broadcasted_iota(jnp.int32, (positions, positions), 0)
    col = lax.broadcasted_iota(jnp.int32, (positions, positions), 1)
    lower = jnp.where(row >= col, 1.0, 0.0).astype(f32)
    line = lax.broadcasted_iota(jnp.int32, (positions, DK), 0)
    units = positions // 8
    sub = lax.broadcasted_iota(jnp.int32, (units, 8, DK), 1)
    over_last = (((1,), (1,)), ((), ()))

    decay_now = []
    for h in range(heads):
        at = slice(h * DK, (h + 1) * DK)
        part = lambda i: proj_ref[:, i * head_cols + h * DK : i * head_cols + (h + 1) * DK]
        q = part(0).astype(f32) * DK ** (-0.5)
        kg = keep_ref[:, at] * jax.nn.sigmoid(-part(1).astype(f32))
        v = part(2)
        logs = jnp.log1p(-kg) + extra_ref[:, h : h + 1]
        c = jnp.dot(
            lower, logs, precision=coarsest_scale_depth, preferred_element_type=f32
        )
        last = c[positions - 1 :, :]
        state[h] = lax.dot_general(
            v,
            (kg * jnp.exp(last - c)).astype(bf16),
            (((0,), (0,)), ((), ())),
            preferred_element_type=f32,
        )
        gone_decay[0, h : h + 1, :] = jnp.exp(last)
        reach[:, at] = (q * jnp.exp(c)).astype(bf16)
        scores = jnp.zeros((positions, positions), f32)
        span = 8
        while span < positions:
            pair = 2 * span
            c3 = c.reshape(positions // pair, pair, DK)
            middle = jnp.broadcast_to(c3[:, span - 1 : span, :], c3.shape).reshape(c.shape)
            fade = jnp.exp(-jnp.abs(c - middle))
            later = (line // span) % 2 == 1
            probe = jnp.where(later, q * fade, 0.0).astype(bf16)
            keyed = jnp.where(later, 0.0, kg * fade).astype(bf16)
            found = lax.dot_general(probe, keyed, over_last, preferred_element_type=f32)
            scores = scores + jnp.where(row // pair == col // pair, found, 0.0)
            span = pair
        result = jnp.dot(scores.astype(bf16), v, preferred_element_type=f32)
        c3 = c.reshape(units, 8, DK)
        q3 = q.reshape(units, 8, DK)
        k3 = kg.reshape(units, 8, DK)
        v3 = v.astype(f32).reshape(units, 8, DK)
        near = result.reshape(units, 8, DK)
        for s in range(8):
            weight = jnp.exp(jnp.minimum(c3 - c3[:, s : s + 1, :], 0.0))
            score = jnp.sum(q3 * k3[:, s : s + 1, :] * weight, axis=2, keepdims=True)
            near = near + jnp.where(sub >= s, score * v3[:, s : s + 1, :], 0.0)
        local[:, at] = near.reshape(positions, DK)
        if h % 2 == 1:
            advance_ring()

    def scan_copies(r):
        target = {"sp": (me + 2**r) % n}
        return [
            pltpu.make_async_remote_copy(
                src_ref=gone.at[r],
                dst_ref=come.at[r],
                send_sem=scan_send.at[r, i],
                recv_sem=scan_recv.at[r, i],
                device_id=target,
            )
            for i, (gone, come) in enumerate(
                [(gone_state, come_state), (gone_decay, come_decay)]
            )
        ]

    before[...] = jnp.zeros_like(before)
    decay_w = [gone_decay[0, h : h + 1, :] for h in range(heads)]
    decay_e = [jnp.ones((1, DK), f32) for h in range(heads)]

    def pool(h):
        at = slice(h * DK, (h + 1) * DK)
        x = proj_ref[:, 4 * head_cols + h * DK : 4 * head_cols + (h + 1) * DK].astype(f32)
        prior = jnp.where(me > 0, tail_in[:, at].astype(f32), 0.0)
        level = (tp * heads + h) % 4
        total = jnp.concatenate([prior, x], axis=0)
        chosen = jnp.zeros((positions, DK), f32)
        for k in range(4):
            total = total + pltpu.roll(total, 2**k, 0)
            chosen = jnp.where(level == k, total[reach_back:, :], chosen)
        window = 2
        for k in range(1, 4):
            window = jnp.where(level == k, 2 ** (1 + k), window)
        count = jnp.minimum(me * positions + line + 1, window).astype(f32)
        mixed = (chosen / count - x).astype(bf16)
        mapped = jnp.dot(mixed, mix_ref[h], preferred_element_type=f32)
        gate = proj_ref[:, 5 * head_cols + h * DK : 5 * head_cols + (h + 1) * DK].astype(f32)
        both[:, head_cols + h * DK : head_cols + (h + 1) * DK] = (
            mapped * pgain_ref[:, at] * (gate * jax.nn.sigmoid(gate))
        ).astype(bf16)

    pools = list(range(heads))
    for r in range(rounds):
        gone_state[r] = state[...].astype(bf16)
        if r > 0:
            for h in range(heads):
                gone_decay[r, h : h + 1, :] = decay_w[h]
        for copy in scan_copies(r):
            copy.start()
            sends.append(copy)
        if r == 0:
            tail_copy.wait_recv()
        if pools:
            pool(pools.pop(0))
        advance_ring()
        for copy in scan_copies(r):
            copy.wait_recv()
        valid = me >= 2**r
        for h in range(heads):
            came = jnp.where(valid, come_state[r, h].astype(f32), 0.0)
            came_decay = jnp.where(valid, come_decay[r, h : h + 1, :], 1.0)
            before[h] = before[h] + decay_e[h] * came
            decay_e[h] = decay_e[h] * came_decay
            if r + 1 < rounds:
                state[h] = state[h] + decay_w[h] * came
                decay_w[h] = decay_w[h] * came_decay
    for h in pools:
        pool(h)
    while pending:
        advance_ring()

    for h in range(heads):
        at = slice(h * DK, (h + 1) * DK)
        rec = local[:, at] + lax.dot_general(
            reach[:, at], before[h].astype(bf16), over_last, preferred_element_type=f32
        )
        normed = rec * lax.rsqrt(jnp.mean(rec * rec, axis=1, keepdims=True) + eps)
        gate = proj_ref[:, 3 * head_cols + h * DK : 3 * head_cols + (h + 1) * DK].astype(f32)
        both[:, at] = (normed * sgain_ref[:, at] * (gate * jax.nn.sigmoid(gate))).astype(bf16)

    own.wait()
    for offset in range(-(steps - 1), steps + 1):
        for q in range(PIECES):
            from_core(offset, q)

    owned = positions // n_tp
    width = w_ref.shape[1]
    quarter = n // 4

    def share(rows, group):
        left = both[rows, :]
        for slot in range(group * quarter, (group + 1) * quarter, 2):
            right = jnp.concatenate([weights[slot], weights[slot + 1]], axis=1)
            yield slot, jnp.dot(left, right, preferred_element_type=f32).astype(bf16)

    def out_copy(turn, group):
        cols = pl.ds(group * quarter * width, quarter * width)
        return pltpu.make_async_remote_copy(
            src_ref=gone_out.at[turn - 1, :, cols],
            dst_ref=come_out.at[turn - 1, :, cols],
            send_sem=out_send.at[turn - 1, group],
            recv_sem=out_recv.at[turn - 1, group],
            device_id={"tp": (tp + turn) % n_tp},
        )

    for turn in range(1, n_tp):
        target = (tp + turn) % n_tp
        rows = pl.ds(pl.multiple_of(target * owned, owned), owned)
        for group in range(4):
            for slot, value in share(rows, group):
                gone_out[turn - 1, :, slot * width : (slot + 2) * width] = value
            copy = out_copy(turn, group)
            copy.start()
            sends.append(copy)
    rows = pl.ds(pl.multiple_of(tp * owned, owned), owned)
    for group in range(4):
        for slot, value in share(rows, group):
            mine[:, slot * width : (slot + 2) * width] = value.astype(f32)
    for turn in range(1, n_tp):
        for group in range(4):
            out_copy(turn, group).wait_recv()
        mine[...] += come_out[turn - 1].astype(f32)
    summed = mine[...]
    out_ref[...] = (
        summed
        * lax.rsqrt(jnp.mean(summed * summed, axis=1, keepdims=True) + eps)
        * post_ref[...]
    ).astype(bf16)
    tail_copy.wait_send()
    for copy in sends:
        copy.wait_send()


def mix(proj, keep, extra, sgain, pool_mix, pgain, shard, post):
    n = lax.axis_size("sp")
    n_tp = lax.axis_size("tp")
    positions, heads = extra.shape
    head_cols = heads * DK
    depth, width = shard.shape
    steps = n // 4
    rounds = (n - 1).bit_length()
    owned = positions // n_tp
    model = n * width
    padded = -(-heads // 8) * 8
    f32, bf16, dma = jnp.float32, jnp.bfloat16, pltpu.SemaphoreType.DMA
    return pl.pallas_call(
        functools.partial(mix_kernel, n, n_tp),
        out_shape=jax.ShapeDtypeStruct((owned, model), bf16),
        in_specs=[pl.BlockSpec(memory_space=pltpu.VMEM)] * 8,
        out_specs=pl.BlockSpec(memory_space=pltpu.VMEM),
        scratch_shapes=[
            pltpu.VMEM((n, depth, width), bf16),
            pltpu.VMEM((positions, head_cols), f32),
            pltpu.VMEM((positions, head_cols), bf16),
            pltpu.VMEM((positions, 2 * head_cols), bf16),
            pltpu.VMEM((heads, DK, DK), f32),
            pltpu.VMEM((heads, DK, DK), f32),
            pltpu.VMEM((rounds, heads, DK, DK), bf16),
            pltpu.VMEM((rounds, padded, DK), f32),
            pltpu.VMEM((rounds, heads, DK, DK), bf16),
            pltpu.VMEM((rounds, padded, DK), f32),
            pltpu.VMEM((16, head_cols), bf16),
            pltpu.VMEM((16, head_cols), bf16),
            pltpu.VMEM((owned, model), f32),
            pltpu.VMEM((n_tp, owned, model), bf16),
            pltpu.VMEM((n_tp, owned, model), bf16),
            dma((2, steps, PIECES)),
            dma((2, steps, PIECES)),
            dma((2 * steps, PIECES)),
            dma((2 * steps, PIECES)),
            dma((rounds, 2)),
            dma((rounds, 2)),
            dma((2,)),
            dma,
            dma((n_tp, 4)),
            dma((n_tp, 4)),
        ],
        compiler_params=pltpu.CompilerParams(
            collective_id=1, has_side_effects=True, vmem_limit_bytes=56 * 1024 * 1024
        ),
        cost_estimate=pl.CostEstimate(
            flops=2 * positions * depth * model, bytes_accessed=4 * depth * width, transcendentals=0
        ),
    )(proj, keep, extra, sgain, pool_mix, pgain, shard, post)


def pair_kernel(
    tok_hbm,
    gain_hbm,
    w0,
    w1,
    w2,
    w3,
    w4,
    w5,
    rate_hbm,
    extra_hbm,
    sgain_hbm,
    mix_hbm,
    pgain_hbm,
    orec_hbm,
    opool_hbm,
    post_hbm,
    out_ref,
    wide,
    scaled,
    inv_rms,
    w_own,
    w_all,
    o_all,
    extra,
    mix_own,
    proj,
    local,
    reach,
    faded,
    kept,
    scored,
    state,
    state_go,
    state_come,
    decay_go,
    decay_come,
    tail_go,
    tail_come,
    total_go,
    total_come,
    last_come,
    y_all,
    y_go,
    part_go,
    part_come,
    mine,
    done,
    gain_ref,
    rate_ref,
    sgain_ref,
    pgain_ref,
    post_ref,
    small_sem,
    own_sem,
    tok_send,
    tok_recv,
    extra_send,
    extra_recv,
    w_send,
    w_recv,
    wy_send,
    wy_recv,
    o_send,
    o_recv,
    oy_send,
    oy_recv,
    scan_send,
    scan_recv,
    y_send,
    y_recv,
    part_send,
    part_recv,
):
    f32, bf16 = jnp.float32, jnp.bfloat16
    me = lax.axis_index("sp")
    x = lax.axis_index("tp")
    z, y, c = me // 4, (me // 2) % 2, me % 2
    odd = z % 2
    pair = z // 2
    head = odd * 2 + c
    is_mid = (z == 1) | (z == 2)
    is_end = jnp.logical_not(is_mid)
    slabs = [z, z + 1 - 2 * odd, 2 - pair, 3 * (1 - pair)]
    my_slot = jnp.where(is_mid, 2, 3)
    rows, feats = tok_hbm.shape
    shard = w0.shape[0]
    parts = (w0, w1, w2, w3, w4, w5)
    units = len(parts)
    positions = wide.shape[0]
    half = positions // 2
    block = rows
    blocks = positions // block
    n_rows = w_all.shape[1]
    tok_pieces = 4
    piece = rows // tok_pieces

    def peer(zz, yy, cc):
        return {"sp": zz * 4 + yy * 2 + cc}

    def peer_x(cc):
        return {"sp": z * 4 + y * 2 + cc, "tp": 1 - x}

    other_c = peer(z, y, 1 - c)
    other_y = peer(z, 1 - y, c)

    def lanes(i, n=1):
        return pl.ds(pl.multiple_of(i * DK, DK), n * DK)

    def own_rows(base, size):
        return pl.ds(pl.multiple_of(base, 16), size)

    def tok_at(zq, cc, xx, q):
        start = zq * half + cc * rows + q * piece
        return wide.at[own_rows(start, piece), pl.ds(pl.multiple_of(xx * feats, 128), feats)]

    barrier = pltpu.get_barrier_semaphore()
    across = peer((z + 2) % 4, y, c)
    across_y = peer((z + 2) % 4, 1 - y, c)
    peers = [other_c, other_y, peer_x(c), peer_x(1 - c), across_y]
    for k in range(1, 4):
        peers += [peer(slabs[k], y, c), peer(slabs[k], y, 1 - c)]
    for to in peers:
        pl.semaphore_signal(barrier, inc=1, device_id=to)

    owns = {}

    def own_copy(name, src, dst):
        copy = pltpu.make_async_copy(src, dst, own_sem.at[len(owns)])
        copy.start()
        owns[name] = copy

    own_tok = wide.at[
        own_rows(odd * half + c * rows, rows), pl.ds(pl.multiple_of(x * feats, 128), feats)
    ]
    own_copy("tok", tok_hbm, own_tok)
    own_copy("extra", extra_hbm, extra.at[odd * 2 + c])
    here = z * 2 + y
    w_landed = own_sem.at[2]
    for u, part in enumerate(parts):
        pltpu.make_async_copy(part, w_own.at[u], w_landed).start()
    o_landed = own_sem.at[3]
    pltpu.make_async_copy(orec_hbm, o_all.at[here, pl.ds(0, 4 * DK)], o_landed).start()
    pltpu.make_async_copy(opool_hbm, o_all.at[here, pl.ds(4 * DK, 4 * DK)], o_landed).start()
    mix_copy = pltpu.make_async_copy(mix_hbm.at[head], mix_own, own_sem.at[4])
    mix_copy.start()
    smalls = []
    for i, (src, dst) in enumerate(
        [
            (gain_hbm, gain_ref),
            (rate_hbm, rate_ref),
            (sgain_hbm, sgain_ref),
            (pgain_hbm, pgain_ref),
            (post_hbm, post_ref),
        ]
    ):
        smalls.append(pltpu.make_async_copy(src, dst, small_sem.at[i]))
        smalls[-1].start()

    pl.semaphore_wait(barrier, len(peers))

    def send(src, dst, send_sem, recv_sem, to):
        pltpu.make_async_remote_copy(
            src_ref=src, dst_ref=dst, send_sem=send_sem, recv_sem=recv_sem, device_id=to
        ).start()

    def sent(ref, send_sem):
        pltpu.make_async_remote_copy(
            src_ref=ref, dst_ref=ref, send_sem=send_sem, recv_sem=send_sem, device_id=other_c
        ).wait_send()

    def arrive(ref, recv_sem):
        pltpu.make_async_remote_copy(
            src_ref=ref, dst_ref=ref, send_sem=recv_sem, recv_sem=recv_sem, device_id=other_c
        ).wait_recv()

    def tok_rows(zq, cc, xx):
        start = zq * half + cc * rows
        return wide.at[own_rows(start, rows), pl.ds(pl.multiple_of(xx * feats, 128), feats)]

    def tok_share(at, near):
        send(at, at, tok_send.at[1], tok_recv.at[9 if near else 10], other_c)

    owns["extra"].wait()
    for e, to in enumerate([other_c, peer(slabs[1], y, c), peer(slabs[1], y, 1 - c)]):
        at = extra.at[odd * 2 + c]
        send(at, at, extra_send.at[0], extra_recv.at[e], to)
    owns["tok"].wait()
    for q in range(tok_pieces):
        at = tok_at(odd, c, x, q)
        send(at, at, tok_send.at[0], tok_recv.at[q], peer(slabs[1], y, c))
    send(own_tok, own_tok, tok_send.at[1], tok_recv.at[8], peer_x(c))
    tok_share(own_tok, True)

    def w_piece(slab, cc, n=1):
        return own_rows((slab * 4 + y * 2 + cc) * shard, n * shard)

    def send_copy(src, dst, send_sem, recv_sem, to):
        return pltpu.make_async_remote_copy(
            src_ref=src, dst_ref=dst, send_sem=send_sem, recv_sem=recv_sem, device_id=to
        )

    ahead = 1

    def w_send_to(u, k, only=None):
        copies = []
        for e in range(2):
            cc = c if e == 0 else 1 - c
            slot = 1 if k == 1 else my_slot
            copies.append(
                send_copy(
                    w_own.at[u, :, lanes((slabs[k] % 2) * 2 + cc)],
                    w_all.at[u, w_piece(z, c)],
                    w_send.at[0],
                    w_recv.at[u, slot],
                    peer(slabs[k], y, cc),
                )
            )
        issue(copies, only)

    def issue(copies, only=None):
        if only is None:
            for copy in copies:
                copy.start()
        else:

            @pl.when(only)
            def _():
                for copy in copies:
                    copy.start()

    pltpu.make_async_copy(w_own, w_own, w_landed).wait()
    for u in range(units):
        pltpu.make_async_copy(
            w_own.at[u, :, lanes(head)], w_all.at[u, w_piece(z, c)], w_recv.at[u, 0]
        ).start()
        send(
            w_own.at[u, :, lanes(odd * 2 + 1 - c)],
            w_all.at[u, w_piece(z, c)],
            w_send.at[0],
            w_recv.at[u, 0],
            other_c,
        )
        w_send_to(u, 1, None if u == 0 else is_mid)
        w_send_to(u, 2, is_mid)
        if u < ahead:
            w_send_to(u, 3, is_mid)

    def w_relay(u, k):
        at = w_all.at[u, w_piece(slabs[k], 0, 2)]
        arrive(at, w_recv.at[u, k])
        send(at, at, wy_send.at[0], wy_recv.at[u], other_y)

    def w_late_end():
        for u in range(units):
            w_send_to(u, 3, is_end)
            w_send_to(u, 2, is_end)
            if u > 0:
                w_send_to(u, 1, is_end)

    def w_late_mid():
        for u in range(ahead, units):
            w_send_to(u, 3, is_mid)

    def w_need(u):
        arrive(w_all.at[u, pl.ds(0, n_rows // 2)], wy_recv.at[u])

    pieces = 4
    depth = o_all.shape[1] // pieces

    def o_at(slab, yy, part):
        return o_all.at[slab * 2 + yy, pl.ds(part * depth, depth)]

    def o_copy(route, part, held, slot, to):
        at = o_at(held, y, part)
        return send_copy(
            at, at, o_send.at[min(route, 1)], o_recv.at[slot - 1, part], peer(to, y, c)
        )

    def o_near():
        for part in range(pieces):
            o_copy(0, part, z, 1, slabs[1]).start()

    def o_across(which):
        @pl.when(is_mid)
        def _():
            for part in which:
                o_copy(1, part, z, 2, slabs[2]).start()

    def o_relay(k, part):
        at = o_at(slabs[k], y, part)
        if k > 0:
            arrive(at, o_recv.at[k - 1, part])
        slot = 4 if (k, part) == (3, pieces - 1) else k
        send(at, at, oy_send.at[0], oy_recv.at[slot], other_y)

    def o_onward(k, part):
        if k == 1:
            o_copy(2, part, slabs[1], 3, slabs[2]).start()
        else:
            o_copy(k + 1, part, slabs[k], k, slabs[1]).start()

    def o_near_relays(which):
        for part in which:
            o_relay(1, part)

            @pl.when(is_mid)
            def _():
                o_onward(1, part)

    def o_mid_relays(k, which):
        @pl.when(is_mid)
        def _():
            for part in which:
                o_relay(k, part)
                o_onward(k, part)

    def o_end_relays(k, which):
        @pl.when(is_end)
        def _():
            for part in which:
                o_relay(k, part)

    def o_need(k):
        arrive(o_all.at[slabs[k] * 2 + 1 - y], oy_recv.at[k])

    def o_need_most():
        arrive(o_all.at[slabs[3] * 2 + 1 - y, pl.ds(0, (pieces - 1) * depth)], oy_recv.at[3])

    def o_need_last():
        arrive(o_at(slabs[3], 1 - y, pieces - 1), oy_recv.at[4])

    for u in range(units):
        w_relay(u, 0)
    pltpu.make_async_copy(o_all.at[here], o_all.at[here], o_landed).wait()

    def tok_z(q):
        at = tok_at(1 - odd, c, x, q)
        arrive(at, tok_recv.at[q])
        send(at, at, tok_send.at[1], tok_recv.at[4 + q], peer_x(c))
        tok_share(at, False)

    def tok_x():
        at = tok_rows(odd, c, 1 - x)
        arrive(at, tok_recv.at[8])
        tok_share(at, True)

    def tok_diagonal(q):
        at = tok_at(1 - odd, c, 1 - x, q)
        arrive(at, tok_recv.at[4 + q])
        tok_share(at, False)

    def tok_shared(zq, near):
        arrive(wide.at[own_rows(zq * half + (1 - c) * rows, rows)], tok_recv.at[9 if near else 10])

    def scale(zq, cc):
        at = own_rows(zq * half + cc * rows, rows)
        values = wide[at, :].astype(f32)
        scaled[at, :] = (values * gain_ref[...]).astype(bf16)
        squares = jnp.sum(values * values, axis=1, keepdims=True)
        inv_rms[at, :] = jnp.broadcast_to(
            lax.rsqrt(squares / wide.shape[1] + eps), (rows, DK)
        )

    def w_relays(u):
        w_relay(u, 1)
        w_relay(u, 2)
        w_relay(u, 3)

    tok_z(0)
    tok_z(1)
    w_late_end()
    for part in range(pieces):
        o_relay(0, part)
    tok_z(2)
    sent(own_tok, tok_send.at[0])
    w_late_mid()
    tok_z(3)
    tok_x()
    for copy in smalls:
        copy.wait()
    scale(odd, c)
    tok_shared(odd, True)
    scale(odd, 1 - c)
    w_relay(0, 2)
    w_relay(0, 1)
    w_relay(0, 3)
    tok_diagonal(0)
    tok_diagonal(1)
    tok_diagonal(2)
    w_relay(1, 1)
    w_relay(1, 2)
    tok_diagonal(3)
    w_relay(1, 3)
    scale(1 - odd, c)
    tok_shared(1 - odd, False)
    scale(1 - odd, 1 - c)
    w_relays(2)

    def project_units(first, count):
        def one(i, _):
            at = own_rows(i * block, block)
            right = [w_all[u] for u in range(first, first + count)]
            right = right[0] if count == 1 else jnp.concatenate(right, axis=1)
            acc = jnp.dot(scaled[at, :], right, preferred_element_type=f32)
            norm = inv_rms[at, :]
            for j in range(count):
                proj[first + j, at, :] = (acc[:, j * DK : (j + 1) * DK] * norm).astype(bf16)
            return 0

        lax.fori_loop(0, blocks, one, 0)

    def project_side(u, yy, last):
        def one(i, _):
            at = own_rows(i * block, block)
            acc = kept[0, at, :] if last else jnp.zeros((block, DK), f32)
            for slab in range(len(slabs)):
                start = pl.multiple_of((slab * 4 + yy * 2) * shard, 2 * shard)
                deep = pl.ds(start, 2 * shard)
                acc = acc + jnp.dot(
                    scaled[at, deep], w_all[u, deep, :], preferred_element_type=f32
                )
            if last:
                proj[u, at, :] = (acc * inv_rms[at, :]).astype(bf16)
            else:
                kept[0, at, :] = acc
            return 0

        lax.fori_loop(0, blocks, one, 0)

    w_need(0)
    w_need(1)
    project_units(0, 2)
    for e, (zq, cc) in enumerate([(odd, 1 - c), (1 - odd, c), (1 - odd, 1 - c)]):
        arrive(extra.at[zq * 2 + cc], extra_recv.at[e])

    rate = rate_ref[:, lanes(head)]
    series = jnp.ones_like(rate)
    for n in range(10, 1, -1):
        series = 1.0 - series * rate / n
    keep = jnp.where(rate < 0.5, rate * series, 1.0 - jnp.exp(-rate))

    row = lax.broadcasted_iota(jnp.int32, (block, block), 0)
    col = lax.broadcasted_iota(jnp.int32, (block, block), 1)
    lower = jnp.where(row >= col, 1.0, 0.0).astype(f32)
    line = lax.broadcasted_iota(jnp.int32, (block, DK), 0)
    eighths = block // 8
    sub = lax.broadcasted_iota(jnp.int32, (eighths, 8, DK), 1)
    over_last = (((1,), (1,)), ((), ()))
    decays = []

    def score_block(b):
        at = slice(b * block, (b + 1) * block)
        q = proj[1, at, :].astype(f32) * DK ** (-0.5)
        kg = keep * jax.nn.sigmoid(-proj[0, at, :].astype(f32))
        added = jnp.broadcast_to(extra[b, pl.ds(head, 1), :], (DK, block)).T
        logs = jnp.log1p(-kg) + added
        cum = jnp.dot(lower, logs, precision=coarsest_scale_depth, preferred_element_type=f32)
        last = cum[block - 1 :, :]
        faded[at, :] = (kg * jnp.exp(last - cum)).astype(bf16)
        decays.append(jnp.exp(last))
        reach[at, :] = (q * jnp.exp(cum)).astype(bf16)
        kept[0, at, :] = cum
        kept[1, at, :] = kg
        scores = jnp.zeros((block, block), f32)
        span = 8
        while span < block:
            twice = 2 * span
            c3 = cum.reshape(block // twice, twice, DK)
            middle = jnp.broadcast_to(c3[:, span - 1 : span, :], c3.shape).reshape(cum.shape)
            fade = jnp.exp(-jnp.abs(cum - middle))
            later = (line // span) % 2 == 1
            probe = jnp.where(later, q * fade, 0.0).astype(bf16)
            keyed = jnp.where(later, 0.0, kg * fade).astype(bf16)
            found = lax.dot_general(probe, keyed, over_last, preferred_element_type=f32)
            scores = scores + jnp.where(row // twice == col // twice, found, 0.0)
            span = twice
        scored[b] = scores.astype(bf16)

    def value_block(b):
        at = slice(b * block, (b + 1) * block)
        q = proj[1, at, :].astype(f32) * DK ** (-0.5)
        v = proj[2, at, :]
        state[b] = lax.dot_general(
            v, faded[at, :], (((0,), (0,)), ((), ())), preferred_element_type=f32
        )
        result = jnp.dot(scored[b], v, preferred_element_type=f32)
        c3 = kept[0, at, :].reshape(eighths, 8, DK)
        q3 = q.reshape(eighths, 8, DK)
        k3 = kept[1, at, :].reshape(eighths, 8, DK)
        v3 = v.astype(f32).reshape(eighths, 8, DK)
        near = result.reshape(eighths, 8, DK)
        for s in range(8):
            weight = jnp.exp(jnp.minimum(c3 - c3[:, s : s + 1, :], 0.0))
            score = jnp.sum(q3 * k3[:, s : s + 1, :] * weight, axis=2, keepdims=True)
            near = near + jnp.where(sub >= s, score * v3[:, s : s + 1, :], 0.0)
        local[at, :] = near.reshape(block, DK)

    score_block(0)
    w_relays(3)
    score_block(1)
    score_block(2)
    score_block(3)
    w_relays(4)
    o_near()
    o_across(range(pieces))
    w_need(2)
    project_units(2, 1)
    for b in range(blocks):
        value_block(b)

    sums = [decays[2 * i + 1] * state[2 * i] + state[2 * i + 1] for i in range(2)]
    fades = [decays[2 * i] * decays[2 * i + 1] for i in range(2)]
    for i in range(2):
        state_go[i] = sums[i].astype(bf16)
        decay_go[i : i + 1, :] = fades[i]
    send(state_go, state_come, scan_send.at[0], scan_recv.at[0], other_y)
    send(decay_go, decay_come, scan_send.at[0], scan_recv.at[1], other_y)
    w_need(3)
    project_units(3, 1)
    for i in range(2):
        tail_go[i] = proj[3, (i + 1) * half - 16 : (i + 1) * half, :]
    send(tail_go, tail_come, scan_send.at[0], scan_recv.at[2], other_y)

    @pl.when(pair == 0)
    def _():
        send(tail_go.at[1], last_come, scan_send.at[1], scan_recv.at[4], across_y)

    w_relays(5)

    arrive(state_come, scan_recv.at[0])
    arrive(decay_come, scan_recv.at[1])
    first_y = y == 0
    theirs = [state_come[i].astype(f32) for i in range(2)]
    their_fades = [decay_come[i : i + 1, :] for i in range(2)]
    order = []
    for i in range(2):
        order.append(
            (jnp.where(first_y, sums[i], theirs[i]), jnp.where(first_y, fades[i], their_fades[i]))
        )
        order.append(
            (jnp.where(first_y, theirs[i], sums[i]), jnp.where(first_y, their_fades[i], fades[i]))
        )
    total = order[0][0]
    for add, fade in order[1:]:
        total = fade * total + add
    total_go[...] = total.astype(bf16)

    @pl.when(pair == 0)
    def _():
        send(total_go, total_come, scan_send.at[1], scan_recv.at[3], across)

    w_need(4)
    project_units(4, 1)
    o_near_relays(range(2))
    o_mid_relays(2, range(2))
    mix_copy.wait()
    arrive(tail_come, scan_recv.at[2])

    @pl.when(pair > 0)
    def _():
        arrive(last_come, scan_recv.at[4])

    @pl.when(pair == 0)
    def _():
        last_come[...] = jnp.zeros_like(last_come)


    at_head = lanes(head)
    level = (x * 4 + head) % 4
    window = 2
    for k in range(1, 4):
        window = jnp.where(level == k, 2 ** (1 + k), window)
    line_half = lax.broadcasted_iota(jnp.int32, (half, DK), 0)
    far = [last_come[...].astype(f32), tail_come[0].astype(f32)]
    their_tails = [tail_come[i].astype(f32) for i in range(2)]
    is_odd = odd == 1

    def pool_half(i):
        at_static = slice(i * half, (i + 1) * half)
        xin = proj[3, at_static, :].astype(f32)
        prior = jnp.where(first_y, far[i], their_tails[i])
        sums_in = jnp.concatenate([prior, xin], axis=0)
        chosen = jnp.zeros((half, DK), f32)
        for k in range(4):
            sums_in = sums_in + pltpu.roll(sums_in, 2**k, 0)
            chosen = jnp.where(level == k, sums_in[16:, :], chosen)
        begins = (4 * pair + 2 * i + y) * half
        count = jnp.minimum(begins + line_half + 1, window).astype(f32)
        mixed = (chosen / count - xin).astype(bf16)
        mapped = jnp.dot(mixed, mix_own[...], preferred_element_type=f32)
        gate = proj[4, at_static, :].astype(f32)
        return mapped * pgain_ref[:, at_head] * (gate * jax.nn.sigmoid(gate))

    z_peer = peer(slabs[1], y, c)
    their_head = (1 - odd) * 2 + c

    def y_at(part, hd, ch):
        return y_all.at[part * 4 + hd, pl.ds(ch * block, block)]

    def y_put(part, ch, low, high):
        at = slice(ch * block, (ch + 1) * block)
        y_go[part, at, :] = jnp.where(is_odd, low, high).astype(bf16)
        y_all[part * 4 + head, at, :] = jnp.where(is_odd, high, low).astype(bf16)
        send(
            y_go.at[part, pl.ds(ch * block, block)],
            y_at(part, head, ch),
            y_send.at[0],
            y_recv.at[part * 2 + ch],
            z_peer,
        )
        at = y_at(part, head, ch)
        send(at, at, y_send.at[0], y_recv.at[4 + ch], other_c)

    def y_pass(part, ch):
        at = y_at(part, their_head, ch)
        arrive(at, y_recv.at[part * 2 + ch])
        send(at, at, y_send.at[0], y_recv.at[4 + ch], other_c)

    def y_need(ch):
        arrive(y_all.at[pl.ds(0, 2)], y_recv.at[4 + ch])

    pooled = [pool_half(i) for i in range(2)]
    for ch in range(2):
        rows_ch = slice(ch * block, (ch + 1) * block)
        y_put(1, ch, pooled[0][rows_ch], pooled[1][rows_ch])
    o_near_relays(range(2, pieces))
    project_side(5, y, False)
    w_need(5)
    project_side(5, 1 - y, True)

    @pl.when(pair > 0)
    def _():
        arrive(total_come, scan_recv.at[3])

    @pl.when(pair == 0)
    def _():
        total_come[...] = jnp.zeros_like(total_come)

    befores = []
    running = total_come[...].astype(f32)
    for i in range(2):
        after_first = order[2 * i][1] * running + order[2 * i][0]
        befores.append(jnp.where(first_y, running, after_first))
        running = order[2 * i + 1][1] * after_first + order[2 * i + 1][0]

    def rec_rows(b, before):
        rows_b = slice(b * block, (b + 1) * block)
        rec = local[rows_b, :] + lax.dot_general(
            reach[rows_b, :], before.astype(bf16), over_last, preferred_element_type=f32
        )
        normed = rec * lax.rsqrt(jnp.mean(rec * rec, axis=1, keepdims=True) + eps)
        gate = proj[5, rows_b, :].astype(f32)
        return normed * sgain_ref[:, at_head] * (gate * jax.nn.sigmoid(gate))

    for ch in range(2):
        recs = []
        for i in range(2):
            b = 2 * i + ch
            recs.append(rec_rows(b, befores[i]))
            befores[i] = decays[b] * befores[i] + state[b]
        y_put(0, ch, recs[0], recs[1])
    o_mid_relays(2, range(2, pieces))
    for ch in range(2):
        y_pass(1, ch)
    o_mid_relays(3, range(2))
    o_end_relays(2, range(2))
    y_pass(0, 0)
    o_mid_relays(3, range(2, pieces))
    y_pass(0, 1)

    owned = part_come.shape[2]

    def rows_for(xx, cc):
        return own_rows(cc * rows + xx * owned, owned)

    def part_copies(k, ch, cols):
        over_x = send_copy(
            part_go.at[k, rows_for(1 - x, ch), cols],
            part_come.at[k, c, :, cols],
            part_send.at[0],
            part_recv.at[k],
            peer_x(ch),
        )
        over_c = send_copy(
            part_go.at[k, rows_for(x, ch), cols],
            part_come.at[k, 2, :, cols],
            part_send.at[0],
            part_recv.at[k],
            other_c,
        )
        return over_x, over_c

    def out_chunk(k, ch, yy=None, rest=False):
        at = slice(ch * block, (ch + 1) * block)
        left = jnp.concatenate(
            [y_all[i, at, :] for i in range(6 if rest else 0, 8)], axis=1
        )
        if yy is None:
            right = jnp.concatenate([o_all[slabs[k] * 2], o_all[slabs[k] * 2 + 1]], axis=1)
            cols = pl.ds(0, 2 * DK)
        else:
            right = o_all[slabs[k] * 2 + yy]
            if rest:
                right = o_all[slabs[k] * 2 + yy, pl.ds((pieces - 1) * depth, depth), :]
            cols = lanes(yy)
        value = jnp.dot(left, right, preferred_element_type=f32)
        if rest:
            value = value + kept[1, at, :]
        part_go[k, at, cols] = value.astype(bf16)
        over_x, over_c = part_copies(k, ch, cols)
        over_x.start()

        @pl.when(c != ch)
        def _():
            over_c.start()

    def drain():
        sent(wide.at[pl.ds(0, 6 * rows // 2)], tok_send.at[1])
        sent(extra.at[pl.ds(0, 3)], extra_send.at[0])
        sent(w_all.at[pl.ds(0, 3), pl.ds(0, 14 * shard)], w_send.at[0])
        sent(w_all.at[pl.ds(0, 3)], wy_send.at[0])
        sent(o_all.at[0], o_send.at[0])
        sent(o_all.at[pl.ds(0, 4)], oy_send.at[0])

        @pl.when(is_mid)
        def _():
            sent(o_all.at[pl.ds(0, 4)], o_send.at[1])

        sent(w_all.at[0, pl.ds(0, 2 * DK + 3 * DK // 8)], scan_send.at[0])

        @pl.when(pair == 0)
        def _():
            sent(w_all.at[0, pl.ds(0, DK + DK // 8)], scan_send.at[1])

        sent(y_all.at[pl.ds(0, 6)], y_send.at[0])

    def gather_chunk(k):
        arrive(part_come.at[k], part_recv.at[k])
        ours = part_go[k, rows_for(x, c), :].astype(f32) + part_come[k, c].astype(f32)
        others = part_come[k, 2].astype(f32) + part_come[k, 1 - c].astype(f32)
        for yy in range(2):
            cols = slice(yy * DK, (yy + 1) * DK)
            mine[:, lanes(slabs[k] * 4 + yy * 2 + c)] = ours[:, cols]
            mine[:, lanes(slabs[k] * 4 + yy * 2 + 1 - c)] = others[:, cols]

    late = [(2, 2), (2, 3), (3, 0), (3, 1), (3, 2), (3, 3)]

    def late_relay():
        k, part = late.pop(0)
        o_end_relays(k, [part])

    for ch in range(2):
        y_need(ch)
        for k in range(2):
            if ch == 0:
                o_need(k)
            out_chunk(k, ch)
            late_relay()
    o_need(2)
    for ch in range(2):
        out_chunk(2, ch)
        late_relay()
    for ch in range(2):
        out_chunk(3, ch, y)
    o_need_most()
    for ch in range(2):
        at = slice(ch * block, (ch + 1) * block)
        left = jnp.concatenate([y_all[i, at, :] for i in range(6)], axis=1)
        right = o_all[slabs[3] * 2 + 1 - y, pl.ds(0, (pieces - 1) * depth), :]
        kept[1, at, :] = jnp.dot(left, right, preferred_element_type=f32)
    o_need_last()
    for ch in range(2):
        out_chunk(3, ch, 1 - y, True)
    drain()
    for k in range(len(slabs)):
        gather_chunk(k)

    def finish():
        summed = mine[...]
        out_ref[...] = (
            summed
            * lax.rsqrt(jnp.mean(summed * summed, axis=1, keepdims=True) + eps)
            * post_ref[...]
        ).astype(bf16)

    finish()
    sent(part_go.at[pl.ds(0, 3)], part_send.at[0])


def pair_layer(
    tokens,
    gain,
    shards,
    rate,
    extra,
    sgain,
    pool_mix,
    pgain,
    out_rec,
    out_pool,
    post,
):
    n = lax.axis_size("sp")
    n_tp = lax.axis_size("tp")
    rows, feats = tokens.shape
    shard, cols = shards[0].shape
    heads = cols // DK
    depth, width = out_rec.shape
    slabs = n // 4
    positions = 4 * rows
    half = 2 * rows
    owned = rows // n_tp
    model = n * width
    f32, bf16, dma = jnp.float32, jnp.bfloat16, pltpu.SemaphoreType.DMA
    units = len(shards)
    hbm = pl.BlockSpec(memory_space=pl.ANY)
    return pl.pallas_call(
        pair_kernel,
        out_shape=pltpu.VMEM((owned, model), bf16),
        in_specs=[pl.BlockSpec(memory_space=pltpu.HBM)] * 16,
        out_specs=pl.BlockSpec(memory_space=pltpu.VMEM),
        scratch_shapes=[
            pltpu.VMEM((positions, n_tp * feats), bf16),
            pltpu.VMEM((positions, n_tp * feats), bf16),
            pltpu.VMEM((positions, DK), f32),
            pltpu.VMEM((units, shard, cols), bf16),
            pltpu.VMEM((units, n * shard, DK), bf16),
            pltpu.VMEM((2 * slabs, 2 * depth, width), bf16),
            pltpu.VMEM((4, heads, rows), f32),
            pltpu.VMEM((DK, DK), bf16),
            pltpu.VMEM((units, positions, DK), bf16),
            pltpu.VMEM((positions, DK), f32),
            pltpu.VMEM((positions, DK), bf16),
            pltpu.VMEM((positions, DK), bf16),
            pltpu.VMEM((2, positions, DK), f32),
            pltpu.VMEM((4, rows, rows), bf16),
            pltpu.VMEM((4, DK, DK), f32),
            pltpu.VMEM((2, DK, DK), bf16),
            pltpu.VMEM((2, DK, DK), bf16),
            pltpu.VMEM((8, DK), f32),
            pltpu.VMEM((8, DK), f32),
            pltpu.VMEM((2, 16, DK), bf16),
            pltpu.VMEM((2, 16, DK), bf16),
            pltpu.VMEM((DK, DK), bf16),
            pltpu.VMEM((DK, DK), bf16),
            pltpu.VMEM((16, DK), bf16),
            pltpu.VMEM((2 * heads, half, DK), bf16),
            pltpu.VMEM((2, half, DK), bf16),
            pltpu.VMEM((slabs, half, 2 * width), bf16),
            pltpu.VMEM((slabs, 3, owned, 2 * width), bf16),
            pltpu.VMEM((owned, model), f32),
            pltpu.VMEM((owned, model), bf16),
            pltpu.VMEM((1, n_tp * feats), f32),
            pltpu.VMEM((1, cols), f32),
            pltpu.VMEM((1, cols), f32),
            pltpu.VMEM((1, cols), f32),
            pltpu.VMEM((1, model), f32),
            dma((5,)),
            dma((5,)),
            dma((2,)),
            dma((11,)),
            dma((1,)),
            dma((3,)),
            dma((1,)),
            dma((units, slabs)),
            dma((1,)),
            dma((units,)),
            dma((2,)),
            dma((3, 4)),
            dma((1,)),
            dma((slabs + 1,)),
            dma((2,)),
            dma((5,)),
            dma((1,)),
            dma((6,)),
            dma((1,)),
            dma((slabs,)),
        ],
        compiler_params=pltpu.CompilerParams(
            collective_id=0, has_side_effects=True, vmem_limit_bytes=32 * 1024 * 1024
        ),
        cost_estimate=pl.CostEstimate(
            flops=2 * positions * n * shard * units * DK,
            bytes_accessed=4 * units * shard * cols,
            transcendentals=0,
        ),
    )(
        *(
            pltpu.with_memory_space_constraint(value, pltpu.HBM)
            for value in (
                tokens,
                gain[None, :],
                *shards,
                rate[None, :],
                extra.T,
                sgain[None, :],
                pool_mix,
                pgain[None, :],
                out_rec,
                out_pool,
                post[None, :],
            )
        )
    )


def per_device(
    tokens_in,
    norm_gain,
    w_query,
    w_forget,
    w_input,
    w_rgate,
    w_pool_in,
    w_pgate,
    floor_rate,
    extra_logdecay,
    state_gain,
    pool_mix,
    pool_gain,
    out_rec,
    out_pool,
    post_gain,
):
    n, n_tp, heads = lax.axis_size("sp"), lax.axis_size("tp"), extra_logdecay.shape[1]
    if n == 16 and n_tp == 2 and heads == 4:
        return pair_layer(
            tokens_in,
            norm_gain,
            [w_forget, w_query, w_input, w_pool_in, w_pgate, w_rgate],
            floor_rate,
            extra_logdecay,
            state_gain,
            pool_mix,
            pool_gain,
            out_rec,
            out_pool,
            post_gain,
        )
    shards = [w_query, w_forget, w_input, w_rgate, w_pool_in, w_pgate]
    proj = project(tokens_in, norm_gain, shards)
    return mix(
        proj,
        -jnp.expm1(-floor_rate)[None, :],
        extra_logdecay,
        state_gain[None, :],
        pool_mix,
        pool_gain[None, :],
        jnp.concatenate([out_rec, out_pool], axis=0),
        post_gain[None, :],
    )


def solution(mesh):
    placed = (
        P("sp", "tp"),
        P(),
        P("sp", "tp"),
        P("sp", "tp"),
        P("sp", "tp"),
        P("sp", "tp"),
        P("sp", "tp"),
        P("sp", "tp"),
        P("tp"),
        P("sp", "tp"),
        P("tp"),
        P("tp", None, None),
        P("tp"),
        P("tp", "sp"),
        P("tp", "sp"),
        P(),
    )
    return jax.shard_map(
        per_device, mesh=mesh, in_specs=placed, out_specs=P(("sp", "tp"), None), check_vma=False
    )
```

```python
import functools

import jax
import jax.numpy as jnp
from jax import lax
from jax.experimental import pallas as pl
from jax.experimental.pallas import tpu as pltpu
from jax.sharding import PartitionSpec as P

DK = 128


eps = 1e-06
coarsest_scale_depth = lax.Precision.HIGHEST


PIECES = 4


def ring_place(chip, chips):
    odd = chip % 2
    return (1 - odd) * (chip // 2) + odd * (chips - 1 - chip // 2)


def ring_chip(place, chips):
    back = place // (chips // 2)
    return (1 - back) * (2 * place) + back * (2 * (chips - 1 - place) + 1)


def project_kernel(
    n,
    n_tp,
    tok_ref,
    gain_ref,
    w0,
    w1,
    w2,
    w3,
    w4,
    w5,
    proj_ref,
    wide,
    scaled,
    weights,
    acc,
    tok_send,
    tok_recv,
    own_sem,
    ring_send,
    ring_recv,
    core_send,
    core_recv,
):
    chips = n // 2
    steps = chips // 2
    me = lax.axis_index("sp")
    tp = lax.axis_index("tp")
    core = me % 2
    place = ring_place(me // 2, chips)

    def chip_at(offset):
        return ring_chip((place + offset + chips) % chips, chips)

    following = 2 * chip_at(1) + core
    preceding = 2 * chip_at(-1) + core
    partner = 2 * (me // 2) + 1 - core
    parts = (w0, w1, w2, w3, w4, w5)
    rows, part_cols = w0.shape
    my_rows = pl.ds(pl.multiple_of(me * rows, 16), rows)
    owns = []
    for i, part in enumerate(parts):
        block = weights.at[my_rows, pl.ds(i * part_cols, part_cols)]
        owns.append(pltpu.make_async_copy(part, block, own_sem.at[i]))
        owns[-1].start()
    piece = rows // PIECES
    features = tok_ref.shape[1]

    barrier = pltpu.get_barrier_semaphore()
    for peer in (following, preceding, partner):
        pl.semaphore_signal(barrier, inc=1, device_id={"sp": peer})
    for turn in range(1, n_tp):
        pl.semaphore_signal(barrier, inc=1, device_id={"tp": (tp + turn) % n_tp})
    pl.semaphore_wait(barrier, 3 + n_tp - 1)

    def rows_of(chip, which, q):
        start = (2 * chip + which) * rows + q * piece
        return pl.ds(pl.multiple_of(start, 8), piece)

    sends = []

    def to_core(offset, q, source):
        slot = offset + steps - 1
        copy = pltpu.make_async_remote_copy(
            src_ref=source,
            dst_ref=weights.at[rows_of(chip_at(offset), core, q)],
            send_sem=core_send.at[slot, q],
            recv_sem=core_recv.at[slot, q],
            device_id={"sp": partner},
        )
        copy.start()
        sends.append(copy)

    def from_core(offset, q):
        slot = offset + steps - 1
        dst = weights.at[rows_of(chip_at(offset), 1 - core, q)]
        pltpu.make_async_remote_copy(
            src_ref=dst,
            dst_ref=dst,
            send_sem=core_send.at[slot, q],
            recv_sem=core_recv.at[slot, q],
            device_id={"sp": partner},
        ).wait_recv()

    def pieces_of(direction, step):
        if step < steps - 1:
            return range(PIECES)
        half = PIECES // 2
        return range(half) if direction == 0 else range(half, PIECES)

    def ring_copy(direction, step, q, source):
        offset = -step if direction == 0 else step
        dst = weights.at[rows_of(chip_at(offset), core, q)]
        return pltpu.make_async_remote_copy(
            src_ref=dst if source is None else source,
            dst_ref=dst,
            send_sem=ring_send.at[direction, step, q],
            recv_sem=ring_recv.at[direction, step, q],
            device_id={"sp": following if direction == 0 else preceding},
        )

    def ring_arrival(direction, step, q):
        offset = -(step + 1) if direction == 0 else step + 1
        dst = weights.at[rows_of(chip_at(offset), core, q)]
        pltpu.make_async_remote_copy(
            src_ref=dst,
            dst_ref=dst,
            send_sem=ring_send.at[direction, step, q],
            recv_sem=ring_recv.at[direction, step, q],
            device_id={"sp": following if direction == 0 else preceding},
        ).wait_recv()

    for own in owns:
        own.wait()
    for q in range(PIECES):
        mine = weights.at[rows_of(me // 2, core, q)]
        for direction in range(2):
            if q in pieces_of(direction, 0):
                copy = ring_copy(direction, 0, q, mine)
                copy.start()
                sends.append(copy)
        to_core(0, q, mine)
    tokens_at = pl.ds(pl.multiple_of(tp * features, 128), features)
    for turn in range(1, n_tp):
        copy = pltpu.make_async_remote_copy(
            src_ref=tok_ref,
            dst_ref=wide.at[:, tokens_at],
            send_sem=tok_send.at[turn - 1],
            recv_sem=tok_recv.at[turn - 1],
            device_id={"tp": (tp + turn) % n_tp},
        )
        copy.start()
        sends.append(copy)
    acc[...] = jnp.zeros_like(acc)
    wide[:, tokens_at] = tok_ref[...]
    for turn in range(1, n_tp):
        theirs = pl.ds(
            pl.multiple_of((tp - turn + n_tp) % n_tp * features, 128), features
        )
        pltpu.make_async_remote_copy(
            src_ref=tok_ref,
            dst_ref=wide.at[:, theirs],
            send_sem=tok_send.at[turn - 1],
            recv_sem=tok_recv.at[turn - 1],
            device_id={"tp": (tp + turn) % n_tp},
        ).wait_recv()
    scaled[...] = (wide[...].astype(jnp.float32) * gain_ref[...]).astype(jnp.bfloat16)

    cols = weights.shape[1]
    tile = cols // 6

    by_chip = (2 * rows) % 128 == 0

    def multiply(offset):
        if not by_chip:
            return
        multiply_rows(pl.ds(pl.multiple_of(chip_at(offset) * 2 * rows, 2 * rows), 2 * rows))

    def multiply_rows(depth):
        def one(i, _):
            at = pl.ds(pl.multiple_of(i * tile, 128), tile)
            acc[:, at] += jnp.dot(
                scaled[:, depth], weights[depth, at], preferred_element_type=jnp.float32
            )
            return 0

        lax.fori_loop(0, 6, one, 0)

    for step in range(steps):
        for q in range(PIECES):
            for direction in range(2):
                if q not in pieces_of(direction, step):
                    continue
                offset = -(step + 1) if direction == 0 else step + 1
                ring_arrival(direction, step, q)
                if step + 1 < steps and q in pieces_of(direction, step + 1):
                    copy = ring_copy(direction, step + 1, q, None)
                    copy.start()
                    sends.append(copy)
                last = offset if abs(offset) < steps else steps
                dst = weights.at[rows_of(chip_at(last), core, q)]
                to_core(last, q, dst)
        for offset in [0] if step == 0 else [-step, step]:
            for q in range(PIECES):
                from_core(offset, q)
            multiply(offset)
    for q in range(PIECES):
        from_core(steps, q)
    multiply(steps)
    if not by_chip:
        multiply_rows(slice(None))
    values = wide[...].astype(jnp.float32)
    squares = jnp.sum(values * values, axis=1, keepdims=True)
    inv_rms = lax.rsqrt(squares / wide.shape[1] + eps)
    proj_ref[...] = (acc[...] * inv_rms).astype(jnp.bfloat16)
    for copy in sends:
        copy.wait_send()


def project(tokens, gain, shards):
    n = lax.axis_size("sp")
    n_tp = lax.axis_size("tp")
    positions, features = tokens.shape
    rows = shards[0].shape[0]
    cols = sum(shard.shape[1] for shard in shards)
    width = n * rows
    steps = n // 4
    dma = pltpu.SemaphoreType.DMA
    return pl.pallas_call(
        functools.partial(project_kernel, n, n_tp),
        out_shape=jax.ShapeDtypeStruct((positions, cols), jnp.bfloat16),
        in_specs=[pl.BlockSpec(memory_space=pltpu.VMEM)] * 2
        + [pl.BlockSpec(memory_space=pl.ANY)] * 6,
        out_specs=pl.BlockSpec(memory_space=pltpu.VMEM),
        scratch_shapes=[
            pltpu.VMEM((positions, width), jnp.bfloat16),
            pltpu.VMEM((positions, width), jnp.bfloat16),
            pltpu.VMEM((width, cols), jnp.bfloat16),
            pltpu.VMEM((positions, cols), jnp.float32),
            dma((n_tp,)),
            dma((n_tp,)),
            dma((6,)),
            dma((2, steps, PIECES)),
            dma((2, steps, PIECES)),
            dma((2 * steps, PIECES)),
            dma((2 * steps, PIECES)),
        ],
        compiler_params=pltpu.CompilerParams(
            collective_id=0, has_side_effects=True, vmem_limit_bytes=56 * 1024 * 1024
        ),
        cost_estimate=pl.CostEstimate(
            flops=2 * positions * width * cols, bytes_accessed=4 * rows * cols, transcendentals=0
        ),
    )(tokens, gain[None, :], *shards)


def mix_kernel(
    n,
    n_tp,
    proj_ref,
    keep_ref,
    extra_ref,
    sgain_ref,
    mix_ref,
    pgain_ref,
    w_ref,
    post_ref,
    out_ref,
    weights,
    local,
    reach,
    both,
    state,
    before,
    gone_state,
    gone_decay,
    come_state,
    come_decay,
    tail,
    tail_in,
    mine,
    gone_out,
    come_out,
    ring_send,
    ring_recv,
    core_send,
    core_recv,
    scan_send,
    scan_recv,
    tail_sem,
    own_sem,
    out_send,
    out_recv,
):
    f32, bf16 = jnp.float32, jnp.bfloat16
    chips = n // 2
    steps = chips // 2
    rounds = (n - 1).bit_length()
    me = lax.axis_index("sp")
    tp = lax.axis_index("tp")
    core = me % 2
    place = ring_place(me // 2, chips)

    def chip_at(offset):
        return ring_chip((place + offset + chips) % chips, chips)

    following = 2 * chip_at(1) + core
    preceding = 2 * chip_at(-1) + core
    partner = 2 * (me // 2) + 1 - core
    piece = w_ref.shape[0] // PIECES

    barrier = pltpu.get_barrier_semaphore()
    for peer in (following, preceding, partner):
        pl.semaphore_signal(barrier, inc=1, device_id={"sp": peer})
    for r in range(rounds):
        pl.semaphore_signal(barrier, inc=1, device_id={"sp": (me + 2**r) % n})
        pl.semaphore_signal(barrier, inc=1, device_id={"sp": (me - 2**r + n) % n})
    for turn in range(1, n_tp):
        pl.semaphore_signal(barrier, inc=1, device_id={"tp": (tp + turn) % n_tp})
    pl.semaphore_wait(barrier, 3 + 2 * rounds + n_tp - 1)

    sends = []

    def spot(chip, which, q):
        return weights.at[2 * chip + which, pl.ds(q * piece, piece)]

    def to_core(offset, q, source):
        slot = offset + steps - 1
        copy = pltpu.make_async_remote_copy(
            src_ref=source,
            dst_ref=spot(chip_at(offset), core, q),
            send_sem=core_send.at[slot, q],
            recv_sem=core_recv.at[slot, q],
            device_id={"sp": partner},
        )
        copy.start()
        sends.append(copy)

    def from_core(offset, q):
        slot = offset + steps - 1
        dst = spot(chip_at(offset), 1 - core, q)
        pltpu.make_async_remote_copy(
            src_ref=dst,
            dst_ref=dst,
            send_sem=core_send.at[slot, q],
            recv_sem=core_recv.at[slot, q],
            device_id={"sp": partner},
        ).wait_recv()

    def pieces_of(direction, step):
        if step < steps - 1:
            return range(PIECES)
        half = PIECES // 2
        return range(half) if direction == 0 else range(half, PIECES)

    def ring_copy(direction, step, q, source, offset):
        dst = spot(chip_at(offset), core, q)
        return pltpu.make_async_remote_copy(
            src_ref=dst if source is None else source,
            dst_ref=dst,
            send_sem=ring_send.at[direction, step, q],
            recv_sem=ring_recv.at[direction, step, q],
            device_id={"sp": following if direction == 0 else preceding},
        )

    def ring_step(step):
        for q in range(PIECES):
            for direction in range(2):
                if q not in pieces_of(direction, step):
                    continue
                offset = -(step + 1) if direction == 0 else step + 1
                ring_copy(direction, step, q, None, offset).wait_recv()
                if step + 1 < steps and q in pieces_of(direction, step + 1):
                    copy = ring_copy(direction, step + 1, q, None, offset)
                    copy.start()
                    sends.append(copy)
                last = offset if abs(offset) < steps else steps
                to_core(last, q, spot(chip_at(last), core, q))

    pending = list(range(steps))

    def advance_ring():
        if pending:
            ring_step(pending.pop(0))

    positions = proj_ref.shape[0]
    head_cols = proj_ref.shape[1] // 6
    heads = head_cols // DK
    reach_back = tail.shape[0]

    tail[...] = proj_ref[positions - reach_back :, 4 * head_cols : 5 * head_cols]
    for q in range(PIECES):
        own_piece = w_ref.at[pl.ds(q * piece, piece)]
        for direction in range(2):
            if q in pieces_of(direction, 0):
                copy = ring_copy(direction, 0, q, own_piece, 0)
                copy.start()
                sends.append(copy)
        to_core(0, q, own_piece)
    own = pltpu.make_async_copy(w_ref, weights.at[me], own_sem)
    own.start()
    tail_copy = pltpu.make_async_remote_copy(
        src_ref=tail,
        dst_ref=tail_in,
        send_sem=tail_sem.at[0],
        recv_sem=tail_sem.at[1],
        device_id={"sp": (me + 1) % n},
    )
    tail_copy.start()

    row = lax.broadcasted_iota(jnp.int32, (positions, positions), 0)
    col = lax.broadcasted_iota(jnp.int32, (positions, positions), 1)
    lower = jnp.where(row >= col, 1.0, 0.0).astype(f32)
    line = lax.broadcasted_iota(jnp.int32, (positions, DK), 0)
    units = positions // 8
    sub = lax.broadcasted_iota(jnp.int32, (units, 8, DK), 1)
    over_last = (((1,), (1,)), ((), ()))

    decay_now = []
    for h in range(heads):
        at = slice(h * DK, (h + 1) * DK)
        part = lambda i: proj_ref[:, i * head_cols + h * DK : i * head_cols + (h + 1) * DK]
        q = part(0).astype(f32) * DK ** (-0.5)
        kg = keep_ref[:, at] * jax.nn.sigmoid(-part(1).astype(f32))
        v = part(2)
        logs = jnp.log1p(-kg) + extra_ref[:, h : h + 1]
        c = jnp.dot(
            lower, logs, precision=coarsest_scale_depth, preferred_element_type=f32
        )
        last = c[positions - 1 :, :]
        state[h] = lax.dot_general(
            v,
            (kg * jnp.exp(last - c)).astype(bf16),
            (((0,), (0,)), ((), ())),
            preferred_element_type=f32,
        )
        gone_decay[0, h : h + 1, :] = jnp.exp(last)
        reach[:, at] = (q * jnp.exp(c)).astype(bf16)
        scores = jnp.zeros((positions, positions), f32)
        span = 8
        while span < positions:
            pair = 2 * span
            c3 = c.reshape(positions // pair, pair, DK)
            middle = jnp.broadcast_to(c3[:, span - 1 : span, :], c3.shape).reshape(c.shape)
            fade = jnp.exp(-jnp.abs(c - middle))
            later = (line // span) % 2 == 1
            probe = jnp.where(later, q * fade, 0.0).astype(bf16)
            keyed = jnp.where(later, 0.0, kg * fade).astype(bf16)
            found = lax.dot_general(probe, keyed, over_last, preferred_element_type=f32)
            scores = scores + jnp.where(row // pair == col // pair, found, 0.0)
            span = pair
        result = jnp.dot(scores.astype(bf16), v, preferred_element_type=f32)
        c3 = c.reshape(units, 8, DK)
        q3 = q.reshape(units, 8, DK)
        k3 = kg.reshape(units, 8, DK)
        v3 = v.astype(f32).reshape(units, 8, DK)
        near = result.reshape(units, 8, DK)
        for s in range(8):
            weight = jnp.exp(jnp.minimum(c3 - c3[:, s : s + 1, :], 0.0))
            score = jnp.sum(q3 * k3[:, s : s + 1, :] * weight, axis=2, keepdims=True)
            near = near + jnp.where(sub >= s, score * v3[:, s : s + 1, :], 0.0)
        local[:, at] = near.reshape(positions, DK)
        if h % 2 == 1:
            advance_ring()

    def scan_copies(r):
        target = {"sp": (me + 2**r) % n}
        return [
            pltpu.make_async_remote_copy(
                src_ref=gone.at[r],
                dst_ref=come.at[r],
                send_sem=scan_send.at[r, i],
                recv_sem=scan_recv.at[r, i],
                device_id=target,
            )
            for i, (gone, come) in enumerate(
                [(gone_state, come_state), (gone_decay, come_decay)]
            )
        ]

    before[...] = jnp.zeros_like(before)
    decay_w = [gone_decay[0, h : h + 1, :] for h in range(heads)]
    decay_e = [jnp.ones((1, DK), f32) for h in range(heads)]

    def pool(h):
        at = slice(h * DK, (h + 1) * DK)
        x = proj_ref[:, 4 * head_cols + h * DK : 4 * head_cols + (h + 1) * DK].astype(f32)
        prior = jnp.where(me > 0, tail_in[:, at].astype(f32), 0.0)
        level = (tp * heads + h) % 4
        total = jnp.concatenate([prior, x], axis=0)
        chosen = jnp.zeros((positions, DK), f32)
        for k in range(4):
            total = total + pltpu.roll(total, 2**k, 0)
            chosen = jnp.where(level == k, total[reach_back:, :], chosen)
        window = 2
        for k in range(1, 4):
            window = jnp.where(level == k, 2 ** (1 + k), window)
        count = jnp.minimum(me * positions + line + 1, window).astype(f32)
        mixed = (chosen / count - x).astype(bf16)
        mapped = jnp.dot(mixed, mix_ref[h], preferred_element_type=f32)
        gate = proj_ref[:, 5 * head_cols + h * DK : 5 * head_cols + (h + 1) * DK].astype(f32)
        both[:, head_cols + h * DK : head_cols + (h + 1) * DK] = (
            mapped * pgain_ref[:, at] * (gate * jax.nn.sigmoid(gate))
        ).astype(bf16)

    pools = list(range(heads))
    for r in range(rounds):
        gone_state[r] = state[...].astype(bf16)
        if r > 0:
            for h in range(heads):
                gone_decay[r, h : h + 1, :] = decay_w[h]
        for copy in scan_copies(r):
            copy.start()
            sends.append(copy)
        if r == 0:
            tail_copy.wait_recv()
        if pools:
            pool(pools.pop(0))
        advance_ring()
        for copy in scan_copies(r):
            copy.wait_recv()
        valid = me >= 2**r
        for h in range(heads):
            came = jnp.where(valid, come_state[r, h].astype(f32), 0.0)
            came_decay = jnp.where(valid, come_decay[r, h : h + 1, :], 1.0)
            before[h] = before[h] + decay_e[h] * came
            decay_e[h] = decay_e[h] * came_decay
            if r + 1 < rounds:
                state[h] = state[h] + decay_w[h] * came
                decay_w[h] = decay_w[h] * came_decay
    for h in pools:
        pool(h)
    while pending:
        advance_ring()

    for h in range(heads):
        at = slice(h * DK, (h + 1) * DK)
        rec = local[:, at] + lax.dot_general(
            reach[:, at], before[h].astype(bf16), over_last, preferred_element_type=f32
        )
        normed = rec * lax.rsqrt(jnp.mean(rec * rec, axis=1, keepdims=True) + eps)
        gate = proj_ref[:, 3 * head_cols + h * DK : 3 * head_cols + (h + 1) * DK].astype(f32)
        both[:, at] = (normed * sgain_ref[:, at] * (gate * jax.nn.sigmoid(gate))).astype(bf16)

    own.wait()
    for offset in range(-(steps - 1), steps + 1):
        for q in range(PIECES):
            from_core(offset, q)

    owned = positions // n_tp
    width = w_ref.shape[1]
    quarter = n // 4

    def share(rows, group):
        left = both[rows, :]
        for slot in range(group * quarter, (group + 1) * quarter, 2):
            right = jnp.concatenate([weights[slot], weights[slot + 1]], axis=1)
            yield slot, jnp.dot(left, right, preferred_element_type=f32).astype(bf16)

    def out_copy(turn, group):
        cols = pl.ds(group * quarter * width, quarter * width)
        return pltpu.make_async_remote_copy(
            src_ref=gone_out.at[turn - 1, :, cols],
            dst_ref=come_out.at[turn - 1, :, cols],
            send_sem=out_send.at[turn - 1, group],
            recv_sem=out_recv.at[turn - 1, group],
            device_id={"tp": (tp + turn) % n_tp},
        )

    for turn in range(1, n_tp):
        target = (tp + turn) % n_tp
        rows = pl.ds(pl.multiple_of(target * owned, owned), owned)
        for group in range(4):
            for slot, value in share(rows, group):
                gone_out[turn - 1, :, slot * width : (slot + 2) * width] = value
            copy = out_copy(turn, group)
            copy.start()
            sends.append(copy)
    rows = pl.ds(pl.multiple_of(tp * owned, owned), owned)
    for group in range(4):
        for slot, value in share(rows, group):
            mine[:, slot * width : (slot + 2) * width] = value.astype(f32)
    for turn in range(1, n_tp):
        for group in range(4):
            out_copy(turn, group).wait_recv()
        mine[...] += come_out[turn - 1].astype(f32)
    summed = mine[...]
    out_ref[...] = (
        summed
        * lax.rsqrt(jnp.mean(summed * summed, axis=1, keepdims=True) + eps)
        * post_ref[...]
    ).astype(bf16)
    tail_copy.wait_send()
    for copy in sends:
        copy.wait_send()


def mix(proj, keep, extra, sgain, pool_mix, pgain, shard, post):
    n = lax.axis_size("sp")
    n_tp = lax.axis_size("tp")
    positions, heads = extra.shape
    head_cols = heads * DK
    depth, width = shard.shape
    steps = n // 4
    rounds = (n - 1).bit_length()
    owned = positions // n_tp
    model = n * width
    padded = -(-heads // 8) * 8
    f32, bf16, dma = jnp.float32, jnp.bfloat16, pltpu.SemaphoreType.DMA
    return pl.pallas_call(
        functools.partial(mix_kernel, n, n_tp),
        out_shape=jax.ShapeDtypeStruct((owned, model), bf16),
        in_specs=[pl.BlockSpec(memory_space=pltpu.VMEM)] * 8,
        out_specs=pl.BlockSpec(memory_space=pltpu.VMEM),
        scratch_shapes=[
            pltpu.VMEM((n, depth, width), bf16),
            pltpu.VMEM((positions, head_cols), f32),
            pltpu.VMEM((positions, head_cols), bf16),
            pltpu.VMEM((positions, 2 * head_cols), bf16),
            pltpu.VMEM((heads, DK, DK), f32),
            pltpu.VMEM((heads, DK, DK), f32),
            pltpu.VMEM((rounds, heads, DK, DK), bf16),
            pltpu.VMEM((rounds, padded, DK), f32),
            pltpu.VMEM((rounds, heads, DK, DK), bf16),
            pltpu.VMEM((rounds, padded, DK), f32),
            pltpu.VMEM((16, head_cols), bf16),
            pltpu.VMEM((16, head_cols), bf16),
            pltpu.VMEM((owned, model), f32),
            pltpu.VMEM((n_tp, owned, model), bf16),
            pltpu.VMEM((n_tp, owned, model), bf16),
            dma((2, steps, PIECES)),
            dma((2, steps, PIECES)),
            dma((2 * steps, PIECES)),
            dma((2 * steps, PIECES)),
            dma((rounds, 2)),
            dma((rounds, 2)),
            dma((2,)),
            dma,
            dma((n_tp, 4)),
            dma((n_tp, 4)),
        ],
        compiler_params=pltpu.CompilerParams(
            collective_id=1, has_side_effects=True, vmem_limit_bytes=56 * 1024 * 1024
        ),
        cost_estimate=pl.CostEstimate(
            flops=2 * positions * depth * model, bytes_accessed=4 * depth * width, transcendentals=0
        ),
    )(proj, keep, extra, sgain, pool_mix, pgain, shard, post)


def pair_kernel(
    tok_hbm,
    gain_hbm,
    w0,
    w1,
    w2,
    w3,
    w4,
    w5,
    rate_hbm,
    extra_hbm,
    sgain_hbm,
    mix_hbm,
    pgain_hbm,
    orec_hbm,
    opool_hbm,
    post_hbm,
    out_ref,
    wide,
    scaled,
    inv_rms,
    w_own,
    w_all,
    o_all,
    extra,
    mix_own,
    proj,
    local,
    reach,
    faded,
    kept,
    scored,
    state,
    state_go,
    state_come,
    decay_go,
    decay_come,
    tail_go,
    tail_come,
    total_go,
    total_come,
    last_come,
    y_all,
    y_go,
    part_go,
    part_come,
    mine,
    done,
    gain_ref,
    rate_ref,
    sgain_ref,
    pgain_ref,
    post_ref,
    small_sem,
    own_sem,
    tok_send,
    tok_recv,
    extra_send,
    extra_recv,
    w_send,
    w_recv,
    wy_send,
    wy_recv,
    o_send,
    o_recv,
    oy_send,
    oy_recv,
    scan_send,
    scan_recv,
    y_send,
    y_recv,
    part_send,
    part_recv,
):
    f32, bf16 = jnp.float32, jnp.bfloat16
    me = lax.axis_index("sp")
    x = lax.axis_index("tp")
    z, y, c = me // 4, (me // 2) % 2, me % 2
    odd = z % 2
    pair = z // 2
    head = odd * 2 + c
    is_mid = (z == 1) | (z == 2)
    is_end = jnp.logical_not(is_mid)
    slabs = [z, z + 1 - 2 * odd, 2 - pair, 3 * (1 - pair)]
    my_slot = jnp.where(is_mid, 2, 3)
    rows, feats = tok_hbm.shape
    shard = w0.shape[0]
    parts = (w0, w1, w2, w3, w4, w5)
    units = len(parts)
    positions = wide.shape[0]
    half = positions // 2
    block = rows
    blocks = positions // block
    n_rows = w_all.shape[1]
    tok_pieces = 4
    piece = rows // tok_pieces

    def peer(zz, yy, cc):
        return {"sp": zz * 4 + yy * 2 + cc}

    def peer_x(cc):
        return {"sp": z * 4 + y * 2 + cc, "tp": 1 - x}

    other_c = peer(z, y, 1 - c)
    other_y = peer(z, 1 - y, c)

    def lanes(i, n=1):
        return pl.ds(pl.multiple_of(i * DK, DK), n * DK)

    def own_rows(base, size):
        return pl.ds(pl.multiple_of(base, 16), size)

    def tok_at(zq, cc, xx, q):
        start = zq * half + cc * rows + q * piece
        return wide.at[own_rows(start, piece), pl.ds(pl.multiple_of(xx * feats, 128), feats)]

    barrier = pltpu.get_barrier_semaphore()
    across = peer((z + 2) % 4, y, c)
    across_y = peer((z + 2) % 4, 1 - y, c)
    peers = [other_c, other_y, peer_x(c), peer_x(1 - c), across_y]
    for k in range(1, 4):
        peers += [peer(slabs[k], y, c), peer(slabs[k], y, 1 - c)]
    for to in peers:
        pl.semaphore_signal(barrier, inc=1, device_id=to)

    owns = {}

    def own_copy(name, src, dst):
        copy = pltpu.make_async_copy(src, dst, own_sem.at[len(owns)])
        copy.start()
        owns[name] = copy

    own_tok = wide.at[
        own_rows(odd * half + c * rows, rows), pl.ds(pl.multiple_of(x * feats, 128), feats)
    ]
    own_copy("tok", tok_hbm, own_tok)
    own_copy("extra", extra_hbm, extra.at[odd * 2 + c])
    here = z * 2 + y
    w_landed = own_sem.at[2]
    for u, part in enumerate(parts):
        pltpu.make_async_copy(part, w_own.at[u], w_landed).start()
    o_landed = own_sem.at[3]
    pltpu.make_async_copy(orec_hbm, o_all.at[here, pl.ds(0, 4 * DK)], o_landed).start()
    pltpu.make_async_copy(opool_hbm, o_all.at[here, pl.ds(4 * DK, 4 * DK)], o_landed).start()
    mix_copy = pltpu.make_async_copy(mix_hbm.at[head], mix_own, own_sem.at[4])
    mix_copy.start()
    smalls = []
    for i, (src, dst) in enumerate(
        [
            (gain_hbm, gain_ref),
            (rate_hbm, rate_ref),
            (sgain_hbm, sgain_ref),
            (pgain_hbm, pgain_ref),
            (post_hbm, post_ref),
        ]
    ):
        smalls.append(pltpu.make_async_copy(src, dst, small_sem.at[i]))
        smalls[-1].start()

    pl.semaphore_wait(barrier, len(peers))

    def send(src, dst, send_sem, recv_sem, to):
        pltpu.make_async_remote_copy(
            src_ref=src, dst_ref=dst, send_sem=send_sem, recv_sem=recv_sem, device_id=to
        ).start()

    def sent(ref, send_sem):
        pltpu.make_async_remote_copy(
            src_ref=ref, dst_ref=ref, send_sem=send_sem, recv_sem=send_sem, device_id=other_c
        ).wait_send()

    def arrive(ref, recv_sem):
        pltpu.make_async_remote_copy(
            src_ref=ref, dst_ref=ref, send_sem=recv_sem, recv_sem=recv_sem, device_id=other_c
        ).wait_recv()

    def tok_rows(zq, cc, xx):
        start = zq * half + cc * rows
        return wide.at[own_rows(start, rows), pl.ds(pl.multiple_of(xx * feats, 128), feats)]

    def tok_share(at, near):
        send(at, at, tok_send.at[1], tok_recv.at[9 if near else 10], other_c)

    owns["extra"].wait()
    for e, to in enumerate([other_c, peer(slabs[1], y, c), peer(slabs[1], y, 1 - c)]):
        at = extra.at[odd * 2 + c]
        send(at, at, extra_send.at[0], extra_recv.at[e], to)
    owns["tok"].wait()
    for q in range(tok_pieces):
        at = tok_at(odd, c, x, q)
        send(at, at, tok_send.at[0], tok_recv.at[q], peer(slabs[1], y, c))
    send(own_tok, own_tok, tok_send.at[1], tok_recv.at[8], peer_x(c))
    tok_share(own_tok, True)

    def w_piece(slab, cc, n=1):
        return own_rows((slab * 4 + y * 2 + cc) * shard, n * shard)

    def send_copy(src, dst, send_sem, recv_sem, to):
        return pltpu.make_async_remote_copy(
            src_ref=src, dst_ref=dst, send_sem=send_sem, recv_sem=recv_sem, device_id=to
        )

    ahead = 1

    def w_send_to(u, k, only=None):
        copies = []
        for e in range(2):
            cc = c if e == 0 else 1 - c
            slot = 1 if k == 1 else my_slot
            copies.append(
                send_copy(
                    w_own.at[u, :, lanes((slabs[k] % 2) * 2 + cc)],
                    w_all.at[u, w_piece(z, c)],
                    w_send.at[0],
                    w_recv.at[u, slot],
                    peer(slabs[k], y, cc),
                )
            )
        issue(copies, only)

    def issue(copies, only=None):
        if only is None:
            for copy in copies:
                copy.start()
        else:

            @pl.when(only)
            def _():
                for copy in copies:
                    copy.start()

    pltpu.make_async_copy(w_own, w_own, w_landed).wait()
    for u in range(units):
        pltpu.make_async_copy(
            w_own.at[u, :, lanes(head)], w_all.at[u, w_piece(z, c)], w_recv.at[u, 0]
        ).start()
        send(
            w_own.at[u, :, lanes(odd * 2 + 1 - c)],
            w_all.at[u, w_piece(z, c)],
            w_send.at[0],
            w_recv.at[u, 0],
            other_c,
        )
        w_send_to(u, 1, None if u == 0 else is_mid)
        w_send_to(u, 2, is_mid)
        if u < ahead:
            w_send_to(u, 3, is_mid)

    def w_relay(u, k):
        at = w_all.at[u, w_piece(slabs[k], 0, 2)]
        arrive(at, w_recv.at[u, k])
        send(at, at, wy_send.at[0], wy_recv.at[u], other_y)

    def w_late_end():
        for u in range(units):
            w_send_to(u, 3, is_end)
            w_send_to(u, 2, is_end)
            if u > 0:
                w_send_to(u, 1, is_end)

    def w_late_mid():
        for u in range(ahead, units):
            w_send_to(u, 3, is_mid)

    def w_need(u):
        arrive(w_all.at[u, pl.ds(0, n_rows // 2)], wy_recv.at[u])

    pieces = 8
    depth = o_all.shape[1] // pieces

    def o_at(slab, yy, part):
        return o_all.at[slab * 2 + yy, pl.ds(part * depth, depth)]

    def o_copy(route, part, held, slot, to):
        at = o_at(held, y, part)
        return send_copy(
            at, at, o_send.at[min(route, 1)], o_recv.at[slot - 1, part], peer(to, y, c)
        )

    def o_near():
        for part in range(pieces):
            o_copy(0, part, z, 1, slabs[1]).start()

    def o_across(which):
        @pl.when(is_mid)
        def _():
            for part in which:
                o_copy(1, part, z, 2, slabs[2]).start()

    def o_relay(k, part):
        at = o_at(slabs[k], y, part)
        if k > 0:
            arrive(at, o_recv.at[k - 1, part])
        slot = 4 if (k, part) == (3, pieces - 1) else k
        send(at, at, oy_send.at[0], oy_recv.at[slot], other_y)

    def o_onward(k, part):
        if k == 1:
            o_copy(2, part, slabs[1], 3, slabs[2]).start()
        else:
            o_copy(k + 1, part, slabs[k], k, slabs[1]).start()

    def o_near_relays(which):
        for part in which:
            o_relay(1, part)

            @pl.when(is_mid)
            def _():
                o_onward(1, part)

    def o_mid_relays(k, which):
        @pl.when(is_mid)
        def _():
            for part in which:
                o_relay(k, part)
                o_onward(k, part)

    def o_end_relays(k, which):
        @pl.when(is_end)
        def _():
            for part in which:
                o_relay(k, part)

    def o_need(k):
        arrive(o_all.at[slabs[k] * 2 + 1 - y], oy_recv.at[k])

    def o_need_most():
        arrive(o_all.at[slabs[3] * 2 + 1 - y, pl.ds(0, (pieces - 1) * depth)], oy_recv.at[3])

    def o_need_last():
        arrive(o_at(slabs[3], 1 - y, pieces - 1), oy_recv.at[4])

    for u in range(units):
        w_relay(u, 0)
    pltpu.make_async_copy(o_all.at[here], o_all.at[here], o_landed).wait()

    def tok_z(q):
        at = tok_at(1 - odd, c, x, q)
        arrive(at, tok_recv.at[q])
        send(at, at, tok_send.at[1], tok_recv.at[4 + q], peer_x(c))
        tok_share(at, False)

    def tok_x():
        at = tok_rows(odd, c, 1 - x)
        arrive(at, tok_recv.at[8])
        tok_share(at, True)

    def tok_diagonal(q):
        at = tok_at(1 - odd, c, 1 - x, q)
        arrive(at, tok_recv.at[4 + q])
        tok_share(at, False)

    def tok_shared(zq, near):
        arrive(wide.at[own_rows(zq * half + (1 - c) * rows, rows)], tok_recv.at[9 if near else 10])

    def scale(zq, cc):
        at = own_rows(zq * half + cc * rows, rows)
        values = wide[at, :].astype(f32)
        scaled[at, :] = (values * gain_ref[...]).astype(bf16)
        squares = jnp.sum(values * values, axis=1, keepdims=True)
        inv_rms[at, :] = jnp.broadcast_to(
            lax.rsqrt(squares / wide.shape[1] + eps), (rows, DK)
        )

    def w_relays(u):
        w_relay(u, 1)
        w_relay(u, 2)
        w_relay(u, 3)

    tok_z(0)
    tok_z(1)
    w_late_end()
    for part in range(pieces):
        o_relay(0, part)
    tok_z(2)
    sent(own_tok, tok_send.at[0])
    w_late_mid()
    tok_z(3)
    tok_x()
    for copy in smalls:
        copy.wait()
    scale(odd, c)
    tok_shared(odd, True)
    scale(odd, 1 - c)
    w_relay(0, 2)
    w_relay(0, 1)
    w_relay(0, 3)
    tok_diagonal(0)
    tok_diagonal(1)
    tok_diagonal(2)
    w_relay(1, 1)
    w_relay(1, 2)
    tok_diagonal(3)
    w_relay(1, 3)
    scale(1 - odd, c)
    tok_shared(1 - odd, False)
    scale(1 - odd, 1 - c)
    w_relays(2)

    def project_units(first, count):
        def one(i, _):
            at = own_rows(i * block, block)
            right = [w_all[u] for u in range(first, first + count)]
            right = right[0] if count == 1 else jnp.concatenate(right, axis=1)
            acc = jnp.dot(scaled[at, :], right, preferred_element_type=f32)
            norm = inv_rms[at, :]
            for j in range(count):
                proj[first + j, at, :] = (acc[:, j * DK : (j + 1) * DK] * norm).astype(bf16)
            return 0

        lax.fori_loop(0, blocks, one, 0)

    def project_side(u, yy, last):
        def one(i, _):
            at = own_rows(i * block, block)
            acc = kept[0, at, :] if last else jnp.zeros((block, DK), f32)
            for slab in range(len(slabs)):
                start = pl.multiple_of((slab * 4 + yy * 2) * shard, 2 * shard)
                deep = pl.ds(start, 2 * shard)
                acc = acc + jnp.dot(
                    scaled[at, deep], w_all[u, deep, :], preferred_element_type=f32
                )
            if last:
                proj[u, at, :] = (acc * inv_rms[at, :]).astype(bf16)
            else:
                kept[0, at, :] = acc
            return 0

        lax.fori_loop(0, blocks, one, 0)

    w_need(0)
    w_need(1)
    project_units(0, 2)
    for e, (zq, cc) in enumerate([(odd, 1 - c), (1 - odd, c), (1 - odd, 1 - c)]):
        arrive(extra.at[zq * 2 + cc], extra_recv.at[e])

    rate = rate_ref[:, lanes(head)]
    series = jnp.ones_like(rate)
    for n in range(10, 1, -1):
        series = 1.0 - series * rate / n
    keep = jnp.where(rate < 0.5, rate * series, 1.0 - jnp.exp(-rate))

    row = lax.broadcasted_iota(jnp.int32, (block, block), 0)
    col = lax.broadcasted_iota(jnp.int32, (block, block), 1)
    lower = jnp.where(row >= col, 1.0, 0.0).astype(f32)
    line = lax.broadcasted_iota(jnp.int32, (block, DK), 0)
    eighths = block // 8
    sub = lax.broadcasted_iota(jnp.int32, (eighths, 8, DK), 1)
    over_last = (((1,), (1,)), ((), ()))
    decays = []

    def score_block(b):
        at = slice(b * block, (b + 1) * block)
        q = proj[1, at, :].astype(f32) * DK ** (-0.5)
        kg = keep * jax.nn.sigmoid(-proj[0, at, :].astype(f32))
        added = jnp.broadcast_to(extra[b, pl.ds(head, 1), :], (DK, block)).T
        logs = jnp.log1p(-kg) + added
        cum = jnp.dot(lower, logs, precision=coarsest_scale_depth, preferred_element_type=f32)
        last = cum[block - 1 :, :]
        faded[at, :] = (kg * jnp.exp(last - cum)).astype(bf16)
        decays.append(jnp.exp(last))
        reach[at, :] = (q * jnp.exp(cum)).astype(bf16)
        kept[0, at, :] = cum
        kept[1, at, :] = kg
        scores = jnp.zeros((block, block), f32)
        span = 8
        while span < block:
            twice = 2 * span
            c3 = cum.reshape(block // twice, twice, DK)
            middle = jnp.broadcast_to(c3[:, span - 1 : span, :], c3.shape).reshape(cum.shape)
            fade = jnp.exp(-jnp.abs(cum - middle))
            later = (line // span) % 2 == 1
            probe = jnp.where(later, q * fade, 0.0).astype(bf16)
            keyed = jnp.where(later, 0.0, kg * fade).astype(bf16)
            found = lax.dot_general(probe, keyed, over_last, preferred_element_type=f32)
            scores = scores + jnp.where(row // twice == col // twice, found, 0.0)
            span = twice
        scored[b] = scores.astype(bf16)

    def value_block(b):
        at = slice(b * block, (b + 1) * block)
        q = proj[1, at, :].astype(f32) * DK ** (-0.5)
        v = proj[2, at, :]
        state[b] = lax.dot_general(
            v, faded[at, :], (((0,), (0,)), ((), ())), preferred_element_type=f32
        )
        result = jnp.dot(scored[b], v, preferred_element_type=f32)
        c3 = kept[0, at, :].reshape(eighths, 8, DK)
        q3 = q.reshape(eighths, 8, DK)
        k3 = kept[1, at, :].reshape(eighths, 8, DK)
        v3 = v.astype(f32).reshape(eighths, 8, DK)
        near = result.reshape(eighths, 8, DK)
        for s in range(8):
            weight = jnp.exp(jnp.minimum(c3 - c3[:, s : s + 1, :], 0.0))
            score = jnp.sum(q3 * k3[:, s : s + 1, :] * weight, axis=2, keepdims=True)
            near = near + jnp.where(sub >= s, score * v3[:, s : s + 1, :], 0.0)
        local[at, :] = near.reshape(block, DK)

    score_block(0)
    w_relays(3)
    score_block(1)
    score_block(2)
    score_block(3)
    w_relays(4)
    o_near()
    o_across(range(pieces))
    w_need(2)
    project_units(2, 1)
    for b in range(blocks):
        value_block(b)

    sums = [decays[2 * i + 1] * state[2 * i] + state[2 * i + 1] for i in range(2)]
    fades = [decays[2 * i] * decays[2 * i + 1] for i in range(2)]
    for i in range(2):
        state_go[i] = sums[i].astype(bf16)
        decay_go[i : i + 1, :] = fades[i]
    send(state_go, state_come, scan_send.at[0], scan_recv.at[0], other_y)
    send(decay_go, decay_come, scan_send.at[0], scan_recv.at[1], other_y)
    w_need(3)
    project_units(3, 1)
    for i in range(2):
        tail_go[i] = proj[3, (i + 1) * half - 16 : (i + 1) * half, :]
    send(tail_go, tail_come, scan_send.at[0], scan_recv.at[2], other_y)

    @pl.when(pair == 0)
    def _():
        send(tail_go.at[1], last_come, scan_send.at[1], scan_recv.at[4], across_y)

    w_relays(5)

    arrive(state_come, scan_recv.at[0])
    arrive(decay_come, scan_recv.at[1])
    first_y = y == 0
    theirs = [state_come[i].astype(f32) for i in range(2)]
    their_fades = [decay_come[i : i + 1, :] for i in range(2)]
    order = []
    for i in range(2):
        order.append(
            (jnp.where(first_y, sums[i], theirs[i]), jnp.where(first_y, fades[i], their_fades[i]))
        )
        order.append(
            (jnp.where(first_y, theirs[i], sums[i]), jnp.where(first_y, their_fades[i], fades[i]))
        )
    total = order[0][0]
    for add, fade in order[1:]:
        total = fade * total + add
    total_go[...] = total.astype(bf16)

    @pl.when(pair == 0)
    def _():
        send(total_go, total_come, scan_send.at[1], scan_recv.at[3], across)

    w_need(4)
    project_units(4, 1)
    o_near_relays(range(4))
    o_mid_relays(2, range(4))
    mix_copy.wait()
    arrive(tail_come, scan_recv.at[2])

    @pl.when(pair > 0)
    def _():
        arrive(last_come, scan_recv.at[4])

    @pl.when(pair == 0)
    def _():
        last_come[...] = jnp.zeros_like(last_come)


    at_head = lanes(head)
    level = (x * 4 + head) % 4
    window = 2
    for k in range(1, 4):
        window = jnp.where(level == k, 2 ** (1 + k), window)
    line_half = lax.broadcasted_iota(jnp.int32, (half, DK), 0)
    far = [last_come[...].astype(f32), tail_come[0].astype(f32)]
    their_tails = [tail_come[i].astype(f32) for i in range(2)]
    is_odd = odd == 1

    def pool_half(i):
        at_static = slice(i * half, (i + 1) * half)
        xin = proj[3, at_static, :].astype(f32)
        prior = jnp.where(first_y, far[i], their_tails[i])
        sums_in = jnp.concatenate([prior, xin], axis=0)
        chosen = jnp.zeros((half, DK), f32)
        for k in range(4):
            sums_in = sums_in + pltpu.roll(sums_in, 2**k, 0)
            chosen = jnp.where(level == k, sums_in[16:, :], chosen)
        begins = (4 * pair + 2 * i + y) * half
        count = jnp.minimum(begins + line_half + 1, window).astype(f32)
        mixed = (chosen / count - xin).astype(bf16)
        mapped = jnp.dot(mixed, mix_own[...], preferred_element_type=f32)
        gate = proj[4, at_static, :].astype(f32)
        return mapped * pgain_ref[:, at_head] * (gate * jax.nn.sigmoid(gate))

    z_peer = peer(slabs[1], y, c)
    their_head = (1 - odd) * 2 + c

    def y_at(part, hd, ch):
        return y_all.at[part * 4 + hd, pl.ds(ch * block, block)]

    def y_put(part, ch, low, high):
        at = slice(ch * block, (ch + 1) * block)
        y_go[part, at, :] = jnp.where(is_odd, low, high).astype(bf16)
        y_all[part * 4 + head, at, :] = jnp.where(is_odd, high, low).astype(bf16)
        send(
            y_go.at[part, pl.ds(ch * block, block)],
            y_at(part, head, ch),
            y_send.at[0],
            y_recv.at[part * 2 + ch],
            z_peer,
        )
        at = y_at(part, head, ch)
        send(at, at, y_send.at[0], y_recv.at[4 + ch], other_c)

    def y_pass(part, ch):
        at = y_at(part, their_head, ch)
        arrive(at, y_recv.at[part * 2 + ch])
        send(at, at, y_send.at[0], y_recv.at[4 + ch], other_c)

    def y_need(ch):
        arrive(y_all.at[pl.ds(0, 2)], y_recv.at[4 + ch])

    pooled = [pool_half(i) for i in range(2)]
    for ch in range(2):
        rows_ch = slice(ch * block, (ch + 1) * block)
        y_put(1, ch, pooled[0][rows_ch], pooled[1][rows_ch])
    o_near_relays(range(4, pieces))
    project_side(5, y, False)

    @pl.when(pair > 0)
    def _():
        arrive(total_come, scan_recv.at[3])

    @pl.when(pair == 0)
    def _():
        total_come[...] = jnp.zeros_like(total_come)

    befores = []
    running = total_come[...].astype(f32)
    for i in range(2):
        after_first = order[2 * i][1] * running + order[2 * i][0]
        befores.append(jnp.where(first_y, running, after_first))
        running = order[2 * i + 1][1] * after_first + order[2 * i + 1][0]

    def rec_rows(b, before):
        rows_b = slice(b * block, (b + 1) * block)
        rec = local[rows_b, :] + lax.dot_general(
            reach[rows_b, :], before.astype(bf16), over_last, preferred_element_type=f32
        )
        normed = rec * lax.rsqrt(jnp.mean(rec * rec, axis=1, keepdims=True) + eps)
        local[rows_b, :] = normed * sgain_ref[:, at_head]

    for ch in range(2):
        for i in range(2):
            b = 2 * i + ch
            rec_rows(b, befores[i])
            befores[i] = decays[b] * befores[i] + state[b]

    def gated(b):
        rows_b = slice(b * block, (b + 1) * block)
        gate = proj[5, rows_b, :].astype(f32)
        return local[rows_b, :] * (gate * jax.nn.sigmoid(gate))

    w_need(5)
    project_side(5, 1 - y, True)
    for ch in range(2):
        recs = [gated(2 * i + ch) for i in range(2)]
        y_put(0, ch, recs[0], recs[1])
    o_mid_relays(2, range(4, pieces))
    for ch in range(2):
        y_pass(1, ch)
    o_mid_relays(3, range(4))
    o_end_relays(2, range(4))
    y_pass(0, 0)
    o_mid_relays(3, range(4, pieces))
    y_pass(0, 1)

    owned = part_come.shape[2]

    def rows_for(xx, cc):
        return own_rows(cc * rows + xx * owned, owned)

    def part_copies(k, ch, cols):
        over_x = send_copy(
            part_go.at[k, rows_for(1 - x, ch), cols],
            part_come.at[k, c, :, cols],
            part_send.at[0],
            part_recv.at[k],
            peer_x(ch),
        )
        over_c = send_copy(
            part_go.at[k, rows_for(x, ch), cols],
            part_come.at[k, 2, :, cols],
            part_send.at[0],
            part_recv.at[k],
            other_c,
        )
        return over_x, over_c

    def out_chunk(k, ch, yy=None, rest=False):
        at = slice(ch * block, (ch + 1) * block)
        left = jnp.concatenate(
            [y_all[i, at, :] for i in range(7 if rest else 0, 8)], axis=1
        )
        if yy is None:
            right = jnp.concatenate([o_all[slabs[k] * 2], o_all[slabs[k] * 2 + 1]], axis=1)
            cols = pl.ds(0, 2 * DK)
        else:
            right = o_all[slabs[k] * 2 + yy]
            if rest:
                right = o_all[slabs[k] * 2 + yy, pl.ds((pieces - 1) * depth, depth), :]
            cols = lanes(yy)
        value = jnp.dot(left, right, preferred_element_type=f32)
        if rest:
            value = value + kept[1, at, :]
        part_go[k, at, cols] = value.astype(bf16)
        over_x, over_c = part_copies(k, ch, cols)
        over_x.start()

        @pl.when(c != ch)
        def _():
            over_c.start()

    def drain():
        sent(wide.at[pl.ds(0, 6 * rows // 2)], tok_send.at[1])
        sent(extra.at[pl.ds(0, 3)], extra_send.at[0])
        sent(w_all.at[pl.ds(0, 3), pl.ds(0, 14 * shard)], w_send.at[0])
        sent(w_all.at[pl.ds(0, 3)], wy_send.at[0])
        sent(o_all.at[0], o_send.at[0])
        sent(o_all.at[pl.ds(0, 4)], oy_send.at[0])

        @pl.when(is_mid)
        def _():
            sent(o_all.at[pl.ds(0, 4)], o_send.at[1])

        sent(w_all.at[0, pl.ds(0, 2 * DK + 3 * DK // 8)], scan_send.at[0])

        @pl.when(pair == 0)
        def _():
            sent(w_all.at[0, pl.ds(0, DK + DK // 8)], scan_send.at[1])

        sent(y_all.at[pl.ds(0, 6)], y_send.at[0])

    def gather_chunk(k):
        arrive(part_come.at[k], part_recv.at[k])
        ours = part_go[k, rows_for(x, c), :].astype(f32) + part_come[k, c].astype(f32)
        others = part_come[k, 2].astype(f32) + part_come[k, 1 - c].astype(f32)
        for yy in range(2):
            cols = slice(yy * DK, (yy + 1) * DK)
            mine[:, lanes(slabs[k] * 4 + yy * 2 + c)] = ours[:, cols]
            mine[:, lanes(slabs[k] * 4 + yy * 2 + 1 - c)] = others[:, cols]

    late = [(2, 4), (2, 6), (3, 0), (3, 2), (3, 4), (3, 6)]

    def late_relay():
        k, part = late.pop(0)
        o_end_relays(k, [part, part + 1])

    for ch in range(2):
        y_need(ch)
        for k in range(2):
            if ch == 0:
                o_need(k)
            out_chunk(k, ch)
            late_relay()
    o_need(2)
    for ch in range(2):
        out_chunk(2, ch)
        late_relay()
    for ch in range(2):
        out_chunk(3, ch, y)
    o_need_most()
    for ch in range(2):
        at = slice(ch * block, (ch + 1) * block)
        left = jnp.concatenate([y_all[i, at, :] for i in range(7)], axis=1)
        right = o_all[slabs[3] * 2 + 1 - y, pl.ds(0, (pieces - 1) * depth), :]
        kept[1, at, :] = jnp.dot(left, right, preferred_element_type=f32)
    o_need_last()
    for ch in range(2):
        out_chunk(3, ch, 1 - y, True)
    drain()
    for k in range(len(slabs)):
        gather_chunk(k)

    def finish():
        summed = mine[...]
        out_ref[...] = (
            summed
            * lax.rsqrt(jnp.mean(summed * summed, axis=1, keepdims=True) + eps)
            * post_ref[...]
        ).astype(bf16)

    finish()
    sent(part_go.at[pl.ds(0, 3)], part_send.at[0])


def pair_layer(
    tokens,
    gain,
    shards,
    rate,
    extra,
    sgain,
    pool_mix,
    pgain,
    out_rec,
    out_pool,
    post,
):
    n = lax.axis_size("sp")
    n_tp = lax.axis_size("tp")
    rows, feats = tokens.shape
    shard, cols = shards[0].shape
    heads = cols // DK
    depth, width = out_rec.shape
    slabs = n // 4
    positions = 4 * rows
    half = 2 * rows
    owned = rows // n_tp
    model = n * width
    f32, bf16, dma = jnp.float32, jnp.bfloat16, pltpu.SemaphoreType.DMA
    units = len(shards)
    hbm = pl.BlockSpec(memory_space=pl.ANY)
    return pl.pallas_call(
        pair_kernel,
        out_shape=pltpu.VMEM((owned, model), bf16),
        in_specs=[pl.BlockSpec(memory_space=pltpu.HBM)] * 16,
        out_specs=pl.BlockSpec(memory_space=pltpu.VMEM),
        scratch_shapes=[
            pltpu.VMEM((positions, n_tp * feats), bf16),
            pltpu.VMEM((positions, n_tp * feats), bf16),
            pltpu.VMEM((positions, DK), f32),
            pltpu.VMEM((units, shard, cols), bf16),
            pltpu.VMEM((units, n * shard, DK), bf16),
            pltpu.VMEM((2 * slabs, 2 * depth, width), bf16),
            pltpu.VMEM((4, heads, rows), f32),
            pltpu.VMEM((DK, DK), bf16),
            pltpu.VMEM((units, positions, DK), bf16),
            pltpu.VMEM((positions, DK), f32),
            pltpu.VMEM((positions, DK), bf16),
            pltpu.VMEM((positions, DK), bf16),
            pltpu.VMEM((2, positions, DK), f32),
            pltpu.VMEM((4, rows, rows), bf16),
            pltpu.VMEM((4, DK, DK), f32),
            pltpu.VMEM((2, DK, DK), bf16),
            pltpu.VMEM((2, DK, DK), bf16),
            pltpu.VMEM((8, DK), f32),
            pltpu.VMEM((8, DK), f32),
            pltpu.VMEM((2, 16, DK), bf16),
            pltpu.VMEM((2, 16, DK), bf16),
            pltpu.VMEM((DK, DK), bf16),
            pltpu.VMEM((DK, DK), bf16),
            pltpu.VMEM((16, DK), bf16),
            pltpu.VMEM((2 * heads, half, DK), bf16),
            pltpu.VMEM((2, half, DK), bf16),
            pltpu.VMEM((slabs, half, 2 * width), bf16),
            pltpu.VMEM((slabs, 3, owned, 2 * width), bf16),
            pltpu.VMEM((owned, model), f32),
            pltpu.VMEM((owned, model), bf16),
            pltpu.VMEM((1, n_tp * feats), f32),
            pltpu.VMEM((1, cols), f32),
            pltpu.VMEM((1, cols), f32),
            pltpu.VMEM((1, cols), f32),
            pltpu.VMEM((1, model), f32),
            dma((5,)),
            dma((5,)),
            dma((2,)),
            dma((11,)),
            dma((1,)),
            dma((3,)),
            dma((1,)),
            dma((units, slabs)),
            dma((1,)),
            dma((units,)),
            dma((2,)),
            dma((3, 8)),
            dma((1,)),
            dma((slabs + 1,)),
            dma((2,)),
            dma((5,)),
            dma((1,)),
            dma((6,)),
            dma((1,)),
            dma((slabs,)),
        ],
        compiler_params=pltpu.CompilerParams(
            collective_id=0, has_side_effects=True, vmem_limit_bytes=32 * 1024 * 1024
        ),
        cost_estimate=pl.CostEstimate(
            flops=2 * positions * n * shard * units * DK,
            bytes_accessed=4 * units * shard * cols,
            transcendentals=0,
        ),
    )(
        *(
            pltpu.with_memory_space_constraint(value, pltpu.HBM)
            for value in (
                tokens,
                gain[None, :],
                *shards,
                rate[None, :],
                extra.T,
                sgain[None, :],
                pool_mix,
                pgain[None, :],
                out_rec,
                out_pool,
                post[None, :],
            )
        )
    )


def per_device(
    tokens_in,
    norm_gain,
    w_query,
    w_forget,
    w_input,
    w_rgate,
    w_pool_in,
    w_pgate,
    floor_rate,
    extra_logdecay,
    state_gain,
    pool_mix,
    pool_gain,
    out_rec,
    out_pool,
    post_gain,
):
    n, n_tp, heads = lax.axis_size("sp"), lax.axis_size("tp"), extra_logdecay.shape[1]
    if n == 16 and n_tp == 2 and heads == 4:
        return pair_layer(
            tokens_in,
            norm_gain,
            [w_forget, w_query, w_input, w_pool_in, w_pgate, w_rgate],
            floor_rate,
            extra_logdecay,
            state_gain,
            pool_mix,
            pool_gain,
            out_rec,
            out_pool,
            post_gain,
        )
    shards = [w_query, w_forget, w_input, w_rgate, w_pool_in, w_pgate]
    proj = project(tokens_in, norm_gain, shards)
    return mix(
        proj,
        -jnp.expm1(-floor_rate)[None, :],
        extra_logdecay,
        state_gain[None, :],
        pool_mix,
        pool_gain[None, :],
        jnp.concatenate([out_rec, out_pool], axis=0),
        post_gain[None, :],
    )


def solution(mesh):
    placed = (
        P("sp", "tp"),
        P(),
        P("sp", "tp"),
        P("sp", "tp"),
        P("sp", "tp"),
        P("sp", "tp"),
        P("sp", "tp"),
        P("sp", "tp"),
        P("tp"),
        P("sp", "tp"),
        P("tp"),
        P("tp", None, None),
        P("tp"),
        P("tp", "sp"),
        P("tp", "sp"),
        P(),
    )
    return jax.shard_map(
        per_device, mesh=mesh, in_specs=placed, out_specs=P(("sp", "tp"), None), check_vma=False
    )
```
